512 devices in a mesh: sp: 32 (over z, x), dp: 16 (over y, core).
Axes of the slice: x: 4, y: 8, z: 8, core: 2. Of those that a mesh axis runs over, the one named last changes fastest.
Arguments:
- queries: bfloat16 [64, 8, 2048, 128], P('dp', None, 'sp'), may hold values from -6 to 6
- keys: bfloat16 [64, 8, 2048, 128], P('dp', None, 'sp'), may hold values from -6 to 6
- values: bfloat16 [64, 8, 2048, 128], P('dp', None, 'sp'), may hold values from -6 to 6
- input_gate: bfloat16 [64, 8, 2048], P('dp', None, 'sp'), may hold values from -6 to 140
- forget_gate: bfloat16 [64, 8, 2048], P('dp', None, 'sp'), may hold values from 0.5 to 11.5
- start_memory: float32 [64, 8, 128, 128], P('dp', None, 'sp'), may hold values from -6 to 6
- start_norm: float32 [64, 8, 128], P('dp', None, 'sp'), may hold values from -24 to 24
- start_level: float32 [64, 8], P('dp'), may hold values from 2 to 4
- head_gain: float32 [8, 128], replicated, may hold values from 0.1 to 1.9
- out_weight: bfloat16 [1024, 4096], P(None, 'dp'), may hold values from -0.1875 to 0.1875
Outputs:
- mixed: bfloat16 [64, 2048, 4096], P('dp', 'sp')
The draws below stay inside these ranges and needn't reach their ends.
All inputs are finite; a program needn't handle non-finite values.
Results may differ from the reference program's by a relative error of at most 0.019.
Values may be sent and summed in bfloat16 or wider, within the bound.
A program may use at most 64 MiB of HBM per device.

```python
import jax
import jax.numpy as jnp
from jax import lax

D = 4096
HEADS = 8
HD = 128
BLOCK = 64
SEG = 64
MIX = 1024
LEN = 2048
BATCH = 64


def draw_input_gate(key, part):
    first, second, third = jax.random.split(key, 3)
    plain = jax.random.normal(first, (BATCH, HEADS, LEN), jnp.float32)
    result = jnp.clip(plain, -6.0, 6.0)
    return result.astype(jnp.bfloat16)


def draw_forget_gate(key, part):
    first, second, third = jax.random.split(key, 3)
    slow_share = 0.5
    slow = jax.random.bernoulli(first, slow_share, (BATCH, HEADS, 1))
    base = jnp.where(slow, jnp.log(LEN / 1.2), 3.5)
    spans = LEN // SEG
    factor = jnp.exp(jax.random.uniform(second, (BATCH, HEADS, spans), jnp.float32, -0.693, 0.693))
    factor = jnp.repeat(factor, SEG, axis=2)
    noise = 0.3 * jax.random.normal(third, (BATCH, HEADS, LEN), jnp.float32)
    result = jnp.clip(base - jnp.log(factor) + noise, 0.5, 11.5)
    return result.astype(jnp.bfloat16)


def block_levels(rng, extent, pieces, low, top_value):
    level, own = 1.0, jax.random.fold_in(rng, 6)
    for dim, parts in pieces:
        steps = jnp.exp(jax.random.uniform(jax.random.fold_in(own, dim), (parts,), jnp.float32, low / len(pieces), top_value / len(pieces)))
        level = level * jnp.repeat(steps, extent[dim] // parts).reshape([-1 if axis == dim else 1 for axis in range(len(extent))])
    return level


def centred(key, shape, spread, bound, shards=(), kind=jnp.bfloat16):
    values = jax.random.normal(key, shape, jnp.float32) * spread
    if len(shards) > 0:
        values = block_levels(key, shape, shards, -0.22, 0.18) * values
    return jnp.clip(values, min=-bound, max=bound).astype(kind)


def setup_inputs(seed: int = 0) -> dict:
    seeds = jax.random.split(jax.random.key(seed), 11)
    queries = centred(seeds[0], (BATCH, HEADS, LEN, HD), 1.0, 6.0, ((0, 16), (2, 32)))
    keys = centred(seeds[1], (BATCH, HEADS, LEN, HD), 1.0, 6.0, ((0, 16), (2, 32)))
    values = centred(seeds[2], (BATCH, HEADS, LEN, HD), 1.0, 6.0, ((0, 16), (2, 32)))
    input_gate = draw_input_gate(jax.random.fold_in(seeds[10], 71), 0)
    forget_gate = draw_forget_gate(jax.random.fold_in(seeds[10], 71), 0)
    start_memory = centred(seeds[5], (BATCH, HEADS, HD, HD), 1.0, 6.0, ((0, 16), (2, 32)), jnp.float32)
    start_norm = centred(seeds[6], (BATCH, HEADS, HD), 4.0, 24.0, ((0, 16), (2, 32)), jnp.float32)
    start_level = jnp.clip(2.0 + 2.0 * jax.random.uniform(seeds[7], (BATCH, HEADS), jnp.float32) ** block_levels(seeds[7], (BATCH, HEADS), ((0, 16),), -0.2, 0.2), 2.0, 4.0)
    head_gain = jnp.clip(1.0 + 0.18 * jax.random.normal(seeds[8], (HEADS, HD), jnp.float32), 0.1, 1.9)
    out_weight = centred(seeds[9], (MIX, D), MIX ** -0.5, 0.1875, ((1, 16),))
    return dict(queries=queries, keys=keys, values=values, input_gate=input_gate, forget_gate=forget_gate, start_memory=start_memory, start_norm=start_norm, start_level=start_level, head_gain=head_gain, out_weight=out_weight)


negative_fill = -1e30
highest = lax.Precision.HIGHEST


def cell_scan(query, key_in, value, input_pre, forget_pre, memory, normal, stabilizer):
    item_count, length, head_width = query.shape
    blocks = length // BLOCK
    factor = head_width ** -0.5

    def blocked(tensor):
        return jnp.moveaxis(tensor.reshape((item_count, blocks, BLOCK) + tensor.shape[2:]), 1, 0)

    inputs = (blocked(query), blocked(key_in), blocked(value),
              blocked(input_pre.astype(jnp.float32)), blocked(jax.nn.log_sigmoid(forget_pre.astype(jnp.float32))))
    causal = jnp.tril(jnp.ones((BLOCK, BLOCK), dtype=bool))

    def advance(state, block_data):
        memory, normal, stabilizer = state
        query_block, key_block, value_block, gate_in, gate_keep = block_data
        query_wide = query_block.astype(jnp.float32)
        key_wide = key_block.astype(jnp.float32)
        value_wide = value_block.astype(jnp.float32)
        scaled = query_wide * factor
        cumulative = jnp.cumsum(gate_keep, axis=-1)
        logits = jnp.where(causal, cumulative[:, :, None] - cumulative[:, None, :] + gate_in[:, None, :], negative_fill)
        carried = cumulative + stabilizer[:, None]
        running_max = jnp.maximum(carried, jnp.max(logits, axis=-1))
        raw = jnp.einsum('ptd,psd->pts', query_wide, key_wide, precision=highest) * factor
        scores = raw * jnp.exp(logits - running_max[..., None])
        rounded = scores.astype(jnp.bfloat16).astype(jnp.float32)
        carry_weight = jnp.exp(carried - running_max)
        numerator = jnp.einsum('pts,pse->pte', rounded, value_wide, precision=highest) + carry_weight[..., None] * jnp.einsum('ptd,pde->pte', scaled, memory, precision=highest)
        denominator = jnp.sum(scores, axis=-1) + carry_weight * jnp.einsum('ptd,pd->pt', scaled, normal, precision=highest)
        output = numerator / jnp.maximum(jnp.abs(denominator), 1.0)[..., None]
        block_total = cumulative[:, -1]
        weights_log = block_total[:, None] - cumulative + gate_in
        stabilizer_new = jnp.maximum(block_total + stabilizer, jnp.max(weights_log, axis=-1))
        weights = jnp.exp(weights_log - stabilizer_new[:, None])
        shrink = jnp.exp(block_total + stabilizer - stabilizer_new)
        weighted = key_wide * weights[..., None]
        packed = weighted.astype(jnp.bfloat16).astype(jnp.float32)
        memory_new = shrink[:, None, None] * memory + jnp.einsum('psd,pse->pde', packed, value_wide, precision=highest)
        normal_new = shrink[:, None] * normal + jnp.sum(weighted, axis=1)
        return (memory_new, normal_new, stabilizer_new), output

    start = (memory.astype(jnp.float32), normal.astype(jnp.float32), stabilizer.astype(jnp.float32))
    _, outputs = lax.scan(advance, start, inputs)
    return jnp.moveaxis(outputs, 0, 1).reshape(item_count, length, head_width).astype(jnp.bfloat16)


def normalize(hidden, gain):
    entries = hidden.astype(jnp.float32)
    return (entries * gain[:, None, :]).astype(jnp.bfloat16)


def reference(queries, keys, values, input_gate, forget_gate, start_memory, start_norm, start_level, head_gain, out_weight):
    batch, heads, length, head_width = queries.shape
    count = batch * heads
    hidden = cell_scan(queries.reshape(count, length, head_width), keys.reshape(count, length, head_width),
                       values.reshape(count, length, head_width), input_gate.reshape(count, length),
                       forget_gate.reshape(count, length), start_memory.reshape(count, head_width, head_width),
                       start_norm.reshape(count, head_width), start_level.reshape(count))
    normed = normalize(hidden.reshape(batch, heads, length, head_width), head_gain)
    flat_rows = normed.transpose(0, 2, 1, 3).reshape(batch * length, heads * head_width)
    mixed = jnp.dot(flat_rows, out_weight, preferred_element_type=jnp.float32).astype(jnp.bfloat16)
    return mixed.reshape(batch, length, out_weight.shape[1])
```

```python
import jax
import jax.numpy as jnp
from jax import lax
from jax.experimental import pallas as pl
from jax.experimental.pallas import tpu as pltpu
from jax.sharding import PartitionSpec as P

MESH = pl.DeviceIdType.MESH
F32 = jnp.float32
BF16 = jnp.bfloat16
S, H, T, D = 4, 8, 64, 128
NX, NZ, NY = 4, 8, 8
FACTOR = D**-0.5
NEG = -1e30
CH = 4
CROWS = 1024 // CH
LAST = 3 * CH + CH // 2


def nt(a, b):
    return lax.dot_general(a, b, (((1,), (1,)), ((), ())), preferred_element_type=F32)


def kernel(
    g_hbm, q_hbm, k_hbm, v_hbm, c_hbm, w_hbm, level, gain, out_hbm,
    qv, kv, vv, gv, cv, kx, vx, gx, cx, wall, a_loc, num_s, den_s, amx_s,
    wrow, esum, amax, kvs, nkv, cz_send, cz_recv, t_send, t_recv, tm_send, tm_recv,
    p_send, p_recv, pm_send, pm_recv, b_send, b_recv, bm_send, bm_recv, hid, ob,
    lsem, xin_s, xin_r, cz_s, cz_r, tz_s, tz_r, pz_s, pz_r, xo_s, xo_r,
    wy_s, wy_r, wd_s, wd_r, wo_s, wo_r, osem,
):
    sp = lax.axis_index("sp")
    dp = lax.axis_index("dp")
    x, z = lax.rem(sp, NX), lax.div(sp, NX)
    y, c = lax.div(dp, 2), lax.rem(dp, 2)

    def xdev(d):
        return {"sp": z * NX + lax.rem(x + d, NX), "dp": dp}

    def zdev(d):
        return {"sp": lax.rem(z + d, NZ) * NX + x, "dp": dp}

    def ydev(d):
        return {"sp": sp, "dp": lax.rem(y + d + NY, NY) * 2 + c}

    mate = {"sp": sp, "dp": y * 2 + (1 - c)}

    def remote(src, dst, ssem, rsem, dev):
        return pltpu.make_async_remote_copy(
            src_ref=src, dst_ref=dst, send_sem=ssem, recv_sem=rsem,
            device_id=dev, device_id_type=MESH,
        )

    loads = [
        pltpu.make_async_copy(g_hbm, gv, lsem.at[0]),
        pltpu.make_async_copy(k_hbm, kv, lsem.at[1]),
        pltpu.make_async_copy(v_hbm, vv, lsem.at[2]),
        pltpu.make_async_copy(w_hbm, wall.at[dp], lsem.at[3]),
        pltpu.make_async_copy(c_hbm, cv, lsem.at[4]),
        pltpu.make_async_copy(q_hbm, qv, lsem.at[5]),
        pltpu.make_async_copy(k_hbm.at[x], kx.at[x], lsem.at[6]),
        pltpu.make_async_copy(v_hbm.at[x], vx.at[x], lsem.at[7]),
        pltpu.make_async_copy(g_hbm.at[x], gx.at[x], lsem.at[8]),
        pltpu.make_async_copy(c_hbm.at[x], cx.at[x], lsem.at[9]),
    ]
    for load in loads:
        load.start()

    barrier = pltpu.get_barrier_semaphore()
    peers = [xdev(d) for d in range(1, NX)] + [zdev(d) for d in range(1, NZ)]
    peers += [ydev(1), ydev(-1), mate]
    for dev in peers:
        pl.semaphore_signal(barrier, inc=1, device_id=dev, device_id_type=MESH)

    rows64 = lax.broadcasted_iota(jnp.int32, (T, T), 0)
    cols64 = lax.broadcasted_iota(jnp.int32, (T, T), 1)
    upper = jnp.where(rows64 <= cols64, 1.0, 0.0).astype(F32)
    causal = rows64 >= cols64

    def gates(g):
        li = g[0:8, 0:T]
        f = g[8:16, 0:T]
        lf = jnp.minimum(f, 0.0) - jnp.log1p(jnp.exp(-jnp.abs(f)))
        b = jnp.dot(lf, upper, precision=lax.Precision.HIGHEST, preferred_element_type=F32)
        return li - b, b[:, T - 1 : T]

    for load in loads:
        load.wait()
    for j in range(S):
        a, _ = gates(gv[j])
        a_loc[8 * j : 8 * j + 8, :] = a

    pl.semaphore_wait(barrier, len(peers))

    def wpart(by, bc, part):
        return wall.at[by * 2 + bc, pl.ds(part * CROWS, CROWS), :]

    def part_of(side, n):
        return (n + side * CH // 2) % CH

    def wchunk(side, n):
        by = lax.rem(y - 1 - n // CH + 2 * NY, NY) if side == 0 else lax.rem(y + 1 + n // CH, NY)
        return wpart(by, c, part_of(side, n))

    def wsend(side, n):
        if n < CH:
            ref = wpart(y, c, part_of(side, n))
        else:
            ref = wchunk(side, n - CH)
        return remote(ref, ref, wy_s.at[side, n], wy_r.at[side, n], ydev(1 if side == 0 else -1))

    def xin(d):
        p = lax.rem(x + d, NX)
        dev = xdev(d)
        i = d - 1
        return [
            remote(gv.at[p], gx.at[x], xin_s.at[0, i], xin_r.at[0, i], dev),
            remote(kv.at[p], kx.at[x], xin_s.at[1, i], xin_r.at[1, i], dev),
            remote(vv.at[p], vx.at[x], xin_s.at[2, i], xin_r.at[2, i], dev),
            remote(cv.at[p], cx.at[x], xin_s.at[3, i], xin_r.at[3, i], dev),
        ]

    def xin_recv(d):
        p = lax.rem(x - d + NX, NX)
        dev = xdev(d)
        i = d - 1
        return [
            remote(gv.at[0], gx.at[p], xin_s.at[0, i], xin_r.at[0, i], dev),
            remote(kv.at[0], kx.at[p], xin_s.at[1, i], xin_r.at[1, i], dev),
            remote(vv.at[0], vx.at[p], xin_s.at[2, i], xin_r.at[2, i], dev),
            remote(cv.at[0], cx.at[p], xin_s.at[3, i], xin_r.at[3, i], dev),
        ]

    for d in (2, 1, 3):
        for copy in xin(d):
            copy.start()
    for n in range(CH):
        wsend(0, n).start()
        wsend(1, n).start()
    w_own = remote(wall.at[dp], wall.at[dp], wo_s.at[0], wo_r.at[0], mate)
    w_own.start()

    def serve(n):
        for side in (0, 1):
            ref = wchunk(side, n)
            remote(ref, ref, wy_s.at[side, n], wy_r.at[side, n], ydev(1)).wait_recv()
            if n + CH < LAST:
                wsend(side, n + CH).start()
            remote(ref, ref, wd_s.at[side, n], wd_r.at[side, n], mate).start()

    def intra(i, _):
        j, h = lax.div(i, H), lax.rem(i, H)
        arow = a_loc[pl.ds(i, 1), :]
        masked = jnp.where(causal, jnp.broadcast_to(arow, (T, T)), NEG)
        top = jnp.max(masked, axis=1, keepdims=True)
        weight = jnp.exp(masked - top)
        scores = nt(qv[j, h], kv[j, h]) * FACTOR * weight
        den_s[i] = jnp.broadcast_to(jnp.sum(scores, axis=1, keepdims=True), (T, D))
        amx_s[i] = jnp.broadcast_to(top, (T, D))
        num_s[i] = jnp.dot(scores.astype(BF16), vv[j, h], preferred_element_type=F32)
        return 0

    def pairs(fn, count):
        def body(i, _):
            for u in range(4):
                fn(i * 4 + u, 0)
            return 0

        lax.fori_loop(0, count // 4, body, 0)

    pairs(intra, S * H)

    def block_states(p):
        a, e = gates(gx[p])
        am = jnp.max(a, axis=1, keepdims=True)
        esum[p] = jnp.broadcast_to(e, (H, D))
        amax[p] = jnp.broadcast_to(am, (H, D))
        wrow[...] = jnp.exp(a - am)

        def one(h, _):
            w = wrow[pl.ds(h, 1), :]
            vt = vx[p, h].astype(F32).T
            hi = w.astype(BF16)
            lo = (w - hi.astype(F32)).astype(BF16)
            rid = lax.broadcasted_iota(jnp.int32, (16, T), 0)
            extra = jnp.where(
                rid == 0,
                jnp.broadcast_to(hi.astype(F32), (16, T)),
                jnp.where(rid == 1, jnp.broadcast_to(lo.astype(F32), (16, T)), 0.0),
            )
            lhs = jnp.concatenate([(vt * w).astype(BF16), extra.astype(BF16)], axis=0)
            st = jnp.dot(lhs, kx[p, h], preferred_element_type=F32)
            kvs[p, h] = st[0:D]
            nkv[p, pl.ds(h, 1), :] = st[D : D + 1] + st[D + 1 : D + 2]
            return 0

        pairs(one, H)

    block_states(x)
    serve(0)
    for count, d in enumerate((1, 3, 2)):
        for copy in xin_recv(d):
            copy.wait_recv()
        block_states(lax.rem(x - d + NX, NX))
        serve(1 + count)

    for i in range(NX):
        for h in range(H):
            cz_send[h, 4 * i : 4 * i + 4, :] = cx[i, 4 * h : 4 * h + 4, :]

    shift = []
    before = jnp.zeros((H, D), F32)
    top = None
    for i in range(NX):
        a = amax[i] - before
        shift.append(a)
        top = a if top is None else jnp.maximum(top, a)
        before = before + esum[i]
    scale = [jnp.exp(a - top) for a in shift]
    ntot = sum(scale[i] * nkv[i] for i in range(NX))
    n0 = sum(gx[i, 16:24, :] for i in range(NX))
    for h in range(H):
        tm_send[h, 0:1, :] = ntot[h : h + 1]
        tm_send[h, 1:2, :] = before[h : h + 1]
        tm_send[h, 2:3, :] = top[h : h + 1]
        tm_send[h, 3:4, :] = n0[h : h + 1]
        t_send[h] = sum(scale[i][h : h + 1] * kvs[i, h] for i in range(NX)).astype(BF16)

    def tz(d):
        p = lax.rem(z + d, NZ)
        dev = zdev(d)
        i = d - 1
        return [
            remote(cz_send.at[p], cz_recv.at[z], tz_s.at[2, i], tz_r.at[2, i], dev),
            remote(tm_send.at[p], tm_recv.at[z], tz_s.at[0, i], tz_r.at[0, i], dev),
            remote(t_send.at[p], t_recv.at[z], tz_s.at[1, i], tz_r.at[1, i], dev),
        ]

    def tz_recv(d):
        p = lax.rem(z - d + NZ, NZ)
        dev = zdev(d)
        i = d - 1
        return [
            remote(cz_send.at[0], cz_recv.at[p], tz_s.at[2, i], tz_r.at[2, i], dev),
            remote(tm_send.at[0], tm_recv.at[p], tz_s.at[0, i], tz_r.at[0, i], dev),
            remote(t_send.at[0], t_recv.at[p], tz_s.at[1, i], tz_r.at[1, i], dev),
        ]

    for d in (4, 3, 5, 2, 6, 1, 7):
        for copy in tz(d):
            copy.start()
    t_recv[z] = t_send[z]
    tm_recv[z] = tm_send[z]
    cz_recv[z] = cz_send[z]
    serve(4)
    for d in (1, 7, 2, 6, 3, 5, 4):
        for copy in tz_recv(d):
            copy.wait_recv()

    m = jnp.full((1, D), level[x, z], F32)
    nrow = sum(tm_recv[i, 3:4, :] for i in range(NZ))
    state = jnp.concatenate([cz_recv[i] for i in range(NZ)], axis=0).T
    for i in range(NZ):
        p_send[i] = state.astype(BF16)
        pm_send[i, 0:1, :] = nrow
        pm_send[i, 1:2, :] = m
        am = tm_recv[i, 2:3, :]
        hi = jnp.maximum(m, am)
        keep, add = jnp.exp(m - hi), jnp.exp(am - hi)
        state = keep * state + add * t_recv[i].astype(F32)
        nrow = keep * nrow + add * tm_recv[i, 0:1, :]
        m = tm_recv[i, 1:2, :] + hi

    def pz(d):
        p = lax.rem(z + d, NZ)
        dev = zdev(d)
        i = d - 1
        return [
            remote(pm_send.at[p], pm_recv.at[z], pz_s.at[0, i], pz_r.at[0, i], dev),
            remote(p_send.at[p], p_recv.at[z], pz_s.at[1, i], pz_r.at[1, i], dev),
        ]

    def pz_recv(d):
        p = lax.rem(z - d + NZ, NZ)
        dev = zdev(d)
        i = d - 1
        return [
            remote(pm_send.at[0], pm_recv.at[p], pz_s.at[0, i], pz_r.at[0, i], dev),
            remote(p_send.at[0], p_recv.at[p], pz_s.at[1, i], pz_r.at[1, i], dev),
        ]

    for d in (4, 3, 5, 2, 6, 1, 7):
        for copy in pz(d):
            copy.start()
    p_recv[z] = p_send[z]
    pm_recv[z] = pm_send[z]
    serve(5)
    serve(6)
    for d in (1, 7, 2, 6, 3, 5, 4):
        for copy in pz_recv(d):
            copy.wait_recv()
    serve(7)

    for h in range(H):
        state = p_recv[h].astype(F32)
        nrow = pm_recv[h, 0:1, :]
        m = pm_recv[h, 1:2, :]
        for i in range(NX):
            b_send[i, h] = state.astype(BF16)
            bm_send[i, h : h + 1, :] = nrow
            bm_send[i, H + h : H + h + 1, :] = m
            if i < NX - 1:
                am = amax[i, h : h + 1, :]
                hi = jnp.maximum(m, am)
                keep, add = jnp.exp(m - hi), jnp.exp(am - hi)
                state = keep * state + add * kvs[i, h]
                nrow = keep * nrow + add * nkv[i, h : h + 1, :]
                m = esum[i, h : h + 1, :] + hi

    def xo(d):
        p = lax.rem(x + d, NX)
        dev = xdev(d)
        i = d - 1
        return [
            remote(bm_send.at[p], bm_recv.at[x], xo_s.at[0, i], xo_r.at[0, i], dev),
            remote(b_send.at[p], b_recv.at[x], xo_s.at[1, i], xo_r.at[1, i], dev),
        ]

    def xo_recv(d):
        p = lax.rem(x - d + NX, NX)
        dev = xdev(d)
        i = d - 1
        return [
            remote(bm_send.at[0], bm_recv.at[p], xo_s.at[0, i], xo_r.at[0, i], dev),
            remote(b_send.at[0], b_recv.at[p], xo_s.at[1, i], xo_r.at[1, i], dev),
        ]

    for d in (2, 1, 3):
        for copy in xo(d):
            copy.start()
    b_recv[x] = b_send[x]
    bm_recv[x] = bm_send[x]

    def finish(j):
        def one(h, _):
            i = j * H + h
            q = qv[j, h]
            nrow = bm_recv[j, pl.ds(h, 1), :]
            m = bm_recv[j, pl.ds(H + h, 1), :]
            qc = nt(q, b_recv[j, h])
            qn = jnp.sum(q.astype(F32) * nrow, axis=1, keepdims=True)
            a = amx_s[i]
            hi = jnp.maximum(a, m)
            keep, add = jnp.exp(m - hi) * FACTOR, jnp.exp(a - hi)
            den = add * den_s[i] + keep * qn
            num = add * num_s[i] + keep * qc
            o = (num / jnp.maximum(jnp.abs(den), 1.0)).astype(BF16)
            normed = (o.astype(F32) * gain[pl.ds(h, 1), :]).astype(BF16)
            hid[pl.ds(pl.multiple_of(j * T, T), T), pl.ds(pl.multiple_of(h * D, D), D)] = normed
            return 0

        pairs(one, H)

    finish(x)
    serve(8)
    for count, d in enumerate((1, 3, 2)):
        for copy in xo_recv(d):
            copy.wait_recv()
        finish(lax.rem(x - d + NX, NX))
        serve(9 + count)
    serve(12)
    serve(13)

    remote(wall.at[dp], wall.at[y * 2 + 1 - c], wo_s.at[0], wo_r.at[0], mate).wait_recv()
    for n in range(LAST):
        for side in (0, 1):
            ref = wchunk(side, n)
            remote(ref, ref, wd_s.at[side, n], wd_r.at[side, n], mate).wait_recv()

    def project(i, _):
        cols = pl.ds(pl.multiple_of(i * 256, 256), 256)
        ob[i] = jnp.dot(hid[...], wall[i], preferred_element_type=F32).astype(BF16)
        pltpu.make_async_copy(ob.at[i], out_hbm.at[:, cols], osem.at[i]).start()
        return 0

    lax.fori_loop(0, 2 * NY, project, 0)

    for i in range(2 * NY):
        pltpu.make_async_copy(ob.at[i], out_hbm.at[:, 256 * i : 256 * i + 256], osem.at[i]).wait()
    for d in range(1, NX):
        for copy in xin(d) + xo(d):
            copy.wait_send()
    for d in range(1, NZ):
        for copy in tz(d) + pz(d):
            copy.wait_send()
    w_own.wait_send()
    for n in range(LAST):
        for side in (0, 1):
            wsend(side, n).wait_send()
            ref = wchunk(side, n)
            remote(ref, ref, wd_s.at[side, n], wd_r.at[side, n], mate).wait_send()


def on_device(queries, keys, values, input_gate, forget_gate, start_memory, start_norm, start_level, head_gain, out_weight):
    sp = lax.axis_index("sp")
    lane = lax.broadcasted_iota(jnp.int32, (S, H, D), 2)
    spread = jnp.where(lane // 4 == sp, jnp.tile(start_norm, (1, 1, D // 4)), 0.0)
    pad = ((0, 0), (0, 0), (0, D - T))
    g = jnp.concatenate(
        [jnp.pad(input_gate.astype(F32), pad), jnp.pad(forget_gate.astype(F32), pad), spread], axis=1
    )
    dma, vmem = pltpu.SemaphoreType.DMA, pltpu.VMEM
    anyspec = pl.BlockSpec(memory_space=pl.ANY)
    out = pl.pallas_call(
        kernel,
        out_shape=jax.ShapeDtypeStruct((S * T, 4096), BF16),
        in_specs=[anyspec] * 6
        + [pl.BlockSpec(memory_space=pltpu.SMEM), pl.BlockSpec(memory_space=pltpu.VMEM)],
        out_specs=anyspec,
        scratch_shapes=[
            vmem((S, H, T, D), BF16), vmem((S, H, T, D), BF16), vmem((S, H, T, D), BF16),
            vmem((S, 24, D), F32), vmem((S, 32, D), F32),
            vmem((NX, H, T, D), BF16), vmem((NX, H, T, D), BF16),
            vmem((NX, 24, D), F32), vmem((NX, 32, D), F32),
            vmem((2 * NY, 1024, 256), BF16),
            vmem((S * H, T), F32),
            vmem((S * H, T, D), F32), vmem((S * H, T, D), F32), vmem((S * H, T, D), F32),
            vmem((H, T), F32), vmem((NX, H, D), F32), vmem((NX, H, D), F32),
            vmem((NX, H, D, D), F32), vmem((NX, H, D), F32),
            vmem((H, 16, D), F32), vmem((NZ, 16, D), F32),
            vmem((H, D, D), BF16), vmem((NZ, D, D), BF16),
            vmem((H, 8, D), F32), vmem((NZ, 8, D), F32),
            vmem((NZ, D, D), BF16), vmem((H, D, D), BF16),
            vmem((NZ, 8, D), F32), vmem((H, 8, D), F32),
            vmem((NX, H, D, D), BF16), vmem((S, H, D, D), BF16),
            vmem((NX, 16, D), F32), vmem((S, 16, D), F32),
            vmem((S * T, H * D), BF16),
            vmem((2 * NY, S * T, 256), BF16),
            dma((10,)),
            dma((4, 3)), dma((4, 3)),
            dma((1,)), dma((1,)),
            dma((3, 7)), dma((3, 7)),
            dma((2, 7)), dma((2, 7)),
            dma((2, 3)), dma((2, 3)),
            dma((2, LAST)), dma((2, LAST)), dma((2, LAST)), dma((2, LAST)),
            dma((1,)), dma((1,)), dma((2 * NY,)),
        ],
        compiler_params=pltpu.CompilerParams(
            collective_id=0, has_side_effects=True, vmem_limit_bytes=48 * 1024 * 1024
        ),
        name="cell_layer",
    )(
        g, queries, keys, values, start_memory.reshape(S, 32, D), out_weight, start_level, head_gain
    )
    return out.reshape(S, T, 4096)


def solution(mesh):
    return jax.shard_map(
        on_device,
        mesh=mesh,
        in_specs=(
            P("dp", None, "sp", None),
            P("dp", None, "sp", None),
            P("dp", None, "sp", None),
            P("dp", None, "sp"),
            P("dp", None, "sp"),
            P("dp", None, "sp", None),
            P("dp", None, "sp"),
            P("dp", None),
            P(),
            P(None, "dp"),
        ),
        out_specs=P("dp", "sp", None),
        check_vma=False,
    )
```

```python
import jax
import jax.numpy as jnp
from jax import lax
from jax.experimental import pallas as pl
from jax.experimental.pallas import tpu as pltpu
from jax.sharding import PartitionSpec as P

MESH = pl.DeviceIdType.MESH
F32 = jnp.float32
BF16 = jnp.bfloat16
S, H, T, D = 4, 8, 64, 128
NX, NZ, NY = 4, 8, 8
FACTOR = D**-0.5
NEG = -1e30
G = 4
HG = H // G
CH = 4
CROWS = 1024 // CH
LAST = 3 * CH + CH // 2


def nt(a, b):
    return lax.dot_general(a, b, (((1,), (1,)), ((), ())), preferred_element_type=F32)


def rev(i):
    return i % 2 * 4 + i // 2 % 2 * 2 + i // 4


def kernel(
    i_hbm, f_hbm, q_hbm, k_hbm, v_hbm, c_hbm, n_hbm, w_hbm, level_hbm, gain_hbm, out,
    qv, kv, vv, iv, fv, cv, nv, kx, vx, ix, fx, cx, nx, level, gain, wall, a_loc, num_s, den_s, amx_s,
    wrow, esum, amax, kvs, nkv, turn, cz_send, cz_recv, t_send, t_recv, tm_send, tm_recv,
    p_send, p_recv, pm_send, pm_recv, b_send, b_recv, bm_send, bm_recv, hid,
    lsem, xs_s, xs_r, xk_s, xk_r, tz_s, tz_r, pz_s, pz_r, xo_s, xo_r,
    wy_s, wy_r, wd_s, wd_r, wo_s, wo_r,
):
    sp = lax.axis_index("sp")
    dp = lax.axis_index("dp")
    x, z = lax.rem(sp, NX), lax.div(sp, NX)
    y, c = lax.div(dp, 2), lax.rem(dp, 2)
    mine = lax.rem(z, 2) * 4 + lax.rem(lax.div(z, 2), 2) * 2 + lax.div(z, 4)

    def xdev(d):
        return {"sp": z * NX + lax.rem(x + d, NX), "dp": dp}

    def zat(p):
        return {"sp": p * NX + x, "dp": dp}

    def ydev(d):
        return {"sp": sp, "dp": lax.rem(y + d + NY, NY) * 2 + c}

    mate = {"sp": sp, "dp": y * 2 + (1 - c)}

    def remote(src, dst, ssem, rsem, dev):
        return pltpu.make_async_remote_copy(
            src_ref=src, dst_ref=dst, send_sem=ssem, recv_sem=rsem,
            device_id=dev, device_id_type=MESH,
        )

    pairs_in = [
        (i_hbm, iv), (f_hbm, fv), (k_hbm, kv), (v_hbm, vv), (w_hbm, wall.at[dp]), (c_hbm, cv), (n_hbm, nv),
        (q_hbm, qv), (k_hbm.at[x], kx.at[x]), (v_hbm.at[x], vx.at[x]), (i_hbm.at[x], ix.at[x]),
        (f_hbm.at[x], fx.at[x]), (c_hbm.at[x], cx.at[x]), (n_hbm.at[x], nx.at[x]),
        (level_hbm, level), (gain_hbm, gain),
    ]
    loads = [pltpu.make_async_copy(src, dst, lsem.at[i]) for i, (src, dst) in enumerate(pairs_in)]
    for load in loads:
        load.start()

    barrier = pltpu.get_barrier_semaphore()
    peers = [xdev(d) for d in range(1, NX)] + [zat(lax.rem(z + d, NZ)) for d in range(1, NZ)]
    peers += [ydev(1), ydev(-1), mate]
    for dev in peers:
        pl.semaphore_signal(barrier, inc=1, device_id=dev, device_id_type=MESH)

    rows64 = lax.broadcasted_iota(jnp.int32, (T, T), 0)
    cols64 = lax.broadcasted_iota(jnp.int32, (T, T), 1)
    upper = jnp.where(rows64 <= cols64, 1.0, 0.0).astype(F32)
    causal = rows64 >= cols64

    def gates(li, f):
        li, f = li.astype(F32), f.astype(F32)
        lf = jnp.minimum(f, 0.0) - jnp.log1p(jnp.exp(-jnp.abs(f)))
        b = jnp.dot(lf, upper, precision=lax.Precision.HIGHEST, preferred_element_type=F32)
        return li - b, b[:, T - 1 : T]

    with jax.named_scope("loads"):
        for load in loads:
            load.wait()
    for j in range(S):
        a, _ = gates(iv[j], fv[j])
        a_loc[8 * j : 8 * j + 8, :] = a

    def block_gates(p):
        a, e = gates(ix[p], fx[p])
        am = jnp.max(a, axis=1, keepdims=True)
        esum[p] = jnp.broadcast_to(e, (H, D))
        amax[p] = jnp.broadcast_to(am, (H, D))
        wrow[p] = jnp.exp(a - am)

    block_gates(x)

    with jax.named_scope("barrier"):
        pl.semaphore_wait(barrier, len(peers))

    def wpart(by, bc, part):
        return wall.at[by * 2 + bc, pl.ds(part * CROWS, CROWS), :]

    def part_of(side, n):
        return (n + side * CH // 2) % CH

    def wchunk(side, n):
        by = lax.rem(y - 1 - n // CH + 2 * NY, NY) if side == 0 else lax.rem(y + 1 + n // CH, NY)
        return wpart(by, c, part_of(side, n))

    def wsend(side, n):
        if n < CH:
            ref = wpart(y, c, part_of(side, n))
        else:
            ref = wchunk(side, n - CH)
        return remote(ref, ref, wy_s.at[side, n], wy_r.at[side, n], ydev(1 if side == 0 else -1))

    def serve(n):
        for side in (0, 1):
            ref = wchunk(side, n)
            with jax.named_scope(f"serve{n}"):
                remote(ref, ref, wy_s.at[side, n], wy_r.at[side, n], ydev(1)).wait_recv()
            if n + CH < LAST:
                wsend(side, n + CH).start()
            remote(ref, ref, wd_s.at[side, n], wd_r.at[side, n], mate).start()

    def xsmall(d, here):
        p = lax.rem(x + d, NX)
        slot = x if here else lax.rem(x - d + NX, NX)
        return [
            remote(src.at[p], dst.at[slot], xs_s.at[k, d - 1], xs_r.at[k, d - 1], xdev(d))
            for k, (src, dst) in enumerate([(iv, ix), (fv, fx), (cv, cx), (nv, nx)])
        ]

    def xkeys(d, g, here):
        p = lax.rem(x + d, NX)
        slot = x if here else lax.rem(x - d + NX, NX)
        heads = pl.ds(g * HG, HG)
        return [
            remote(
                src.at[p, heads], dst.at[slot, heads],
                xk_s.at[k, g, d - 1], xk_r.at[k, g, d - 1], xdev(d),
            )
            for k, (src, dst) in enumerate([(kv, kx), (vv, vx)])
        ]

    for d in (2, 1, 3):
        for copy in xsmall(d, True)[:2]:
            copy.start()
    for g in range(G):
        for d in (2, 1, 3):
            for copy in xkeys(d, g, True):
                copy.start()
        if g == 0:
            for d in (2, 1, 3):
                for copy in xsmall(d, True)[2:]:
                    copy.start()
    for n in range(CH):
        wsend(0, n).start()
        wsend(1, n).start()
    w_own = remote(wall.at[dp], wall.at[dp], wo_s.at[0], wo_r.at[0], mate)
    w_own.start()

    def intra(i):
        j, h = lax.div(i, H), lax.rem(i, H)
        arow = a_loc[pl.ds(i, 1), :]
        masked = jnp.where(causal, jnp.broadcast_to(arow, (T, T)), NEG)
        top = jnp.max(masked, axis=1, keepdims=True)
        weight = jnp.exp(masked - top)
        scores = nt(qv[j, h], kv[j, h]) * FACTOR * weight
        den_s[i] = jnp.broadcast_to(jnp.sum(scores, axis=1, keepdims=True), (T, D))
        amx_s[i] = jnp.broadcast_to(top, (T, D))
        num_s[i] = jnp.dot(scores.astype(BF16), vv[j, h], preferred_element_type=F32)

    def inner(part):
        def body(i, _):
            for u in range(4):
                intra(part * 8 + i * 4 + u)
            return 0

        with jax.named_scope("intra"):
            lax.fori_loop(0, 2, body, 0)

    def state(p, h):
        w = wrow[p, pl.ds(h, 1), :]
        vt = vx[p, h].astype(F32).T
        hi = w.astype(BF16)
        lo = (w - hi.astype(F32)).astype(BF16)
        rid = lax.broadcasted_iota(jnp.int32, (16, T), 0)
        extra = jnp.where(
            rid == 0,
            jnp.broadcast_to(hi.astype(F32), (16, T)),
            jnp.where(rid == 1, jnp.broadcast_to(lo.astype(F32), (16, T)), 0.0),
        )
        lhs = jnp.concatenate([(vt * w).astype(BF16), extra.astype(BF16)], axis=0)
        st = jnp.dot(lhs, kx[p, h], preferred_element_type=F32)
        kvs[p, h] = st[0:D]
        nkv[p, pl.ds(h, 1), :] = st[D : D + 1] + st[D + 1 : D + 2]

    def states(p, g):
        with jax.named_scope("states"):
            for u in range(HG):
                state(p, g * HG + u)

    inner(0)

    def own(i, _):
        for u in range(4):
            state(x, i * 4 + u)
        return 0

    lax.fori_loop(0, 2, own, 0)
    inner(1)
    with jax.named_scope("xgates"):
        for d in (1, 3, 2):
            for copy in xsmall(d, False)[:2]:
                copy.wait_recv()
            block_gates(lax.rem(x - d + NX, NX))

    shift = []
    before = jnp.zeros((H, D), F32)
    top = None
    for i in range(NX):
        a = amax[i] - before
        shift.append(a)
        top = a if top is None else jnp.maximum(top, a)
        before = before + esum[i]
    scale = [jnp.exp(a - top) for a in shift]

    def tz(h):
        p = rev(h)
        d = lax.rem(p - z + NZ, NZ)
        return d, [
            remote(tm_send.at[h], tm_recv.at[z], tz_s.at[0, d], tz_r.at[0, d], zat(p)),
            remote(t_send.at[h], t_recv.at[z], tz_s.at[1, d], tz_r.at[1, d], zat(p)),
        ]

    def total(g):
        for d in (1, 3, 2):
            with jax.named_scope(f"xin{g}{d}"):
                for copy in xkeys(d, g, False):
                    copy.wait_recv()
            states(lax.rem(x - d + NX, NX), g)
        for h in range(g * HG, g * HG + HG):
            ntot = sum(scale[i][h : h + 1] * nkv[i, h : h + 1, :] for i in range(NX))
            t_send[h] = sum(scale[i][h : h + 1] * kvs[i, h] for i in range(NX)).astype(BF16)
            tm_send[h, 0:1, :] = ntot
            tm_send[h, 1:2, :] = before[h : h + 1]
            tm_send[h, 2:3, :] = top[h : h + 1]
            tm_send[h, 3:4, :] = nfirst[h : h + 1]
        for h in range(g * HG, g * HG + HG):
            d, copies = tz(h)

            @pl.when(d != 0)
            def _():
                for copy in copies:
                    copy.start()

    def cz(d):
        p = lax.rem(z + d, NZ)
        h = lax.rem(p, 2) * 4 + lax.rem(lax.div(p, 2), 2) * 2 + lax.div(p, 4)
        return remote(cz_send.at[h], cz_recv.at[z], tz_s.at[2, d], tz_r.at[2, d], zat(p))

    with jax.named_scope("xstart"):
        for d in (1, 3, 2):
            for copy in xsmall(d, False)[2:]:
                copy.wait_recv()
    for i in range(NX):
        turn[4 * i : 4 * i + 4, 0:H] = nx[i]
        for h in range(H):
            cz_send[h, 4 * i : 4 * i + 4, :] = cx[i, 4 * h : 4 * h + 4, :]
    first_lanes = lax.broadcasted_iota(jnp.int32, (H, D), 1) < 4 * NX
    nfirst = jnp.where(first_lanes, turn[...].T[0:H], 0.0)
    for d in (4, 3, 5, 2, 6, 1, 7):
        cz(d).start()

    def pz(d):
        p = lax.rem(z + d, NZ)
        return [
            remote(pm_send.at[p], pm_recv.at[mine], pz_s.at[0, d], pz_r.at[0, d], zat(p)),
            remote(p_send.at[p], p_recv.at[mine], pz_s.at[1, d], pz_r.at[1, d], zat(p)),
        ]

    def scan(g):
        @pl.when(lax.div(mine, HG) == g)
        def _():
            with jax.named_scope(f"zin{g}"):
                for d in range(1, NZ):
                    p = lax.rem(z - d + NZ, NZ)
                    for src, dst, k in ((tm_send, tm_recv, 0), (t_send, t_recv, 1), (cz_send, cz_recv, 2)):
                        remote(src.at[0], dst.at[p], tz_s.at[k, d], tz_r.at[k, d], zat(p)).wait_recv()
            with jax.named_scope("scan"):
                t_recv[z] = t_send[mine]
                tm_recv[z] = tm_send[mine]
                cz_recv[z] = cz_send[mine]
                lanes = lax.broadcasted_iota(jnp.int32, (1, H), 1)
                m = jnp.sum(jnp.where(lanes == mine, level[pl.ds(x, 1), :], 0.0), axis=1, keepdims=True)
                m = jnp.broadcast_to(m, (1, D))
                nrow = tm_recv[0, 3:4, :]
                for i in range(1, NZ):
                    nrow = nrow + pltpu.roll(tm_recv[i, 3:4, :], 4 * NX * i, 1)
                cur = jnp.concatenate([cz_recv[i] for i in range(NZ)], axis=0).T
                for i in range(NZ):
                    p_send[i] = cur.astype(BF16)
                    pm_send[i, 0:1, :] = nrow
                    pm_send[i, 1:2, :] = m
                    am = tm_recv[i, 2:3, :]
                    hi = jnp.maximum(m, am)
                    keep, add = jnp.exp(m - hi), jnp.exp(am - hi)
                    cur = keep * cur + add * t_recv[i].astype(F32)
                    nrow = keep * nrow + add * tm_recv[i, 0:1, :]
                    m = tm_recv[i, 1:2, :] + hi
                for d in (4, 3, 5, 2, 6, 1, 7):
                    for copy in pz(d):
                        copy.start()
                p_recv[mine] = p_send[z]
                pm_recv[mine] = pm_send[z]

    def xo(d, g, here):
        p = lax.rem(x + d, NX)
        slot = x if here else lax.rem(x - d + NX, NX)
        heads = pl.ds(g * HG, HG)
        return [
            remote(
                bm_send.at[p, g], bm_recv.at[slot, g],
                xo_s.at[0, g, d - 1], xo_r.at[0, g, d - 1], xdev(d),
            ),
            remote(
                b_send.at[p, heads], b_recv.at[slot, heads],
                xo_s.at[1, g, d - 1], xo_r.at[1, g, d - 1], xdev(d),
            ),
        ]

    def spread(g):
        for h in range(g * HG, g * HG + HG):
            p = rev(h)
            d = lax.rem(z - p + NZ, NZ)

            @pl.when(d != 0)
            def _():
                with jax.named_scope(f"zout{g}"):
                    for src, dst, k in ((pm_send, pm_recv, 0), (p_send, p_recv, 1)):
                        remote(src.at[0], dst.at[h], pz_s.at[k, d], pz_r.at[k, d], zat(p)).wait_recv()

        for u in range(HG):
            h = g * HG + u
            cur = p_recv[h].astype(F32)
            nrow = pm_recv[h, 0:1, :]
            m = pm_recv[h, 1:2, :]
            for i in range(NX):
                b_send[i, h] = cur.astype(BF16)
                bm_send[i, g, 2 * u : 2 * u + 1, :] = nrow
                bm_send[i, g, 2 * u + 1 : 2 * u + 2, :] = m
                if i < NX - 1:
                    am = amax[i, h : h + 1, :]
                    hi = jnp.maximum(m, am)
                    keep, add = jnp.exp(m - hi), jnp.exp(am - hi)
                    cur = keep * cur + add * kvs[i, h]
                    nrow = keep * nrow + add * nkv[i, h : h + 1, :]
                    m = esum[i, h : h + 1, :] + hi
        for d in (2, 1, 3):
            for copy in xo(d, g, True):
                copy.start()
        heads = pl.ds(g * HG, HG)
        b_recv[x, heads] = b_send[x, heads]
        bm_recv[x, g] = bm_send[x, g]

    def finish_one(j, g):
        for u in range(HG):
            h = g * HG + u
            i = j * H + h
            q = qv[j, h]
            nrow = bm_recv[j, g, 2 * u : 2 * u + 1, :]
            m = bm_recv[j, g, 2 * u + 1 : 2 * u + 2, :]
            qc = nt(q, b_recv[j, h])
            qn = jnp.sum(q.astype(F32) * nrow, axis=1, keepdims=True)
            a = amx_s[i]
            hi = jnp.maximum(a, m)
            keep, add = jnp.exp(m - hi) * FACTOR, jnp.exp(a - hi)
            den = add * den_s[i] + keep * qn
            num = add * num_s[i] + keep * qc
            o = (num / jnp.maximum(jnp.abs(den), 1.0)).astype(BF16)
            normed = (o.astype(F32) * gain[h : h + 1, :]).astype(BF16)
            hid[pl.ds(pl.multiple_of(j * T, T), T), h * D : h * D + D] = normed

    def finish(g):
        with jax.named_scope("finish"):
            finish_one(x, g)
        for d in (1, 3, 2):
            with jax.named_scope(f"xout{g}{d}"):
                for copy in xo(d, g, False):
                    copy.wait_recv()
            with jax.named_scope("finish"):
                finish_one(lax.rem(x - d + NX, NX), g)

    def project(dist):
        def body(i, _):
            t = lax.div(i, 2)
            away = lax.div(t + 1, 2) * (1 - 2 * lax.rem(t, 2))
            block = lax.rem(y + away + NY, NY) * 2 + lax.rem(i, 2)
            cols = pl.ds(pl.multiple_of(block * 256, 256), 256)
            out[:, cols] = jnp.dot(hid[...], wall[block], preferred_element_type=F32).astype(BF16)
            return 0

        if dist == 0:
            low, high = 0, 2
            remote(wall.at[dp], wall.at[y * 2 + 1 - c], wo_s.at[0], wo_r.at[0], mate).wait_recv()
        else:
            low, high = 4 * dist - 2, min(4 * dist + 2, 4 * NY // 2)
            with jax.named_scope(f"mate{dist}"):
                for n in range(CH * dist - CH, min(CH * dist, LAST)):
                    for side in (0, 1):
                        ref = wchunk(side, n)
                        remote(ref, ref, wd_s.at[side, n], wd_r.at[side, n], mate).wait_recv()
        with jax.named_scope("project"):
            lax.fori_loop(low, high, body, 0)

    total(0)
    serve(0)
    inner(2)
    total(1)
    serve(1)
    inner(3)
    scan(0)
    total(2)
    serve(2)
    scan(1)
    serve(3)
    total(3)
    spread(0)
    scan(2)
    serve(4)
    spread(1)
    scan(3)
    serve(5)
    finish(0)
    spread(2)
    serve(6)
    finish(1)
    spread(3)
    serve(7)
    finish(2)
    serve(8)
    finish(3)
    project(0)
    project(1)
    serve(9)
    project(2)
    serve(10)
    serve(11)
    project(3)
    serve(12)
    serve(13)
    project(4)

    for d in range(1, NX):
        for copy in xsmall(d, True):
            copy.wait_send()
        for g in range(G):
            for copy in xkeys(d, g, True) + xo(d, g, True):
                copy.wait_send()
    for d in range(1, NZ):
        p = lax.rem(z + d, NZ)
        for src, dst, k in ((tm_send, tm_recv, 0), (t_send, t_recv, 1), (cz_send, cz_recv, 2)):
            remote(src.at[0], dst.at[0], tz_s.at[k, d], tz_r.at[k, d], zat(p)).wait_send()
        for copy in pz(d):
            copy.wait_send()
    w_own.wait_send()
    for n in range(LAST):
        for side in (0, 1):
            wsend(side, n).wait_send()
            ref = wchunk(side, n)
            remote(ref, ref, wd_s.at[side, n], wd_r.at[side, n], mate).wait_send()


def on_device(queries, keys, values, input_gate, forget_gate, start_memory, start_norm, start_level, head_gain, out_weight):
    arrays = (
        input_gate, forget_gate, queries, keys, values, start_memory.reshape(S, 32, D),
        jnp.transpose(start_norm, (0, 2, 1)), out_weight, start_level, head_gain,
    )
    dma, vmem = pltpu.SemaphoreType.DMA, pltpu.VMEM
    out = pl.pallas_call(
        kernel,
        out_shape=pltpu.VMEM((S * T, 4096), BF16),
        in_specs=[pl.BlockSpec(memory_space=pltpu.HBM)] * len(arrays),
        out_specs=pl.BlockSpec(memory_space=pltpu.VMEM),
        scratch_shapes=[
            vmem((S, H, T, D), BF16), vmem((S, H, T, D), BF16), vmem((S, H, T, D), BF16),
            vmem((S, H, T), BF16), vmem((S, H, T), BF16), vmem((S, 32, D), F32), vmem((S, 4, H), F32),
            vmem((NX, H, T, D), BF16), vmem((NX, H, T, D), BF16),
            vmem((NX, H, T), BF16), vmem((NX, H, T), BF16), vmem((NX, 32, D), F32), vmem((NX, 4, H), F32),
            vmem((S, H), F32), vmem((H, D), F32),
            vmem((2 * NY, 1024, 256), BF16),
            vmem((S * H, T), F32),
            vmem((S * H, T, D), F32), vmem((S * H, T, D), F32), vmem((S * H, T, D), F32),
            vmem((NX, H, T), F32), vmem((NX, H, D), F32), vmem((NX, H, D), F32),
            vmem((NX, H, D, D), F32), vmem((NX, H, D), F32), vmem((D, D), F32),
            vmem((H, 16, D), F32), vmem((NZ, 16, D), F32),
            vmem((H, D, D), BF16), vmem((NZ, D, D), BF16),
            vmem((H, 8, D), F32), vmem((NZ, 8, D), F32),
            vmem((NZ, D, D), BF16), vmem((H, D, D), BF16),
            vmem((NZ, 8, D), F32), vmem((H, 8, D), F32),
            vmem((NX, H, D, D), BF16), vmem((S, H, D, D), BF16),
            vmem((NX, G, 8, D), F32), vmem((S, G, 8, D), F32),
            vmem((S * T, H * D), BF16),
            dma((16,)),
            dma((4, 3)), dma((4, 3)), dma((2, G, 3)), dma((2, G, 3)),
            dma((3, 8)), dma((3, 8)), dma((2, 8)), dma((2, 8)),
            dma((2, G, 3)), dma((2, G, 3)),
            dma((2, LAST)), dma((2, LAST)), dma((2, LAST)), dma((2, LAST)),
            dma((1,)), dma((1,)),
        ],
        compiler_params=pltpu.CompilerParams(
            collective_id=0, has_side_effects=True, vmem_limit_bytes=50_000_000
        ),
        name="cell_layer",
    )(*(pltpu.with_memory_space_constraint(array, pltpu.HBM) for array in arrays))
    return out.reshape(S, T, 4096)


def solution(mesh):
    return jax.shard_map(
        on_device,
        mesh=mesh,
        in_specs=(
            P("dp", None, "sp", None),
            P("dp", None, "sp", None),
            P("dp", None, "sp", None),
            P("dp", None, "sp"),
            P("dp", None, "sp"),
            P("dp", None, "sp", None),
            P("dp", None, "sp"),
            P("dp", None),
            P(),
            P(None, "dp"),
        ),
        out_specs=P("dp", "sp", None),
        check_vma=False,
    )
```

```python
import jax
import jax.numpy as jnp
from jax import lax
from jax.experimental import pallas as pl
from jax.experimental.pallas import tpu as pltpu
from jax.sharding import PartitionSpec as P

MESH = pl.DeviceIdType.MESH
F32 = jnp.float32
BF16 = jnp.bfloat16
S, H, T, D = 4, 8, 64, 128
NX, NZ, NY = 4, 8, 8
FACTOR = D**-0.5
NEG = -1e30
G = 4
HG = H // G
RA = 768
RB = (1024 - RA) // NX


def nt(a, b):
    return lax.dot_general(a, b, (((1,), (1,)), ((), ())), preferred_element_type=F32)


def rev(i):
    return i % 2 * 4 + i // 2 % 2 * 2 + i // 4


def kernel(
    i_hbm, f_hbm, q_hbm, k_hbm, v_hbm, c_hbm, n_hbm, w_hbm, level_hbm, gain_hbm, out,
    qv, kv, vv, iv, fv, cv, nv, kx, vx, ix, fx, cx, nx, level, gain, wall, a_loc, num_s, den_s, amx_s,
    wrow, esum, amax, kvs, nkv, turn, cz_send, cz_recv, t_send, t_recv, tm_send, tm_recv,
    p_send, p_recv, pm_send, pm_recv, b_send, b_recv, bm_send, bm_recv, hid, acc,
    lsem, xs_s, xs_r, xk_s, xk_r, tz_s, tz_r, pz_s, pz_r, xo_s, xo_r,
    wy_s, wy_r, wd_s, wd_r, wo_s, wo_r, ws_s, ws_r,
):
    sp = lax.axis_index("sp")
    dp = lax.axis_index("dp")
    x, z = lax.rem(sp, NX), lax.div(sp, NX)
    y, c = lax.div(dp, 2), lax.rem(dp, 2)
    mine = lax.rem(z, 2) * 4 + lax.rem(lax.div(z, 2), 2) * 2 + lax.div(z, 4)

    def xdev(d):
        return {"sp": z * NX + lax.rem(x + d, NX), "dp": dp}

    def zat(p):
        return {"sp": p * NX + x, "dp": dp}

    def ydev(d):
        return {"sp": sp, "dp": lax.rem(y + d + NY, NY) * 2 + c}

    mate = {"sp": sp, "dp": y * 2 + (1 - c)}

    def remote(src, dst, ssem, rsem, dev):
        return pltpu.make_async_remote_copy(
            src_ref=src, dst_ref=dst, send_sem=ssem, recv_sem=rsem,
            device_id=dev, device_id_type=MESH,
        )

    barrier = pltpu.get_barrier_semaphore()
    peers = [xdev(d) for d in range(1, NX)] + [zat(lax.rem(z + d, NZ)) for d in range(1, NZ)]
    peers += [ydev(1), ydev(-1), mate]
    for dev in peers:
        pl.semaphore_signal(barrier, inc=1, device_id=dev, device_id_type=MESH)

    pairs_in = [
        (i_hbm, iv), (f_hbm, fv), (k_hbm, kv), (v_hbm, vv), (w_hbm, wall.at[c, 0]), (c_hbm, cv), (n_hbm, nv),
        (q_hbm, qv), (k_hbm.at[x], kx.at[x]), (v_hbm.at[x], vx.at[x]), (i_hbm.at[x], ix.at[x]),
        (f_hbm.at[x], fx.at[x]), (c_hbm.at[x], cx.at[x]), (n_hbm.at[x], nx.at[x]),
        (level_hbm, level), (gain_hbm, gain),
    ]
    loads = [pltpu.make_async_copy(src, dst, lsem.at[i]) for i, (src, dst) in enumerate(pairs_in)]
    for load in loads:
        load.start()

    rows64 = lax.broadcasted_iota(jnp.int32, (T, T), 0)
    cols64 = lax.broadcasted_iota(jnp.int32, (T, T), 1)
    upper = jnp.where(rows64 <= cols64, 1.0, 0.0).astype(F32)
    causal = rows64 >= cols64

    def gates(li, f):
        li, f = li.astype(F32), f.astype(F32)
        lf = jnp.minimum(f, 0.0) - jnp.log1p(jnp.exp(-jnp.abs(f)))
        b = jnp.dot(lf, upper, precision=lax.Precision.HIGHEST, preferred_element_type=F32)
        return li - b, b[:, T - 1 : T]

    with jax.named_scope("loads"):
        for load in loads:
            load.wait()
    for j in range(S):
        a, _ = gates(iv[j], fv[j])
        a_loc[8 * j : 8 * j + 8, :] = a

    def block_gates(p):
        a, e = gates(ix[p], fx[p])
        am = jnp.max(a, axis=1, keepdims=True)
        esum[p] = jnp.broadcast_to(e, (H, D))
        amax[p] = jnp.broadcast_to(am, (H, D))
        wrow[p] = jnp.exp(a - am)

    block_gates(x)

    with jax.named_scope("barrier"):
        pl.semaphore_wait(barrier, len(peers))

    def rows_of(side, kind):
        if kind == "b":
            return pl.ds(pl.multiple_of(RA + RB * x, RB), RB)
        if kind == "half":
            return pl.ds(pl.multiple_of(RA + RB * x + side * (RB // 2), RB // 2), RB // 2)
        if kind == "cut":
            return pl.ds(256 + 128 * side, 128)
        return pl.ds(256 * (2 - kind if side else kind), 256)

    ring = [(0, "b"), (0, 0), (1, "b"), (0, 1), (2, "b"), (0, 2), (3, "half")]
    ring += [(1, 0), (1, 1), (1, 2), (2, 0), (2, 1), (2, 2), (3, 0), (3, "cut")]
    onward = {(0, "b"): (1, "b"), (1, "b"): (2, "b"), (2, "b"): (3, "half"), (2, 1): (3, "cut")}
    for k in range(3):
        onward[0, k], onward[1, k] = (1, k), (2, k)
    onward[2, 0] = (3, 0)

    def wsend(side, item):
        level, kind = item
        k = ring.index(item)
        rows = rows_of(side, kind)
        src, dst = (level, level + 1) if side else ((NY - level) % NY, NY - 1 - level)
        return remote(
            wall.at[c, src, rows], wall.at[c, dst, rows],
            wy_s.at[side, k], wy_r.at[side, k], ydev(-1 if side else 1),
        )

    def wmate(side, item):
        level, kind = item
        k = ring.index(item)
        ref = wall.at[c, level + 1 if side else NY - 1 - level, rows_of(side, kind)]
        return remote(ref, ref, wd_s.at[side, k], wd_r.at[side, k], mate)

    def wmate_recv(side, item):
        level, kind = item
        k = ring.index(item)
        ref = wall.at[1 - c, level + 1 if side else NY - 1 - level, rows_of(side, kind)]
        return remote(ref, ref, wd_s.at[side, k], wd_r.at[side, k], mate)

    def serve(level, kind):
        item = (level, kind)
        with jax.named_scope(f"serve{level}{kind}"):
            for side in (0, 1):
                wsend(side, item).wait_recv()
        for side in (0, 1):
            if item in onward:
                wsend(side, onward[item]).start()
            if kind not in ("b", "half"):
                wmate(side, item).start()

    def begin(level, kind):
        for side in (0, 1):
            wsend(side, (level, kind)).start()

    def wspread(k):
        side, far = k % 2, k // 2
        to = xdev(NX - 1 if side else 1)
        if far:
            own = lax.rem(x + (1 if side else NX - 1), NX)
            rows = pl.ds(pl.multiple_of(RA + RB * own + side * (RB // 2), RB // 2), RB // 2)
        else:
            rows = pl.ds(pl.multiple_of(RA + RB * x, RB), RB)
        ref = wall.at[c, 1:NY, rows]
        return remote(ref, ref, ws_s.at[k], ws_r.at[k], to)

    def wspread_recv(k):
        side, far = k % 2, k // 2
        away = (2 if far else 1) if side else NX - (2 if far else 1)
        own = lax.rem(x + away, NX)
        if far:
            rows = pl.ds(pl.multiple_of(RA + RB * own + side * (RB // 2), RB // 2), RB // 2)
        else:
            rows = pl.ds(pl.multiple_of(RA + RB * own, RB), RB)
        ref = wall.at[c, 1:NY, rows]
        return remote(ref, ref, ws_s.at[k], ws_r.at[k], xdev(1))

    def wrest(core):
        ref = wall.at[core, 1:NY, RA:1024]
        return remote(ref, ref, ws_s.at[4], ws_r.at[4], mate)

    def xsmall(d, here):
        p = lax.rem(x + d, NX)
        slot = x if here else lax.rem(x - d + NX, NX)
        return [
            remote(src.at[p], dst.at[slot], xs_s.at[k, d - 1], xs_r.at[k, d - 1], xdev(d))
            for k, (src, dst) in enumerate([(iv, ix), (fv, fx), (cv, cx), (nv, nx)])
        ]

    def xkeys(d, g, here):
        p = lax.rem(x + d, NX)
        slot = x if here else lax.rem(x - d + NX, NX)
        heads = pl.ds(g * HG, HG)
        return [
            remote(
                src.at[p, heads], dst.at[slot, heads],
                xk_s.at[k, g, d - 1], xk_r.at[k, g, d - 1], xdev(d),
            )
            for k, (src, dst) in enumerate([(kv, kx), (vv, vx)])
        ]

    begin(0, "b")
    begin(0, 0)
    for d in (2, 1, 3):
        for copy in xsmall(d, True):
            copy.start()
    for g in range(G):
        for d in (2, 1, 3):
            for copy in xkeys(d, g, True):
                copy.start()
    ref = wall.at[c, 0]
    w_own = remote(ref, ref, wo_s.at[0], wo_r.at[0], mate)
    w_own.start()

    def intra(i):
        j, h = lax.div(i, H), lax.rem(i, H)
        arow = a_loc[pl.ds(i, 1), :]
        masked = jnp.where(causal, jnp.broadcast_to(arow, (T, T)), NEG)
        top = jnp.max(masked, axis=1, keepdims=True)
        weight = jnp.exp(masked - top)
        scores = nt(qv[j, h], kv[j, h]) * FACTOR * weight
        den_s[i] = jnp.broadcast_to(jnp.sum(scores, axis=1, keepdims=True), (T, D))
        amx_s[i] = jnp.broadcast_to(top, (T, D))
        num_s[i] = jnp.dot(scores.astype(BF16), vv[j, h], preferred_element_type=F32)

    def inner(part):
        def body(i, _):
            for u in range(4):
                intra(part * 8 + i * 4 + u)
            return 0

        with jax.named_scope("intra"):
            lax.fori_loop(0, 2, body, 0)

    def state(p, h):
        w = wrow[p, pl.ds(h, 1), :]
        vt = vx[p, h].astype(F32).T
        hi = w.astype(BF16)
        lo = (w - hi.astype(F32)).astype(BF16)
        rid = lax.broadcasted_iota(jnp.int32, (16, T), 0)
        extra = jnp.where(
            rid == 0,
            jnp.broadcast_to(hi.astype(F32), (16, T)),
            jnp.where(rid == 1, jnp.broadcast_to(lo.astype(F32), (16, T)), 0.0),
        )
        lhs = jnp.concatenate([(vt * w).astype(BF16), extra.astype(BF16)], axis=0)
        st = jnp.dot(lhs, kx[p, h], preferred_element_type=F32)
        kvs[p, h] = st[0:D]
        nkv[p, pl.ds(h, 1), :] = st[D : D + 1] + st[D + 1 : D + 2]

    def states(p, g):
        with jax.named_scope("states"):
            for u in range(HG):
                state(p, g * HG + u)

    inner(0)

    def own(i, _):
        for u in range(4):
            state(x, i * 4 + u)
        return 0

    lax.fori_loop(0, 2, own, 0)
    serve(0, "b")
    begin(0, 1)
    with jax.named_scope("xgates"):
        for d in (1, 3, 2):
            for copy in xsmall(d, False):
                copy.wait_recv()
            block_gates(lax.rem(x - d + NX, NX))

    shift = []
    before = jnp.zeros((H, D), F32)
    top = None
    for i in range(NX):
        a = amax[i] - before
        shift.append(a)
        top = a if top is None else jnp.maximum(top, a)
        before = before + esum[i]
    scale = [jnp.exp(a - top) for a in shift]

    def tz(h):
        p = rev(h)
        d = lax.rem(p - z + NZ, NZ)
        return d, [
            remote(tm_send.at[h], tm_recv.at[z], tz_s.at[0, d], tz_r.at[0, d], zat(p)),
            remote(t_send.at[h], t_recv.at[z], tz_s.at[1, d], tz_r.at[1, d], zat(p)),
        ]

    def total(g):
        for d in (1, 3, 2):
            with jax.named_scope(f"xin{g}{d}"):
                for copy in xkeys(d, g, False):
                    copy.wait_recv()
            states(lax.rem(x - d + NX, NX), g)
        for h in range(g * HG, g * HG + HG):
            ntot = sum(scale[i][h : h + 1] * nkv[i, h : h + 1, :] for i in range(NX))
            t_send[h] = sum(scale[i][h : h + 1] * kvs[i, h] for i in range(NX)).astype(BF16)
            tm_send[h, 0:1, :] = ntot
            tm_send[h, 1:2, :] = before[h : h + 1]
            tm_send[h, 2:3, :] = top[h : h + 1]
            tm_send[h, 3:4, :] = nfirst[h : h + 1]
        for h in range(g * HG, g * HG + HG):
            d, copies = tz(h)

            @pl.when(d != 0)
            def _():
                for copy in copies:
                    copy.start()

    def cz(d):
        p = lax.rem(z + d, NZ)
        h = lax.rem(p, 2) * 4 + lax.rem(lax.div(p, 2), 2) * 2 + lax.div(p, 4)
        return remote(cz_send.at[h], cz_recv.at[z], tz_s.at[2, d], tz_r.at[2, d], zat(p))

    for i in range(NX):
        turn[4 * i : 4 * i + 4, 0:H] = nx[i]
        for h in range(H):
            cz_send[h, 4 * i : 4 * i + 4, :] = cx[i, 4 * h : 4 * h + 4, :]
    first_lanes = lax.broadcasted_iota(jnp.int32, (H, D), 1) < 4 * NX
    nfirst = jnp.where(first_lanes, turn[...].T[0:H], 0.0)

    def pz(d):
        p = lax.rem(z + d, NZ)
        return [
            remote(pm_send.at[p], pm_recv.at[mine], pz_s.at[0, d], pz_r.at[0, d], zat(p)),
            remote(p_send.at[p], p_recv.at[mine], pz_s.at[1, d], pz_r.at[1, d], zat(p)),
        ]

    def scan(g):
        @pl.when(lax.div(mine, HG) == g)
        def _():
            with jax.named_scope(f"zin{g}"):
                for d in range(1, NZ):
                    p = lax.rem(z - d + NZ, NZ)
                    for src, dst, k in ((tm_send, tm_recv, 0), (t_send, t_recv, 1), (cz_send, cz_recv, 2)):
                        remote(src.at[0], dst.at[p], tz_s.at[k, d], tz_r.at[k, d], zat(p)).wait_recv()
            with jax.named_scope("scan"):
                t_recv[z] = t_send[mine]
                tm_recv[z] = tm_send[mine]
                cz_recv[z] = cz_send[mine]
                lanes = lax.broadcasted_iota(jnp.int32, (1, H), 1)
                m = jnp.sum(jnp.where(lanes == mine, level[pl.ds(x, 1), :], 0.0), axis=1, keepdims=True)
                m = jnp.broadcast_to(m, (1, D))
                nrow = tm_recv[0, 3:4, :]
                for i in range(1, NZ):
                    nrow = nrow + pltpu.roll(tm_recv[i, 3:4, :], 4 * NX * i, 1)
                cur = jnp.concatenate([cz_recv[i] for i in range(NZ)], axis=0).T
                for i in range(NZ):
                    p_send[i] = cur.astype(BF16)
                    pm_send[i, 0:1, :] = nrow
                    pm_send[i, 1:2, :] = m
                    am = tm_recv[i, 2:3, :]
                    hi = jnp.maximum(m, am)
                    keep, add = jnp.exp(m - hi), jnp.exp(am - hi)
                    cur = keep * cur + add * t_recv[i].astype(F32)
                    nrow = keep * nrow + add * tm_recv[i, 0:1, :]
                    m = tm_recv[i, 1:2, :] + hi
                for d in (4, 3, 5, 2, 6, 1, 7):
                    for copy in pz(d):
                        copy.start()
                p_recv[mine] = p_send[z]
                pm_recv[mine] = pm_send[z]

    def xo(d, g, here):
        p = lax.rem(x + d, NX)
        slot = x if here else lax.rem(x - d + NX, NX)
        heads = pl.ds(g * HG, HG)
        return [
            remote(
                bm_send.at[p, g], bm_recv.at[slot, g],
                xo_s.at[0, g, d - 1], xo_r.at[0, g, d - 1], xdev(d),
            ),
            remote(
                b_send.at[p, heads], b_recv.at[slot, heads],
                xo_s.at[1, g, d - 1], xo_r.at[1, g, d - 1], xdev(d),
            ),
        ]

    def spread(g):
        for h in range(g * HG, g * HG + HG):
            p = rev(h)
            d = lax.rem(z - p + NZ, NZ)

            @pl.when(d != 0)
            def _():
                with jax.named_scope(f"zout{g}"):
                    for src, dst, k in ((pm_send, pm_recv, 0), (p_send, p_recv, 1)):
                        remote(src.at[0], dst.at[h], pz_s.at[k, d], pz_r.at[k, d], zat(p)).wait_recv()

        for u in range(HG):
            h = g * HG + u
            cur = p_recv[h].astype(F32)
            nrow = pm_recv[h, 0:1, :]
            m = pm_recv[h, 1:2, :]
            for i in range(NX):
                b_send[i, h] = cur.astype(BF16)
                bm_send[i, g, 2 * u : 2 * u + 1, :] = nrow
                bm_send[i, g, 2 * u + 1 : 2 * u + 2, :] = m
                if i < NX - 1:
                    am = amax[i, h : h + 1, :]
                    hi = jnp.maximum(m, am)
                    keep, add = jnp.exp(m - hi), jnp.exp(am - hi)
                    cur = keep * cur + add * kvs[i, h]
                    nrow = keep * nrow + add * nkv[i, h : h + 1, :]
                    m = esum[i, h : h + 1, :] + hi
        for d in (2, 1, 3):
            for copy in xo(d, g, True):
                copy.start()
        heads = pl.ds(g * HG, HG)
        b_recv[x, heads] = b_send[x, heads]
        bm_recv[x, g] = bm_send[x, g]

    def finish_one(j, g):
        for u in range(HG):
            h = g * HG + u
            i = j * H + h
            q = qv[j, h]
            nrow = bm_recv[j, g, 2 * u : 2 * u + 1, :]
            m = bm_recv[j, g, 2 * u + 1 : 2 * u + 2, :]
            qc = nt(q, b_recv[j, h])
            qn = jnp.sum(q.astype(F32) * nrow, axis=1, keepdims=True)
            a = amx_s[i]
            hi = jnp.maximum(a, m)
            keep, add = jnp.exp(m - hi) * FACTOR, jnp.exp(a - hi)
            den = add * den_s[i] + keep * qn
            num = add * num_s[i] + keep * qc
            o = (num / jnp.maximum(jnp.abs(den), 1.0)).astype(BF16)
            normed = (o.astype(F32) * gain[h : h + 1, :]).astype(BF16)
            hid[pl.ds(pl.multiple_of(j * T, T), T), h * D : h * D + D] = normed

    def finish(g):
        with jax.named_scope("finish"):
            finish_one(x, g)
        for d in (1, 3, 2):
            with jax.named_scope(f"xout{g}{d}"):
                for copy in xo(d, g, False):
                    copy.wait_recv()
            with jax.named_scope("finish"):
                finish_one(lax.rem(x - d + NX, NX), g)

    def columns(core, r):
        block = lax.rem(y + r, NY) * 2 + core
        return pl.ds(pl.multiple_of(block * 256, 256), 256)

    def early(slots):
        def body(i, _):
            core = lax.rem(i, 2)
            r = lax.rem(slots[0] + lax.div(i, 2), NY)
            acc[core, r] = jnp.dot(hid[:, 0:RA], wall[core, r, 0:RA], preferred_element_type=F32)
            return 0

        with jax.named_scope("early"):
            lax.fori_loop(0, 2 * len(slots), body, 0)

    def mates(items):
        with jax.named_scope("mate"):
            for item in items:
                for side in (0, 1):
                    wmate_recv(side, item).wait_recv()

    def late():
        def body(i, _):
            core = lax.rem(i, 2)
            r = lax.rem(NY - 3 + lax.div(i, 2), NY)
            part = jnp.dot(hid[:, RA:1024], wall[core, r, RA:1024], preferred_element_type=F32)
            out[:, columns(core, r)] = (acc[core, r] + part).astype(BF16)
            return 0

        with jax.named_scope("late"):
            lax.fori_loop(0, 2 * (NY - 1), body, 0)

    def last():
        def body(core, _):
            whole = jnp.dot(hid[...], wall[core, NY // 2], preferred_element_type=F32)
            out[:, columns(core, NY // 2)] = whole.astype(BF16)
            return 0

        with jax.named_scope("last"):
            lax.fori_loop(0, 2, body, 0)

    def sent_w(*items):
        for item in items:
            for side in (0, 1):
                wsend(side, item).wait_send()

    def sent_mate(*items):
        for item in items:
            for side in (0, 1):
                wmate(side, item).wait_send()

    for d in (4, 3, 5, 2, 6, 1, 7):
        cz(d).start()
    inner(1)
    total(0)
    serve(1, "b")
    begin(0, 2)
    inner(2)
    total(1)
    serve(2, "b")
    serve(0, 0)
    serve(0, 1)
    inner(3)
    total(2)
    serve(3, "half")
    wspread(0).start()
    wspread(1).start()
    scan(0)
    serve(0, 2)
    total(3)
    scan(1)
    serve(1, 0)
    for d in range(1, NX):
        for copy in xsmall(d, True):
            copy.wait_send()
        for g in range(G):
            for copy in xkeys(d, g, True):
                copy.wait_send()
    serve(1, 1)
    spread(0)
    with jax.named_scope("wspread"):
        wspread_recv(0).wait_recv()
        wspread_recv(1).wait_recv()
    wspread(2).start()
    wspread(3).start()
    scan(2)
    spread(1)
    serve(1, 2)
    scan(3)
    sent_w((0, "b"), (1, "b"), (2, "b"), (3, "half"), (0, 0), (0, 1), (0, 2))
    finish(0)
    serve(2, 0)
    spread(2)
    for d in range(1, NZ):
        p = lax.rem(z + d, NZ)
        for src, dst, k in ((tm_send, tm_recv, 0), (t_send, t_recv, 1), (cz_send, cz_recv, 2)):
            remote(src.at[0], dst.at[0], tz_s.at[k, d], tz_r.at[k, d], zat(p)).wait_send()
    finish(1)
    serve(2, 1)
    spread(3)
    with jax.named_scope("wspread"):
        wspread_recv(2).wait_recv()
        wspread_recv(3).wait_recv()
    wrest(c).start()
    finish(2)
    serve(2, 2)
    ref = wall.at[1 - c, 0]
    remote(ref, ref, wo_s.at[0], wo_r.at[0], mate).wait_recv()
    mates([(0, 0), (0, 1), (0, 2), (1, 0), (1, 1), (1, 2)])
    early([6, 7, 0, 1, 2])
    sent_w((1, 0), (1, 1), (1, 2))
    sent_mate((0, 0), (0, 1), (0, 2), (1, 0), (1, 1), (1, 2))
    for d in range(1, NZ):
        for copy in pz(d):
            copy.wait_send()
    mates([(2, 0), (2, 1), (2, 2)])
    early([3])
    early([5])
    finish(3)
    serve(3, 0)
    with jax.named_scope("rest"):
        wrest(1 - c).wait_recv()
    late()
    serve(3, "cut")
    for d in range(1, NX):
        for g in range(G):
            for copy in xo(d, g, True):
                copy.wait_send()
    sent_w((2, 0), (2, 1), (2, 2))
    sent_mate((2, 0), (2, 1), (2, 2))
    w_own.wait_send()
    for k in range(4):
        wspread(k).wait_send()
    wrest(c).wait_send()
    mates([(3, 0), (3, "cut")])
    last()
    sent_w((3, 0), (3, "cut"))
    sent_mate((3, 0), (3, "cut"))


def on_device(queries, keys, values, input_gate, forget_gate, start_memory, start_norm, start_level, head_gain, out_weight):
    arrays = (
        input_gate, forget_gate, queries, keys, values, start_memory.reshape(S, 32, D),
        jnp.transpose(start_norm, (0, 2, 1)), out_weight, start_level, head_gain,
    )
    dma, vmem = pltpu.SemaphoreType.DMA, pltpu.VMEM
    out = pl.pallas_call(
        kernel,
        out_shape=pltpu.VMEM((S * T, 4096), BF16),
        in_specs=[pl.BlockSpec(memory_space=pltpu.HBM)] * len(arrays),
        out_specs=pl.BlockSpec(memory_space=pltpu.VMEM),
        scratch_shapes=[
            vmem((S, H, T, D), BF16), vmem((S, H, T, D), BF16), vmem((S, H, T, D), BF16),
            vmem((S, H, T), BF16), vmem((S, H, T), BF16), vmem((S, 32, D), F32), vmem((S, 4, H), F32),
            vmem((NX, H, T, D), BF16), vmem((NX, H, T, D), BF16),
            vmem((NX, H, T), BF16), vmem((NX, H, T), BF16), vmem((NX, 32, D), F32), vmem((NX, 4, H), F32),
            vmem((S, H), F32), vmem((H, D), F32),
            vmem((2, NY, 1024, 256), BF16),
            vmem((S * H, T), F32),
            vmem((S * H, T, D), F32), vmem((S * H, T, D), F32), vmem((S * H, T, D), F32),
            vmem((NX, H, T), F32), vmem((NX, H, D), F32), vmem((NX, H, D), F32),
            vmem((NX, H, D, D), F32), vmem((NX, H, D), F32), vmem((D, D), F32),
            vmem((H, 16, D), F32), vmem((NZ, 16, D), F32),
            vmem((H, D, D), BF16), vmem((NZ, D, D), BF16),
            vmem((H, 8, D), F32), vmem((NZ, 8, D), F32),
            vmem((NZ, D, D), BF16), vmem((H, D, D), BF16),
            vmem((NZ, 8, D), F32), vmem((H, 8, D), F32),
            vmem((NX, H, D, D), BF16), vmem((S, H, D, D), BF16),
            vmem((NX, G, 8, D), F32), vmem((S, G, 8, D), F32),
            vmem((S * T, H * D), BF16), vmem((2, NY, S * T, 256), F32),
            dma((16,)),
            dma((4, 3)), dma((4, 3)), dma((2, G, 3)), dma((2, G, 3)),
            dma((3, 8)), dma((3, 8)), dma((2, 8)), dma((2, 8)),
            dma((2, G, 3)), dma((2, G, 3)),
            dma((2, 15)), dma((2, 15)), dma((2, 15)), dma((2, 15)),
            dma((1,)), dma((1,)), dma((5,)), dma((5,)),
        ],
        compiler_params=pltpu.CompilerParams(
            collective_id=0, has_side_effects=True, vmem_limit_bytes=50_000_000
        ),
        name="cell_layer",
    )(*(pltpu.with_memory_space_constraint(array, pltpu.HBM) for array in arrays))
    return out.reshape(S, T, 4096)


def solution(mesh):
    return jax.shard_map(
        on_device,
        mesh=mesh,
        in_specs=(
            P("dp", None, "sp", None),
            P("dp", None, "sp", None),
            P("dp", None, "sp", None),
            P("dp", None, "sp"),
            P("dp", None, "sp"),
            P("dp", None, "sp", None),
            P("dp", None, "sp"),
            P("dp", None),
            P(),
            P(None, "dp"),
        ),
        out_specs=P("dp", "sp", None),
        check_vma=False,
    )
```

```python
import jax
import jax.numpy as jnp
from jax import lax
from jax.experimental import pallas as pl
from jax.experimental.pallas import tpu as pltpu
from jax.sharding import PartitionSpec as P

MESH = pl.DeviceIdType.MESH
F32 = jnp.float32
BF16 = jnp.bfloat16
S, H, T, D = 4, 8, 64, 128
NX, NZ, NY = 4, 8, 8
FACTOR = D**-0.5
NEG = -1e30
G = 4
HG = H // G
RA = 768
RB = (1024 - RA) // NX


def nt(a, b):
    return lax.dot_general(a, b, (((1,), (1,)), ((), ())), preferred_element_type=F32)


def rev(i):
    return i % 2 * 4 + i // 2 % 2 * 2 + i // 4


def kernel(
    i_hbm, f_hbm, q_hbm, k_hbm, v_hbm, c_hbm, n_hbm, w_hbm, level_hbm, gain_hbm, out,
    qv, kv, vv, iv, fv, cv, nv, kx, vx, ix, fx, cx, nx, level, gain, wall, a_loc, num_s, den_s, amx_s,
    wrow, esum, amax, kvs, nkv, turn, cz_send, cz_recv, t_send, t_recv, tm_send, tm_recv,
    p_send, p_recv, pm_send, pm_recv, b_send, b_recv, bm_send, bm_recv, hid, acc,
    lsem, sent, xs_r, xk_r, tz_r, pz_r, xo_r, wy_r, wd_r, ws_r, wo_r, hello,
):
    sp = lax.axis_index("sp")
    dp = lax.axis_index("dp")
    x, z = lax.rem(sp, NX), lax.div(sp, NX)
    y, c = lax.div(dp, 2), lax.rem(dp, 2)
    mine = lax.rem(z, 2) * 4 + lax.rem(lax.div(z, 2), 2) * 2 + lax.div(z, 4)

    def xdev(d):
        return {"sp": z * NX + lax.rem(x + d, NX), "dp": dp}

    def zat(p):
        return {"sp": p * NX + x, "dp": dp}

    def ydev(d):
        return {"sp": sp, "dp": lax.rem(y + d + NY, NY) * 2 + c}

    mate = {"sp": sp, "dp": y * 2 + (1 - c)}

    def remote(src, dst, ssem, rsem, dev):
        return pltpu.make_async_remote_copy(
            src_ref=src, dst_ref=dst, send_sem=ssem, recv_sem=rsem,
            device_id=dev, device_id_type=MESH,
        )

    barrier = pltpu.get_barrier_semaphore()
    peers = [xdev(d) for d in range(1, NX)] + [ydev(1), ydev(-1), mate]
    for dev in peers:
        pl.semaphore_signal(barrier, inc=1, device_id=dev, device_id_type=MESH)
    for d in range(1, NZ):

        @pl.when(z + d < NZ)
        def _():
            dev = zat(lax.rem(z + d, NZ))
            pl.semaphore_signal(barrier, inc=1, device_id=dev, device_id_type=MESH)

    loads = [
        (i_hbm, iv, 0), (f_hbm, fv, 1), (k_hbm, kv, 2), (v_hbm, vv, 2), (w_hbm, wall.at[c, 0], 2), (q_hbm, qv, 2),
        (c_hbm, cv, 3), (n_hbm, nv, 4), (level_hbm, level, 5), (gain_hbm, gain, 6),
    ]
    for src, dst, k in loads:
        pltpu.make_async_copy(src, dst, lsem.at[k]).start()

    rows64 = lax.broadcasted_iota(jnp.int32, (T, T), 0)
    cols64 = lax.broadcasted_iota(jnp.int32, (T, T), 1)
    upper = jnp.where(rows64 <= cols64, 1.0, 0.0).astype(F32)
    causal = rows64 >= cols64

    def gates(li, f):
        li, f = li.astype(F32), f.astype(F32)
        lf = jnp.minimum(f, 0.0) - jnp.log1p(jnp.exp(-jnp.abs(f)))
        b = jnp.dot(lf, upper, precision=lax.Precision.HIGHEST, preferred_element_type=F32)
        return li - b, b[:, T - 1 : T]

    def arrived(ref, sem):
        pltpu.make_async_copy(ref, ref, sem).wait()

    with jax.named_scope("loads"):
        arrived(iv, lsem.at[0])
        arrived(fv, lsem.at[1])
    for j in range(S):
        a, _ = gates(iv[j], fv[j])
        a_loc[8 * j : 8 * j + 8, :] = a

    def block_gates(p, li, f):
        a, e = gates(li, f)
        am = jnp.max(a, axis=1, keepdims=True)
        esum[p] = jnp.broadcast_to(e, (H, D))
        amax[p] = jnp.broadcast_to(am, (H, D))
        wrow[p] = jnp.exp(a - am)

    block_gates(x, iv[x], fv[x])
    arrived(wall.at[c, 0:4], lsem.at[2])
    for k, ref in ((3, cv), (4, nv), (5, level), (6, gain)):
        arrived(ref, lsem.at[k])
    cx[x] = cv[x]
    nx[x] = nv[x]

    with jax.named_scope("barrier"):
        pl.semaphore_wait(barrier, len(peers) + z)
    for d in range(1, NZ):

        @pl.when(z >= d)
        def _():
            dev = zat(lax.rem(z - d + NZ, NZ))
            pl.semaphore_signal(hello, inc=1, device_id=dev, device_id_type=MESH)

    def rows_of(side, kind):
        if kind == "b":
            return pl.ds(pl.multiple_of(RA + RB * x, RB), RB)
        if kind == "half":
            return pl.ds(pl.multiple_of(RA + RB * x + side * (RB // 2), RB // 2), RB // 2)
        if kind == "cut":
            return pl.ds(256 + 128 * side, 128)
        return pl.ds(256 * (2 - kind if side else kind), 256)

    ring = [(0, "b"), (0, 0), (1, "b"), (0, 1), (2, "b"), (0, 2), (3, "half")]
    ring += [(1, 0), (1, 1), (1, 2), (2, 0), (2, 1), (2, 2), (3, 0), (3, "cut")]
    onward = {(0, "b"): (1, "b"), (1, "b"): (2, "b"), (2, "b"): (3, "half"), (2, 1): (3, "cut")}
    for k in range(3):
        onward[0, k], onward[1, k] = (1, k), (2, k)
    onward[2, 0] = (3, 0)

    def wsend(side, item):
        level, kind = item
        k = ring.index(item)
        rows = rows_of(side, kind)
        src, dst = (level, level + 1) if side else ((NY - level) % NY, NY - 1 - level)
        return remote(
            wall.at[c, src, rows], wall.at[c, dst, rows],
            sent.at[12], wy_r.at[k], ydev(-1 if side else 1),
        )

    def wmate(side, item):
        level, kind = item
        ref = wall.at[c, level + 1 if side else NY - 1 - level, rows_of(side, kind)]
        return remote(ref, ref, sent.at[13], wd_r.at[max(0, level - 1)], mate)

    def serve(level, kind):
        item = (level, kind)
        count = {"b": RB, "half": RB // 2, "cut": 128}.get(kind, 256)
        with jax.named_scope(f"serve{level}{kind}"):
            arrived(wall.at[c, 0:2, 0:count], wy_r.at[ring.index(item)])
        for side in (0, 1):
            if item in onward:
                wsend(side, onward[item]).start()
            if kind not in ("b", "half"):
                wmate(side, item).start()

    def begin(level, kind):
        for side in (0, 1):
            wsend(side, (level, kind)).start()

    def wspread(k):
        side, far = k % 2, k // 2
        to = xdev(NX - 1 if side else 1)
        if far:
            own = lax.rem(x + (1 if side else NX - 1), NX)
            rows = pl.ds(pl.multiple_of(RA + RB * own + side * (RB // 2), RB // 2), RB // 2)
        else:
            rows = pl.ds(pl.multiple_of(RA + RB * x, RB), RB)
        ref = wall.at[c, 1:NY, rows]
        return remote(ref, ref, sent.at[14], ws_r.at[far], to)

    def wrest():
        ref = wall.at[c, 1:NY, RA:1024]
        return remote(ref, ref, sent.at[15], ws_r.at[2], mate)

    small = [(iv, ix), (fv, fx), (cv, cx), (nv, nx)]

    def xsmall(d):
        p = lax.rem(x + d, NX)
        return [
            remote(src.at[p], dst.at[x], sent.at[k], xs_r.at[k], xdev(d)) for k, (src, dst) in enumerate(small)
        ]

    def xkeys(d, g):
        p = lax.rem(x + d, NX)
        heads = pl.ds(g * HG, HG)
        return [
            remote(src.at[p, heads], dst.at[x, heads], sent.at[4], xk_r.at[k, g], xdev(d))
            for k, (src, dst) in enumerate([(kv, kx), (vv, vx)])
        ]

    begin(0, "b")
    begin(0, 0)
    for d in (2, 1, 3):
        for copy in xsmall(d):
            copy.start()
    for g in range(G):
        for d in (2, 1, 3):
            for copy in xkeys(d, g):
                copy.start()
    remote(wall.at[c, 0], wall.at[c, 0], sent.at[15], wo_r.at[0], mate).start()

    def intra(i):
        j, h = lax.div(i, H), lax.rem(i, H)
        arow = a_loc[pl.ds(i, 1), :]
        masked = jnp.where(causal, jnp.broadcast_to(arow, (T, T)), NEG)
        top = jnp.max(masked, axis=1, keepdims=True)
        weight = jnp.exp(masked - top)
        scores = nt(qv[j, h], kv[j, h]) * FACTOR * weight
        den_s[i] = jnp.broadcast_to(jnp.sum(scores, axis=1, keepdims=True), (T, D))
        amx_s[i] = jnp.broadcast_to(top, (T, D))
        num_s[i] = jnp.dot(scores.astype(BF16), vv[j, h], preferred_element_type=F32)

    def inner(part):
        def body(i, _):
            for u in range(4):
                intra(part * 8 + i * 4 + u)
            return 0

        with jax.named_scope("intra"):
            lax.fori_loop(0, 2, body, 0)

    def state(p, h, keys, values):
        w = wrow[p, pl.ds(h, 1), :]
        vt = values[p, h].astype(F32).T
        hi = w.astype(BF16)
        lo = (w - hi.astype(F32)).astype(BF16)
        rid = lax.broadcasted_iota(jnp.int32, (16, T), 0)
        extra = jnp.where(
            rid == 0,
            jnp.broadcast_to(hi.astype(F32), (16, T)),
            jnp.where(rid == 1, jnp.broadcast_to(lo.astype(F32), (16, T)), 0.0),
        )
        lhs = jnp.concatenate([(vt * w).astype(BF16), extra.astype(BF16)], axis=0)
        st = jnp.dot(lhs, keys[p, h], preferred_element_type=F32)
        kvs[p, h] = st[0:D]
        nkv[p, pl.ds(h, 1), :] = st[D : D + 1] + st[D + 1 : D + 2]

    def states(p, g):
        with jax.named_scope("states"):
            for u in range(HG):
                state(p, g * HG + u, kx, vx)

    inner(0)

    def own(i, _):
        for u in range(4):
            state(x, i * 4 + u, kv, vv)
        return 0

    lax.fori_loop(0, 2, own, 0)
    serve(0, "b")
    begin(0, 1)
    with jax.named_scope("xgates"):
        for k, (src, dst) in enumerate(small):
            arrived(dst.at[0:3], xs_r.at[k])
        for d in (1, 3, 2):
            p = lax.rem(x - d + NX, NX)
            block_gates(p, ix[p], fx[p])

    shift = []
    before = jnp.zeros((H, D), F32)
    top = None
    for i in range(NX):
        a = amax[i] - before
        shift.append(a)
        top = a if top is None else jnp.maximum(top, a)
        before = before + esum[i]
    scale = [jnp.exp(a - top) for a in shift]

    def tz(h):
        p = rev(h)
        d = lax.rem(p - z + NZ, NZ)
        return d, [
            remote(tm_send.at[h], tm_recv.at[z], sent.at[5], tz_r.at[0], zat(p)),
            remote(t_send.at[h], t_recv.at[z], sent.at[6], tz_r.at[1], zat(p)),
        ]

    def total(g):
        with jax.named_scope(f"xin{g}"):
            for k, ref in enumerate((kx, vx)):
                arrived(ref.at[0:3, 0:HG], xk_r.at[k, g])
        for d in (1, 3, 2):
            states(lax.rem(x - d + NX, NX), g)
        for h in range(g * HG, g * HG + HG):
            ntot = sum(scale[i][h : h + 1] * nkv[i, h : h + 1, :] for i in range(NX))
            t_send[h] = sum(scale[i][h : h + 1] * kvs[i, h] for i in range(NX)).astype(BF16)
            tm_send[h, 0:1, :] = ntot
            tm_send[h, 1:2, :] = before[h : h + 1]
            tm_send[h, 2:3, :] = top[h : h + 1]
            tm_send[h, 3:4, :] = nfirst[h : h + 1]

    def total_send(g):
        for h in range(g * HG, g * HG + HG):
            d, copies = tz(h)

            @pl.when(d != 0)
            def _():
                for copy in copies:
                    copy.start()

    def cz(d):
        p = lax.rem(z + d, NZ)
        h = lax.rem(p, 2) * 4 + lax.rem(lax.div(p, 2), 2) * 2 + lax.div(p, 4)
        return remote(cz_send.at[h], cz_recv.at[z], sent.at[7], tz_r.at[2], zat(p))

    for i in range(NX):
        turn[4 * i : 4 * i + 4, 0:H] = nx[i]
        for h in range(H):
            cz_send[h, 4 * i : 4 * i + 4, :] = cx[i, 4 * h : 4 * h + 4, :]
    first_lanes = lax.broadcasted_iota(jnp.int32, (H, D), 1) < 4 * NX
    nfirst = jnp.where(first_lanes, turn[...].T[0:H], 0.0)

    group = lax.div(mine, HG)

    def pz(d):
        p = lax.rem(z + d, NZ)
        return [
            remote(pm_send.at[p], pm_recv.at[mine], sent.at[8], pz_r.at[0, group], zat(p)),
            remote(p_send.at[p], p_recv.at[mine], sent.at[9], pz_r.at[1, group], zat(p)),
        ]

    def scan(g):
        @pl.when(group == g)
        def _():
            with jax.named_scope(f"zin{g}"):
                for k, ref in enumerate((tm_recv, t_recv, cz_recv)):
                    arrived(ref.at[0 : NZ - 1], tz_r.at[k])
            with jax.named_scope("scan"):
                t_recv[z] = t_send[mine]
                tm_recv[z] = tm_send[mine]
                cz_recv[z] = cz_send[mine]
                lanes = lax.broadcasted_iota(jnp.int32, (1, H), 1)
                m = jnp.sum(jnp.where(lanes == mine, level[pl.ds(x, 1), :], 0.0), axis=1, keepdims=True)
                m = jnp.broadcast_to(m, (1, D))
                nrow = tm_recv[0, 3:4, :]
                for i in range(1, NZ):
                    nrow = nrow + pltpu.roll(tm_recv[i, 3:4, :], 4 * NX * i, 1)
                cur = jnp.concatenate([cz_recv[i] for i in range(NZ)], axis=0).T
                for i in range(NZ):
                    p_send[i] = cur.astype(BF16)
                    pm_send[i, 0:1, :] = nrow
                    pm_send[i, 1:2, :] = m
                    am = tm_recv[i, 2:3, :]
                    hi = jnp.maximum(m, am)
                    keep, add = jnp.exp(m - hi), jnp.exp(am - hi)
                    cur = keep * cur + add * t_recv[i].astype(F32)
                    nrow = keep * nrow + add * tm_recv[i, 0:1, :]
                    m = tm_recv[i, 1:2, :] + hi
                for d in (4, 3, 5, 2, 6, 1, 7):
                    for copy in pz(d):
                        copy.start()
                p_recv[mine] = p_send[z]
                pm_recv[mine] = pm_send[z]

    def xo(d, g):
        p = lax.rem(x + d, NX)
        heads = pl.ds(g * HG, HG)
        return [
            remote(bm_send.at[p, g], bm_recv.at[x, g], sent.at[10], xo_r.at[0, g], xdev(d)),
            remote(b_send.at[p, heads], b_recv.at[x, heads], sent.at[11], xo_r.at[1, g], xdev(d)),
        ]

    def spread(g):
        with jax.named_scope(f"zout{g}"):

            @pl.when(group == g)
            def _():
                for k, ref in enumerate((pm_recv, p_recv)):
                    arrived(ref.at[0 : HG - 1], pz_r.at[k, g])

            @pl.when(group != g)
            def _():
                for k, ref in enumerate((pm_recv, p_recv)):
                    arrived(ref.at[0:HG], pz_r.at[k, g])

        for u in range(HG):
            h = g * HG + u
            cur = p_recv[h].astype(F32)
            nrow = pm_recv[h, 0:1, :]
            m = pm_recv[h, 1:2, :]
            for i in range(NX):
                b_send[i, h] = cur.astype(BF16)
                bm_send[i, g, 2 * u : 2 * u + 1, :] = nrow
                bm_send[i, g, 2 * u + 1 : 2 * u + 2, :] = m
                if i < NX - 1:
                    am = amax[i, h : h + 1, :]
                    hi = jnp.maximum(m, am)
                    keep, add = jnp.exp(m - hi), jnp.exp(am - hi)
                    cur = keep * cur + add * kvs[i, h]
                    nrow = keep * nrow + add * nkv[i, h : h + 1, :]
                    m = esum[i, h : h + 1, :] + hi
        for d in (2, 1, 3):
            for copy in xo(d, g):
                copy.start()
        heads = pl.ds(g * HG, HG)
        b_recv[x, heads] = b_send[x, heads]
        bm_recv[x, g] = bm_send[x, g]

    def finish_one(j, g):
        for u in range(HG):
            h = g * HG + u
            i = j * H + h
            q = qv[j, h]
            nrow = bm_recv[j, g, 2 * u : 2 * u + 1, :]
            m = bm_recv[j, g, 2 * u + 1 : 2 * u + 2, :]
            qc = nt(q, b_recv[j, h])
            qn = jnp.sum(q.astype(F32) * nrow, axis=1, keepdims=True)
            a = amx_s[i]
            hi = jnp.maximum(a, m)
            keep, add = jnp.exp(m - hi) * FACTOR, jnp.exp(a - hi)
            den = add * den_s[i] + keep * qn
            num = add * num_s[i] + keep * qc
            o = (num / jnp.maximum(jnp.abs(den), 1.0)).astype(BF16)
            normed = (o.astype(F32) * gain[h : h + 1, :]).astype(BF16)
            hid[pl.ds(pl.multiple_of(j * T, T), T), h * D : h * D + D] = normed

    def finish(g):
        with jax.named_scope("finish"):
            finish_one(x, g)
        with jax.named_scope(f"xout{g}"):
            arrived(bm_recv.at[0:3, 0], xo_r.at[0, g])
            arrived(b_recv.at[0:3, 0:HG], xo_r.at[1, g])
        with jax.named_scope("finish"):
            for d in (1, 3, 2):
                finish_one(lax.rem(x - d + NX, NX), g)

    def columns(core, r):
        block = lax.rem(y + r, NY) * 2 + core
        return pl.ds(pl.multiple_of(block * 256, 256), 256)

    def early_one(r):
        for core in (0, 1):
            acc[core, r] = jnp.dot(hid[:, 0:RA], wall[core, r, 0:RA], preferred_element_type=F32)

    def late_one(r):
        for core in (0, 1):
            part = jnp.dot(hid[:, RA:1024], wall[core, r, RA:1024], preferred_element_type=F32)
            out[:, columns(core, r)] = (acc[core, r] + part).astype(BF16)

    def twos(name, fn, low, high):
        def body(i, _):
            fn(lax.rem(NY - 2 + 2 * i, NY))
            fn(lax.rem(NY - 1 + 2 * i, NY))
            return 0

        with jax.named_scope(name):
            lax.fori_loop(low, high, body, 0)

    def last():
        with jax.named_scope("last"):
            for core in (0, 1):
                whole = jnp.dot(hid[...], wall[core, NY // 2], preferred_element_type=F32)
                out[:, columns(core, NY // 2)] = whole.astype(BF16)

    def mates(level):
        with jax.named_scope("mate"):
            count = (4, 2, 1)[level]
            arrived(wall.at[c, 0:count, 0:RA], wd_r.at[level])

    def zgate():
        with jax.named_scope("zgate"):

            @pl.when(z < NZ - 1)
            def _():
                pl.semaphore_wait(hello, NZ - 1 - z)

    def cz_all():
        for d in (4, 3, 5, 2, 6, 1, 7):
            cz(d).start()

    def wspread_near():
        with jax.named_scope("wspread"):
            arrived(wall.at[c, 1:NY, 0 : 2 * RB], ws_r.at[0])
        wspread(2).start()
        wspread(3).start()

    def wspread_far():
        with jax.named_scope("wspread"):
            arrived(wall.at[c, 1:NY, 0:RB], ws_r.at[1])
        wrest().start()

    def sent_cell():
        for k, ref in enumerate((iv, fv, cv, nv)):
            arrived(ref.at[0:3], sent.at[k])
        arrived(b_send.at[0:3], sent.at[4])
        for k, ref in ((5, tm_send), (6, t_send), (7, cz_send), (8, pm_send), (9, p_send)):
            arrived(ref.at[0 : NZ - 1], sent.at[k])
        arrived(wall.at[c, 1:NY, 0 : 3 * RB], sent.at[14])

    def sent_rest():
        arrived(bm_send.at[0:3], sent.at[10])
        arrived(b_send.at[0:3], sent.at[11])
        arrived(wall.at[c, :, 0:352], sent.at[15])

    def sent_ring():
        arrived(wall.at[c, 1:NY, 0:832], sent.at[12])
        arrived(wall.at[c, 1:NY, 0:768], sent.at[13])

    inner(1)
    total(0)
    serve(1, "b")
    begin(0, 2)

    @pl.when(z < NZ // 2)
    def _():
        inner(2)
        total(1)
        zgate()
        total_send(0)
        cz_all()
        total_send(1)
        serve(2, "b")
        serve(0, 0)
        serve(0, 1)
        inner(3)
        total(2)
        total_send(2)
        serve(3, "half")
        wspread(0).start()
        wspread(1).start()
        serve(0, 2)
        total(3)
        total_send(3)
        serve(1, 0)
        serve(1, 1)
        wspread_near()
        scan(0)
        serve(1, 2)
        scan(1)
        wspread_far()
        serve(2, 0)
        scan(2)
        spread(0)
        serve(2, 1)
        scan(3)
        spread(1)
        serve(2, 2)
        finish(0)
        spread(2)
        finish(1)
        serve(3, 0)
        serve(3, "cut")
        spread(3)
        arrived(wall.at[c, 0], wo_r.at[0])
        mates(0)
        mates(1)
        mates(2)
        finish(2)
        twos("early", early_one, 0, 4)
        sent_cell()
        finish(3)
        arrived(wall.at[c, 1:NY, RA:1024], ws_r.at[2])
        twos("late", late_one, 0, 4)
        sent_rest()
        sent_ring()

    @pl.when(z >= NZ // 2)
    def _():
        zgate()
        total_send(0)
        cz_all()
        inner(2)
        total(1)
        total_send(1)
        serve(2, "b")
        serve(0, 0)
        serve(0, 1)
        inner(3)
        total(2)
        total_send(2)
        serve(3, "half")
        wspread(0).start()
        wspread(1).start()
        scan(0)
        serve(0, 2)
        total(3)
        total_send(3)
        scan(1)
        serve(1, 0)
        spread(0)
        serve(1, 1)
        wspread_near()
        scan(2)
        spread(1)
        serve(1, 2)
        scan(3)
        finish(0)
        serve(2, 0)
        spread(2)
        finish(1)
        serve(2, 1)
        spread(3)
        wspread_far()
        arrived(wall.at[c, 0], wo_r.at[0])
        mates(0)
        finish(2)
        twos("early", early_one, 0, 2)
        serve(2, 2)
        sent_cell()
        finish(3)
        mates(1)
        with jax.named_scope("early"):
            early_one(2)
            early_one(3)
            early_one(5)
        serve(3, 0)
        arrived(wall.at[c, 1:NY, RA:1024], ws_r.at[2])
        twos("late", late_one, 0, 3)
        with jax.named_scope("late"):
            late_one(5)
        serve(3, "cut")
        sent_rest()
        mates(2)
        last()
        sent_ring()

def on_device(queries, keys, values, input_gate, forget_gate, start_memory, start_norm, start_level, head_gain, out_weight):
    arrays = (
        input_gate, forget_gate, queries, keys, values, start_memory.reshape(S, 32, D),
        jnp.transpose(start_norm, (0, 2, 1)), out_weight, start_level, head_gain,
    )
    dma, vmem = pltpu.SemaphoreType.DMA, pltpu.VMEM
    out = pl.pallas_call(
        kernel,
        out_shape=pltpu.VMEM((S * T, 4096), BF16),
        in_specs=[pl.BlockSpec(memory_space=pltpu.HBM)] * len(arrays),
        out_specs=pl.BlockSpec(memory_space=pltpu.VMEM),
        scratch_shapes=[
            vmem((S, H, T, D), BF16), vmem((S, H, T, D), BF16), vmem((S, H, T, D), BF16),
            vmem((S, H, T), BF16), vmem((S, H, T), BF16), vmem((S, 32, D), F32), vmem((S, 4, H), F32),
            vmem((NX, H, T, D), BF16), vmem((NX, H, T, D), BF16),
            vmem((NX, H, T), BF16), vmem((NX, H, T), BF16), vmem((NX, 32, D), F32), vmem((NX, 4, H), F32),
            vmem((S, H), F32), vmem((H, D), F32),
            vmem((2, NY, 1024, 256), BF16),
            vmem((S * H, T), F32),
            vmem((S * H, T, D), F32), vmem((S * H, T, D), F32), vmem((S * H, T, D), F32),
            vmem((NX, H, T), F32), vmem((NX, H, D), F32), vmem((NX, H, D), F32),
            vmem((NX, H, D, D), F32), vmem((NX, H, D), F32), vmem((D, D), F32),
            vmem((H, 16, D), F32), vmem((NZ, 16, D), F32),
            vmem((H, D, D), BF16), vmem((NZ, D, D), BF16),
            vmem((H, 8, D), F32), vmem((NZ, 8, D), F32),
            vmem((NZ, D, D), BF16), vmem((H, D, D), BF16),
            vmem((NZ, 8, D), F32), vmem((H, 8, D), F32),
            vmem((NX, H, D, D), BF16), vmem((S, H, D, D), BF16),
            vmem((NX, G, 8, D), F32), vmem((S, G, 8, D), F32),
            vmem((S * T, H * D), BF16), vmem((2, NY, S * T, 256), F32),
            dma((7,)), dma((16,)), dma((4,)), dma((2, G)), dma((3,)), dma((2, G)), dma((2, G)),
            dma((15,)), dma((3,)), dma((3,)), dma((1,)), pltpu.SemaphoreType.REGULAR,
        ],
        compiler_params=pltpu.CompilerParams(
            collective_id=0, has_side_effects=True, vmem_limit_bytes=50_000_000
        ),
        name="cell_layer",
    )(*(pltpu.with_memory_space_constraint(array, pltpu.HBM) for array in arrays))
    return out.reshape(S, T, 4096)


def solution(mesh):
    return jax.shard_map(
        on_device,
        mesh=mesh,
        in_specs=(
            P("dp", None, "sp", None),
            P("dp", None, "sp", None),
            P("dp", None, "sp", None),
            P("dp", None, "sp"),
            P("dp", None, "sp"),
            P("dp", None, "sp", None),
            P("dp", None, "sp"),
            P("dp", None),
            P(),
            P(None, "dp"),
        ),
        out_specs=P("dp", "sp", None),
        check_vma=False,
    )
```

```python
import jax
import jax.numpy as jnp
from jax import lax
from jax.experimental import pallas as pl
from jax.experimental.pallas import tpu as pltpu
from jax.sharding import PartitionSpec as P

MESH = pl.DeviceIdType.MESH
F32 = jnp.float32
BF16 = jnp.bfloat16
S, H, T, D = 4, 8, 64, 128
NX, NZ, NY = 4, 8, 8
FACTOR = D**-0.5
NEG = -1e30
FEW = 3
G = 4
HG = H // G
RA = 768
RB = (1024 - RA) // NX


def nt(a, b):
    return lax.dot_general(a, b, (((1,), (1,)), ((), ())), preferred_element_type=F32)


def rev(i):
    return i % 2 * 4 + i // 2 % 2 * 2 + i // 4


def kernel(
    i_hbm, f_hbm, q_hbm, k_hbm, v_hbm, c_hbm, n_hbm, w_hbm, level_hbm, gain_hbm, out,
    qv, kv, vv, iv, fv, cv, nv, kx, vx, ix, fx, cx, nx, level, gain, wall, a_loc, num_s, den_s, amx_s,
    wrow, esum, amax, kvs, nkv, turn, cz_send, cz_recv, held, held_n, t_send, t_recv, tm_send, tm_recv,
    p_send, p_recv, pm_send, pm_recv, b_send, b_recv, bm_send, bm_recv, hid, acc,
    lsem, sent, xs_r, xk_r, tz_r, pz_r, xo_r, wy_r, wd_r, ws_r, wo_r, hello,
):
    sp = lax.axis_index("sp")
    dp = lax.axis_index("dp")
    x, z = lax.rem(sp, NX), lax.div(sp, NX)
    y, c = lax.div(dp, 2), lax.rem(dp, 2)
    mine = lax.rem(z, 2) * 4 + lax.rem(lax.div(z, 2), 2) * 2 + lax.div(z, 4)

    def xdev(d):
        return {"sp": z * NX + lax.rem(x + d, NX), "dp": dp}

    def zat(p):
        return {"sp": p * NX + x, "dp": dp}

    def ydev(d):
        return {"sp": sp, "dp": lax.rem(y + d + NY, NY) * 2 + c}

    mate = {"sp": sp, "dp": y * 2 + (1 - c)}

    def remote(src, dst, ssem, rsem, dev):
        return pltpu.make_async_remote_copy(
            src_ref=src, dst_ref=dst, send_sem=ssem, recv_sem=rsem,
            device_id=dev, device_id_type=MESH,
        )

    barrier = pltpu.get_barrier_semaphore()
    peers = [xdev(d) for d in range(1, NX)] + [ydev(1), ydev(-1), mate]
    for dev in peers:
        pl.semaphore_signal(barrier, inc=1, device_id=dev, device_id_type=MESH)
    for d in range(1, NZ):

        @pl.when(z + d < NZ)
        def _():
            dev = zat(lax.rem(z + d, NZ))
            pl.semaphore_signal(barrier, inc=1, device_id=dev, device_id_type=MESH)

    loads = [
        (i_hbm, iv, 0), (f_hbm, fv, 1), (k_hbm, kv, 2), (v_hbm, vv, 2), (w_hbm, wall.at[c, 0], 2), (q_hbm, qv, 2),
        (c_hbm, cv, 3), (n_hbm, nv, 4), (level_hbm, level, 5), (gain_hbm, gain, 6),
    ]
    for src, dst, k in loads:
        pltpu.make_async_copy(src, dst, lsem.at[k]).start()

    rows64 = lax.broadcasted_iota(jnp.int32, (T, T), 0)
    cols64 = lax.broadcasted_iota(jnp.int32, (T, T), 1)
    upper = jnp.where(rows64 <= cols64, 1.0, 0.0).astype(F32)
    causal = rows64 >= cols64

    def gates(li, f):
        li, f = li.astype(F32), f.astype(F32)
        lf = jnp.minimum(f, 0.0) - jnp.log1p(jnp.exp(-jnp.abs(f)))
        b = jnp.dot(lf, upper, precision=lax.Precision.HIGHEST, preferred_element_type=F32)
        return li - b, b[:, T - 1 : T]

    def arrived(ref, sem):
        pltpu.make_async_copy(ref, ref, sem).wait()

    with jax.named_scope("loads"):
        arrived(iv, lsem.at[0])
        arrived(fv, lsem.at[1])
    for j in range(S):
        a, _ = gates(iv[j], fv[j])
        a_loc[8 * j : 8 * j + 8, :] = a

    def block_gates(p, li, f):
        a, e = gates(li, f)
        am = jnp.max(a, axis=1, keepdims=True)
        esum[p] = jnp.broadcast_to(e, (H, D))
        amax[p] = jnp.broadcast_to(am, (H, D))
        wrow[p] = jnp.exp(a - am)

    block_gates(x, iv[x], fv[x])
    arrived(wall.at[c, 0:4], lsem.at[2])
    for k, ref in ((3, cv), (4, nv), (5, level), (6, gain)):
        arrived(ref, lsem.at[k])
    cx[x] = cv[x]
    nx[x] = nv[x]

    with jax.named_scope("barrier"):
        pl.semaphore_wait(barrier, len(peers) + z)
    for d in range(1, NZ):

        @pl.when(z >= d)
        def _():
            dev = zat(lax.rem(z - d + NZ, NZ))
            pl.semaphore_signal(hello, inc=1, device_id=dev, device_id_type=MESH)

    def rows_of(side, kind):
        if kind == "b":
            return pl.ds(pl.multiple_of(RA + RB * x, RB), RB)
        if kind == "half":
            return pl.ds(pl.multiple_of(RA + RB * x + side * (RB // 2), RB // 2), RB // 2)
        if kind == "cut":
            return pl.ds(256 + 128 * side, 128)
        return pl.ds(256 * (2 - kind if side else kind), 256)

    ring = [(0, "b"), (0, 0), (1, "b"), (0, 1), (2, "b"), (0, 2), (3, "half")]
    ring += [(1, 0), (1, 1), (1, 2), (2, 0), (2, 1), (2, 2), (3, 0), (3, "cut")]
    onward = {(0, "b"): (1, "b"), (1, "b"): (2, "b"), (2, "b"): (3, "half"), (2, 1): (3, "cut")}
    for k in range(3):
        onward[0, k], onward[1, k] = (1, k), (2, k)
    onward[2, 0] = (3, 0)

    def wsend(side, item):
        level, kind = item
        k = ring.index(item)
        rows = rows_of(side, kind)
        src, dst = (level, level + 1) if side else ((NY - level) % NY, NY - 1 - level)
        return remote(
            wall.at[c, src, rows], wall.at[c, dst, rows],
            sent.at[12], wy_r.at[k], ydev(-1 if side else 1),
        )

    def wmate(side, item):
        level, kind = item
        ref = wall.at[c, level + 1 if side else NY - 1 - level, rows_of(side, kind)]
        return remote(ref, ref, sent.at[13], wd_r.at[max(0, level - 1)], mate)

    def serve(level, kind):
        item = (level, kind)
        count = {"b": RB, "half": RB // 2, "cut": 128}.get(kind, 256)
        with jax.named_scope(f"serve{level}{kind}"):
            arrived(wall.at[c, 0:2, 0:count], wy_r.at[ring.index(item)])
        for side in (0, 1):
            if item in onward:
                wsend(side, onward[item]).start()
            if kind not in ("b", "half"):
                wmate(side, item).start()

    def begin(level, kind):
        for side in (0, 1):
            wsend(side, (level, kind)).start()

    def wspread(d):
        rows = pl.ds(pl.multiple_of(RA + RB * x, RB), RB)
        ref = wall.at[c, 1:NY, rows]
        return remote(ref, ref, sent.at[14], ws_r.at[0], xdev(d))

    def wrest():
        ref = wall.at[c, 1:NY, RA:1024]
        return remote(ref, ref, sent.at[15], ws_r.at[2], mate)

    small = [(iv, ix), (fv, fx), (cv, cx), (nv, nx)]

    def xsmall(d):
        p = lax.rem(x + d, NX)
        return [
            remote(src.at[p], dst.at[x], sent.at[k], xs_r.at[k], xdev(d)) for k, (src, dst) in enumerate(small)
        ]

    def xkeys(d, g):
        p = lax.rem(x + d, NX)
        heads = pl.ds(g * HG, HG)
        return [
            remote(src.at[p, heads], dst.at[x, heads], sent.at[4], xk_r.at[k, g], xdev(d))
            for k, (src, dst) in enumerate([(kv, kx), (vv, vx)])
        ]

    begin(0, "b")
    begin(0, 0)
    for d in (2, 1, 3):
        for copy in xsmall(d):
            copy.start()
    for g in range(G):
        for d in (2, 1, 3):
            for copy in xkeys(d, g):
                copy.start()
    remote(wall.at[c, 0], wall.at[c, 0], sent.at[15], wo_r.at[0], mate).start()

    def intra(i):
        j, h = lax.div(i, H), lax.rem(i, H)
        arow = a_loc[pl.ds(i, 1), :]
        masked = jnp.where(causal, jnp.broadcast_to(arow, (T, T)), NEG)
        top = jnp.max(masked, axis=1, keepdims=True)
        weight = jnp.exp(masked - top)
        scores = nt(qv[j, h], kv[j, h]) * FACTOR * weight
        den_s[i] = jnp.broadcast_to(jnp.sum(scores, axis=1, keepdims=True), (T, D))
        amx_s[i] = jnp.broadcast_to(top, (T, D))
        num_s[i] = jnp.dot(scores.astype(BF16), vv[j, h], preferred_element_type=F32)

    def inner(part):
        def body(i, _):
            for u in range(4):
                intra(part * 8 + i * 4 + u)
            return 0

        with jax.named_scope("intra"):
            lax.fori_loop(0, 2, body, 0)

    def state(p, h, keys, values):
        w = wrow[p, pl.ds(h, 1), :]
        vt = values[p, h].astype(F32).T
        hi = w.astype(BF16)
        lo = (w - hi.astype(F32)).astype(BF16)
        rid = lax.broadcasted_iota(jnp.int32, (16, T), 0)
        extra = jnp.where(
            rid == 0,
            jnp.broadcast_to(hi.astype(F32), (16, T)),
            jnp.where(rid == 1, jnp.broadcast_to(lo.astype(F32), (16, T)), 0.0),
        )
        lhs = jnp.concatenate([(vt * w).astype(BF16), extra.astype(BF16)], axis=0)
        st = jnp.dot(lhs, keys[p, h], preferred_element_type=F32)
        kvs[p, h] = st[0:D]
        nkv[p, pl.ds(h, 1), :] = st[D : D + 1] + st[D + 1 : D + 2]

    def states(p, g):
        with jax.named_scope("states"):
            for u in range(HG):
                state(p, g * HG + u, kx, vx)

    inner(0)

    def own(i, _):
        for u in range(4):
            state(x, i * 4 + u, kv, vv)
        return 0

    lax.fori_loop(0, 2, own, 0)
    serve(0, "b")
    begin(0, 1)
    with jax.named_scope("xgates"):
        for k, (src, dst) in enumerate(small):
            arrived(dst.at[0:3], xs_r.at[k])
        for d in (1, 3, 2):
            p = lax.rem(x - d + NX, NX)
            block_gates(p, ix[p], fx[p])

    shift = []
    before = jnp.zeros((H, D), F32)
    top = None
    for i in range(NX):
        a = amax[i] - before
        shift.append(a)
        top = a if top is None else jnp.maximum(top, a)
        before = before + esum[i]
    scale = [jnp.exp(a - top) for a in shift]

    half = jnp.minimum(lax.div(z, FEW), 1)

    def tz(h):
        p = rev(h)
        d = lax.rem(p - z + NZ, NZ)
        return d, [
            remote(tm_send.at[h], tm_recv.at[z], sent.at[5], tz_r.at[0, half], zat(p)),
            remote(t_send.at[h], t_recv.at[z], sent.at[6], tz_r.at[1, half], zat(p)),
        ]

    def total(g):
        with jax.named_scope(f"xin{g}"):
            for k, ref in enumerate((kx, vx)):
                arrived(ref.at[0:3, 0:HG], xk_r.at[k, g])
        for d in (1, 3, 2):
            states(lax.rem(x - d + NX, NX), g)
        for h in range(g * HG, g * HG + HG):
            ntot = sum(scale[i][h : h + 1] * nkv[i, h : h + 1, :] for i in range(NX))
            t_send[h] = sum(scale[i][h : h + 1] * kvs[i, h] for i in range(NX)).astype(BF16)
            tm_send[h, 0:1, :] = ntot
            tm_send[h, 1:2, :] = before[h : h + 1]
            tm_send[h, 2:3, :] = top[h : h + 1]

    def total_send(g):
        for h in range(g * HG, g * HG + HG):
            d, copies = tz(h)

            @pl.when(d != 0)
            def _():
                for copy in copies:
                    copy.start()

    def cz(d):
        p = lax.rem(z + d, NZ)
        h = lax.rem(p, 2) * 4 + lax.rem(lax.div(p, 2), 2) * 2 + lax.div(p, 4)
        return remote(cz_send.at[h], cz_recv.at[z], sent.at[7], tz_r.at[2, 0], zat(p))

    for i in range(NX):
        turn[4 * i : 4 * i + 4, 0:H] = nx[i]
        for h in range(H):
            cz_send[h, 4 * i : 4 * i + 4, :] = cx[i, 4 * h : 4 * h + 4, :]
    first_lanes = lax.broadcasted_iota(jnp.int32, (H, D), 1) < 4 * NX
    nfirst = jnp.where(first_lanes, turn[...].T[0:H], 0.0)
    for h in range(H):
        cz_send[h, 16:17, :] = nfirst[h : h + 1]

    group = lax.div(mine, HG)

    def scan_states(low, high, cur, nrow, m):
        for i in range(low, high):
            p_send[i] = cur.astype(BF16)
            pm_send[i, 0:1, :] = nrow
            pm_send[i, 1:2, :] = m
            if i == FEW:
                held[...] = cur
                held_n[0:1, :] = nrow
                held_n[1:2, :] = m
            if i < high - 1:
                cur, nrow, m = scan_step(i, cur, nrow, m)
        for p in range(low, high):

            @pl.when(z != p)
            def _():
                remote(pm_send.at[p], pm_recv.at[mine], sent.at[8], pz_r.at[0, group], zat(p)).start()
                remote(p_send.at[p], p_recv.at[mine], sent.at[9], pz_r.at[1, group], zat(p)).start()

            @pl.when(z == p)
            def _():
                p_recv[mine] = p_send[p]
                pm_recv[mine] = pm_send[p]

    def scan_step(i, cur, nrow, m):
        am = tm_recv[i, 2:3, :]
        hi = jnp.maximum(m, am)
        keep, add = jnp.exp(m - hi), jnp.exp(am - hi)
        cur = keep * cur + add * t_recv[i].astype(F32)
        nrow = keep * nrow + add * tm_recv[i, 0:1, :]
        return cur, nrow, tm_recv[i, 1:2, :] + hi

    def totals_wait(k, count):
        @pl.when(half == k)
        def _():
            arrived(tm_recv.at[0 : count - 1], tz_r.at[0, k])
            arrived(t_recv.at[0 : count - 1], tz_r.at[1, k])

        @pl.when(half != k)
        def _():
            arrived(tm_recv.at[0:count], tz_r.at[0, k])
            arrived(t_recv.at[0:count], tz_r.at[1, k])

    def scan_low(g):
        @pl.when(group == g)
        def _():
            with jax.named_scope(f"zlow{g}"):
                arrived(cz_recv.at[0 : NZ - 1], tz_r.at[2, 0])
                totals_wait(0, FEW)
            with jax.named_scope("scan"):
                t_recv[z] = t_send[mine]
                tm_recv[z] = tm_send[mine]
                cz_recv[z] = cz_send[mine]
                lanes = lax.broadcasted_iota(jnp.int32, (1, H), 1)
                m = jnp.sum(jnp.where(lanes == mine, level[pl.ds(x, 1), :], 0.0), axis=1, keepdims=True)
                m = jnp.broadcast_to(m, (1, D))
                nrow = cz_recv[0, 16:17, :]
                for i in range(1, NZ):
                    nrow = nrow + pltpu.roll(cz_recv[i, 16:17, :], 4 * NX * i, 1)
                cur = jnp.concatenate([cz_recv[i, 0:16, :] for i in range(NZ)], axis=0).T
                scan_states(0, FEW + 1, cur, nrow, m)

    def scan_high(g):
        @pl.when(group == g)
        def _():
            with jax.named_scope(f"zhigh{g}"):
                totals_wait(1, NZ - FEW)
            with jax.named_scope("scan"):
                state = scan_step(FEW, held[...], held_n[0:1, :], held_n[1:2, :])
                scan_states(FEW + 1, NZ, *state)

    def xo(d, g):
        p = lax.rem(x + d, NX)
        heads = pl.ds(g * HG, HG)
        return [
            remote(bm_send.at[p, g], bm_recv.at[x, g], sent.at[10], xo_r.at[0, g], xdev(d)),
            remote(b_send.at[p, heads], b_recv.at[x, heads], sent.at[11], xo_r.at[1, g], xdev(d)),
        ]

    def spread(g):
        with jax.named_scope(f"zout{g}"):

            @pl.when(group == g)
            def _():
                for k, ref in enumerate((pm_recv, p_recv)):
                    arrived(ref.at[0 : HG - 1], pz_r.at[k, g])

            @pl.when(group != g)
            def _():
                for k, ref in enumerate((pm_recv, p_recv)):
                    arrived(ref.at[0:HG], pz_r.at[k, g])

        for u in range(HG):
            h = g * HG + u
            cur = p_recv[h].astype(F32)
            nrow = pm_recv[h, 0:1, :]
            m = pm_recv[h, 1:2, :]
            for i in range(NX):
                b_send[i, h] = cur.astype(BF16)
                bm_send[i, g, 2 * u : 2 * u + 1, :] = nrow
                bm_send[i, g, 2 * u + 1 : 2 * u + 2, :] = m
                if i < NX - 1:
                    am = amax[i, h : h + 1, :]
                    hi = jnp.maximum(m, am)
                    keep, add = jnp.exp(m - hi), jnp.exp(am - hi)
                    cur = keep * cur + add * kvs[i, h]
                    nrow = keep * nrow + add * nkv[i, h : h + 1, :]
                    m = esum[i, h : h + 1, :] + hi
        for d in (2, 1, 3):
            for copy in xo(d, g):
                copy.start()
        heads = pl.ds(g * HG, HG)
        b_recv[x, heads] = b_send[x, heads]
        bm_recv[x, g] = bm_send[x, g]

    def finish_one(j, g):
        for u in range(HG):
            h = g * HG + u
            i = j * H + h
            q = qv[j, h]
            nrow = bm_recv[j, g, 2 * u : 2 * u + 1, :]
            m = bm_recv[j, g, 2 * u + 1 : 2 * u + 2, :]
            qc = nt(q, b_recv[j, h])
            qn = jnp.sum(q.astype(F32) * nrow, axis=1, keepdims=True)
            a = amx_s[i]
            hi = jnp.maximum(a, m)
            keep, add = jnp.exp(m - hi) * FACTOR, jnp.exp(a - hi)
            den = add * den_s[i] + keep * qn
            num = add * num_s[i] + keep * qc
            o = (num / jnp.maximum(jnp.abs(den), 1.0)).astype(BF16)
            normed = (o.astype(F32) * gain[h : h + 1, :]).astype(BF16)
            hid[pl.ds(pl.multiple_of(j * T, T), T), h * D : h * D + D] = normed

    def finish(g):
        with jax.named_scope("finish"):
            finish_one(x, g)
        with jax.named_scope(f"xout{g}"):
            arrived(bm_recv.at[0:3, 0], xo_r.at[0, g])
            arrived(b_recv.at[0:3, 0:HG], xo_r.at[1, g])
        with jax.named_scope("finish"):
            for d in (1, 3, 2):
                finish_one(lax.rem(x - d + NX, NX), g)

    def columns(core, r):
        block = lax.rem(y + r, NY) * 2 + core
        return pl.ds(pl.multiple_of(block * 256, 256), 256)

    def early_one(r):
        for core in (0, 1):
            acc[core, r] = jnp.dot(hid[:, 0:RA], wall[core, r, 0:RA], preferred_element_type=F32)

    def late_one(r):
        for core in (0, 1):
            part = jnp.dot(hid[:, RA:1024], wall[core, r, RA:1024], preferred_element_type=F32)
            out[:, columns(core, r)] = (acc[core, r] + part).astype(BF16)

    def twos(name, fn, low, high):
        def body(i, _):
            fn(lax.rem(NY - 2 + 2 * i, NY))
            fn(lax.rem(NY - 1 + 2 * i, NY))
            return 0

        with jax.named_scope(name):
            lax.fori_loop(low, high, body, 0)

    def last():
        with jax.named_scope("last"):
            for core in (0, 1):
                whole = jnp.dot(hid[...], wall[core, NY // 2], preferred_element_type=F32)
                out[:, columns(core, NY // 2)] = whole.astype(BF16)

    def mates(level):
        with jax.named_scope("mate"):
            count = (4, 2, 1)[level]
            arrived(wall.at[c, 0:count, 0:RA], wd_r.at[level])

    def zgate():
        with jax.named_scope("zgate"):

            @pl.when(z < NZ - 1)
            def _():
                pl.semaphore_wait(hello, NZ - 1 - z)

    def cz_all():
        for d in (4, 3, 5, 2, 6, 1, 7):
            cz(d).start()

    def wspread_start():
        for d in (2, 1, 3):
            wspread(d).start()

    def wspread_done():
        with jax.named_scope("wspread"):
            arrived(wall.at[c, 1:NY, 0 : 3 * RB], ws_r.at[0])
        wrest().start()

    def sent_cell():
        for k, ref in enumerate((iv, fv, cv, nv)):
            arrived(ref.at[0:3], sent.at[k])
        arrived(b_send.at[0:3], sent.at[4])
        for k, ref in ((5, tm_send), (6, t_send), (7, cz_send), (8, pm_send), (9, p_send)):
            arrived(ref.at[0 : NZ - 1], sent.at[k])
        arrived(wall.at[c, 1:NY, 0 : 3 * RB], sent.at[14])

    def sent_rest():
        arrived(bm_send.at[0:3], sent.at[10])
        arrived(b_send.at[0:3], sent.at[11])
        arrived(wall.at[c, :, 0:352], sent.at[15])

    def sent_ring():
        arrived(wall.at[c, 1:NY, 0:832], sent.at[12])
        arrived(wall.at[c, 1:NY, 0:768], sent.at[13])

    @pl.when(z >= NZ // 2)
    def _():
        zgate()
        cz_all()

    inner(1)
    serve(1, "b")
    begin(0, 2)
    total(0)

    @pl.when(z < NZ // 2)
    def _():
        inner(2)
        total(1)
        zgate()
        cz_all()
        total_send(0)
        total_send(1)
        serve(2, "b")
        serve(0, 0)
        serve(0, 1)
        inner(3)
        total(2)
        total_send(2)
        serve(3, "half")
        wspread_start()
        serve(0, 2)
        total(3)
        total_send(3)
        scan_low(0)
        scan_low(1)
        serve(1, 0)
        scan_low(2)
        scan_low(3)
        scan_high(0)
        serve(1, 1)
        scan_high(1)
        spread(0)
        serve(1, 2)
        scan_high(2)
        scan_high(3)
        spread(1)
        serve(2, 0)
        spread(2)
        wspread_done()
        finish(0)
        serve(2, 1)
        spread(3)
        arrived(wall.at[c, 0], wo_r.at[0])
        sent_cell()
        finish(1)
        mates(0)
        serve(2, 2)
        finish(2)
        twos("early", early_one, 0, 2)
        serve(3, 0)
        mates(1)
        with jax.named_scope("early"):
            early_one(2)
            early_one(3)
            early_one(5)
        serve(3, "cut")
        finish(3)

    @pl.when(z >= NZ // 2)
    def _():
        total_send(0)
        inner(2)
        total(1)
        total_send(1)
        serve(2, "b")
        serve(0, 0)
        serve(0, 1)
        inner(3)
        scan_low(0)
        total(2)
        total_send(2)
        serve(3, "half")
        wspread_start()
        scan_low(1)
        scan_high(0)
        serve(0, 2)
        total(3)
        total_send(3)
        scan_low(2)
        scan_high(1)
        serve(1, 0)
        scan_low(3)
        spread(0)
        scan_high(2)
        serve(1, 1)
        scan_high(3)
        spread(1)
        serve(1, 2)
        spread(2)
        serve(2, 0)
        finish(0)
        spread(3)
        wspread_done()
        serve(2, 1)
        finish(1)
        arrived(wall.at[c, 0], wo_r.at[0])
        mates(0)
        serve(2, 2)
        finish(2)
        twos("early", early_one, 0, 2)
        sent_cell()
        serve(3, 0)
        mates(1)
        with jax.named_scope("early"):
            early_one(2)
            early_one(3)
            early_one(5)
        finish(3)
        serve(3, "cut")

    arrived(wall.at[c, 1:NY, RA:1024], ws_r.at[2])
    twos("late", late_one, 0, 3)
    with jax.named_scope("late"):
        late_one(5)
    sent_rest()
    mates(2)
    last()
    sent_ring()


def on_device(queries, keys, values, input_gate, forget_gate, start_memory, start_norm, start_level, head_gain, out_weight):
    arrays = (
        input_gate, forget_gate, queries, keys, values, start_memory.reshape(S, 32, D),
        jnp.transpose(start_norm, (0, 2, 1)), out_weight, start_level, head_gain,
    )
    dma, vmem = pltpu.SemaphoreType.DMA, pltpu.VMEM
    out = pl.pallas_call(
        kernel,
        out_shape=pltpu.VMEM((S * T, 4096), BF16),
        in_specs=[pl.BlockSpec(memory_space=pltpu.HBM)] * len(arrays),
        out_specs=pl.BlockSpec(memory_space=pltpu.VMEM),
        scratch_shapes=[
            vmem((S, H, T, D), BF16), vmem((S, H, T, D), BF16), vmem((S, H, T, D), BF16),
            vmem((S, H, T), BF16), vmem((S, H, T), BF16), vmem((S, 32, D), F32), vmem((S, 4, H), F32),
            vmem((NX, H, T, D), BF16), vmem((NX, H, T, D), BF16),
            vmem((NX, H, T), BF16), vmem((NX, H, T), BF16), vmem((NX, 32, D), F32), vmem((NX, 4, H), F32),
            vmem((S, H), F32), vmem((H, D), F32),
            vmem((2, NY, 1024, 256), BF16),
            vmem((S * H, T), F32),
            vmem((S * H, T, D), F32), vmem((S * H, T, D), F32), vmem((S * H, T, D), F32),
            vmem((NX, H, T), F32), vmem((NX, H, D), F32), vmem((NX, H, D), F32),
            vmem((NX, H, D, D), F32), vmem((NX, H, D), F32), vmem((D, D), F32),
            vmem((H, 24, D), F32), vmem((NZ, 24, D), F32), vmem((D, D), F32), vmem((8, D), F32),
            vmem((H, D, D), BF16), vmem((NZ, D, D), BF16),
            vmem((H, 8, D), F32), vmem((NZ, 8, D), F32),
            vmem((NZ, D, D), BF16), vmem((H, D, D), BF16),
            vmem((NZ, 8, D), F32), vmem((H, 8, D), F32),
            vmem((NX, H, D, D), BF16), vmem((S, H, D, D), BF16),
            vmem((NX, G, 8, D), F32), vmem((S, G, 8, D), F32),
            vmem((S * T, H * D), BF16), vmem((2, NY, S * T, 256), F32),
            dma((7,)), dma((16,)), dma((4,)), dma((2, G)), dma((3, 2)), dma((2, G)), dma((2, G)),
            dma((15,)), dma((3,)), dma((3,)), dma((1,)), pltpu.SemaphoreType.REGULAR,
        ],
        compiler_params=pltpu.CompilerParams(
            collective_id=0, has_side_effects=True, vmem_limit_bytes=50_000_000
        ),
        name="cell_layer",
    )(*(pltpu.with_memory_space_constraint(array, pltpu.HBM) for array in arrays))
    return out.reshape(S, T, 4096)


def solution(mesh):
    return jax.shard_map(
        on_device,
        mesh=mesh,
        in_specs=(
            P("dp", None, "sp", None),
            P("dp", None, "sp", None),
            P("dp", None, "sp", None),
            P("dp", None, "sp"),
            P("dp", None, "sp"),
            P("dp", None, "sp", None),
            P("dp", None, "sp"),
            P("dp", None),
            P(),
            P(None, "dp"),
        ),
        out_specs=P("dp", "sp", None),
        check_vma=False,
    )
```

```python
import jax
import jax.numpy as jnp
from jax import lax
from jax.experimental import pallas as pl
from jax.experimental.pallas import tpu as pltpu
from jax.sharding import PartitionSpec as P

MESH = pl.DeviceIdType.MESH
F32 = jnp.float32
BF16 = jnp.bfloat16
S, H, T, D = 4, 8, 64, 128
NX, NZ, NY = 4, 8, 8
FACTOR = D**-0.5
NEG = -1e30
G = 4
HG = H // G
RA = 768
RB = (1024 - RA) // NX


def nt(a, b):
    return lax.dot_general(a, b, (((1,), (1,)), ((), ())), preferred_element_type=F32)


def kernel(
    i_hbm, f_hbm, q_hbm, k_hbm, v_hbm, c_hbm, n_hbm, w_hbm, level_hbm, gain_hbm, out,
    qv, kv, vv, iv, fv, cv, nv, kx, vx, ix, fx, cx, nx, level, gain, wall, a_loc, num_s, den_s, amx_s,
    wrow, esum, amax, kvs, nkv, turn, cz_send, cz_recv, nz_send, nz_recv, first_c, first_n, tot, ntot,
    p_send, p_recv, pm_send, pm_recv, b_send, b_recv, bm_send, bm_recv, hid, acc,
    lsem, sent, xs_r, xk_r, tz_r, pz_r, xo_r, wy_r, wd_r, ws_r, wo_r, hello, hello_next,
):
    sp = lax.axis_index("sp")
    dp = lax.axis_index("dp")
    x, z = lax.rem(sp, NX), lax.div(sp, NX)
    y, c = lax.div(dp, 2), lax.rem(dp, 2)
    def xdev(d):
        return {"sp": z * NX + lax.rem(x + d, NX), "dp": dp}

    def zat(p):
        return {"sp": p * NX + x, "dp": dp}

    def ydev(d):
        return {"sp": sp, "dp": lax.rem(y + d + NY, NY) * 2 + c}

    mate = {"sp": sp, "dp": y * 2 + (1 - c)}

    def remote(src, dst, ssem, rsem, dev):
        return pltpu.make_async_remote_copy(
            src_ref=src, dst_ref=dst, send_sem=ssem, recv_sem=rsem,
            device_id=dev, device_id_type=MESH,
        )

    barrier = pltpu.get_barrier_semaphore()
    peers = [xdev(d) for d in range(1, NX)] + [ydev(1), ydev(-1), mate]
    for dev in peers:
        pl.semaphore_signal(barrier, inc=1, device_id=dev, device_id_type=MESH)
    for d in range(1, NZ):

        @pl.when(z + d < NZ)
        def _():
            dev = zat(lax.rem(z + d, NZ))
            pl.semaphore_signal(barrier, inc=1, device_id=dev, device_id_type=MESH)

    loads = [
        (i_hbm, iv, 0), (f_hbm, fv, 1), (k_hbm, kv, 2), (v_hbm, vv, 2), (w_hbm, wall.at[c, 0], 2), (q_hbm, qv, 2),
        (c_hbm, cv, 3), (n_hbm, nv, 4), (level_hbm, level, 5), (gain_hbm, gain, 6),
    ]
    for src, dst, k in loads:
        pltpu.make_async_copy(src, dst, lsem.at[k]).start()

    rows64 = lax.broadcasted_iota(jnp.int32, (T, T), 0)
    cols64 = lax.broadcasted_iota(jnp.int32, (T, T), 1)
    upper = jnp.where(rows64 <= cols64, 1.0, 0.0).astype(F32)
    causal = rows64 >= cols64

    def gates(li, f):
        li, f = li.astype(F32), f.astype(F32)
        lf = jnp.minimum(f, 0.0) - jnp.log1p(jnp.exp(-jnp.abs(f)))
        b = jnp.dot(lf, upper, precision=lax.Precision.HIGHEST, preferred_element_type=F32)
        return li - b, b[:, T - 1 : T]

    def arrived(ref, sem):
        pltpu.make_async_copy(ref, ref, sem).wait()

    with jax.named_scope("loads"):
        arrived(iv, lsem.at[0])
        arrived(fv, lsem.at[1])
    for j in range(S):
        a, _ = gates(iv[j], fv[j])
        a_loc[8 * j : 8 * j + 8, :] = a

    def block_gates(p, li, f):
        a, e = gates(li, f)
        am = jnp.max(a, axis=1, keepdims=True)
        esum[p] = jnp.broadcast_to(e, (H, D))
        amax[p] = jnp.broadcast_to(am, (H, D))
        wrow[p] = jnp.exp(a - am)

    block_gates(x, iv[x], fv[x])
    arrived(wall.at[c, 0:4], lsem.at[2])
    for k, ref in ((3, cv), (4, nv), (5, level), (6, gain)):
        arrived(ref, lsem.at[k])
    cx[x] = cv[x]
    nx[x] = nv[x]

    with jax.named_scope("barrier"):
        pl.semaphore_wait(barrier, len(peers) + z)
    for d in range(1, NZ):

        @pl.when(z >= d)
        def _():
            dev = zat(lax.rem(z - d + NZ, NZ))
            pl.semaphore_signal(hello, inc=1, device_id=dev, device_id_type=MESH)
            if d == 1:
                pl.semaphore_signal(hello_next, inc=1, device_id=dev, device_id_type=MESH)

    def rows_of(side, kind):
        if kind == "b":
            return pl.ds(pl.multiple_of(RA + RB * x, RB), RB)
        if kind == "half":
            return pl.ds(pl.multiple_of(RA + RB * x + side * (RB // 2), RB // 2), RB // 2)
        if kind == "cut":
            return pl.ds(256 + 128 * side, 128)
        return pl.ds(256 * (2 - kind if side else kind), 256)

    ring = [(0, "b"), (0, 0), (1, "b"), (0, 1), (2, "b"), (0, 2), (3, "half")]
    ring += [(1, 0), (1, 1), (1, 2), (2, 0), (2, 1), (2, 2), (3, 0), (3, "cut")]
    onward = {(0, "b"): (1, "b"), (1, "b"): (2, "b"), (2, "b"): (3, "half"), (2, 1): (3, "cut")}
    for k in range(3):
        onward[0, k], onward[1, k] = (1, k), (2, k)
    onward[2, 0] = (3, 0)

    def wsend(side, item):
        level, kind = item
        k = ring.index(item)
        rows = rows_of(side, kind)
        src, dst = (level, level + 1) if side else ((NY - level) % NY, NY - 1 - level)
        return remote(
            wall.at[c, src, rows], wall.at[c, dst, rows],
            sent.at[12], wy_r.at[k], ydev(-1 if side else 1),
        )

    def wmate(side, item):
        level, kind = item
        ref = wall.at[c, level + 1 if side else NY - 1 - level, rows_of(side, kind)]
        return remote(ref, ref, sent.at[13], wd_r.at[max(0, level - 1)], mate)

    def serve(level, kind):
        item = (level, kind)
        count = {"b": RB, "half": RB // 2, "cut": 128}.get(kind, 256)
        with jax.named_scope(f"serve{level}{kind}"):
            arrived(wall.at[c, 0:2, 0:count], wy_r.at[ring.index(item)])
        for side in (0, 1):
            if item in onward:
                wsend(side, onward[item]).start()
            if kind not in ("b", "half"):
                wmate(side, item).start()

    def begin(level, kind):
        for side in (0, 1):
            wsend(side, (level, kind)).start()

    def wspread(d):
        rows = pl.ds(pl.multiple_of(RA + RB * x, RB), RB)
        ref = wall.at[c, 1:NY, rows]
        return remote(ref, ref, sent.at[14], ws_r.at[0], xdev(d))

    def wrest():
        ref = wall.at[c, 1:NY, RA:1024]
        return remote(ref, ref, sent.at[15], ws_r.at[2], mate)

    small = [(iv, ix), (fv, fx), (cv, cx), (nv, nx)]

    def xsmall(d):
        p = lax.rem(x + d, NX)
        return [
            remote(src.at[p], dst.at[x], sent.at[k], xs_r.at[k], xdev(d)) for k, (src, dst) in enumerate(small)
        ]

    def xkeys(d, g):
        p = lax.rem(x + d, NX)
        heads = pl.ds(g * HG, HG)
        return [
            remote(src.at[p, heads], dst.at[x, heads], sent.at[4], xk_r.at[k, g], xdev(d))
            for k, (src, dst) in enumerate([(kv, kx), (vv, vx)])
        ]

    begin(0, "b")
    begin(0, 0)
    for d in (2, 1, 3):
        for copy in xsmall(d):
            copy.start()
    for g in range(G):
        for d in (2, 1, 3):
            for copy in xkeys(d, g):
                copy.start()
    remote(wall.at[c, 0], wall.at[c, 0], sent.at[15], wo_r.at[0], mate).start()

    def intra(i):
        j, h = lax.div(i, H), lax.rem(i, H)
        arow = a_loc[pl.ds(i, 1), :]
        masked = jnp.where(causal, jnp.broadcast_to(arow, (T, T)), NEG)
        top = jnp.max(masked, axis=1, keepdims=True)
        weight = jnp.exp(masked - top)
        scores = nt(qv[j, h], kv[j, h]) * FACTOR * weight
        den_s[i] = jnp.broadcast_to(jnp.sum(scores, axis=1, keepdims=True), (T, D))
        amx_s[i] = jnp.broadcast_to(top, (T, D))
        num_s[i] = jnp.dot(scores.astype(BF16), vv[j, h], preferred_element_type=F32)

    def inner(part):
        def body(i, _):
            for u in range(4):
                intra(part * 8 + i * 4 + u)
            return 0

        with jax.named_scope("intra"):
            lax.fori_loop(0, 2, body, 0)

    def state(p, h, keys, values):
        w = wrow[p, pl.ds(h, 1), :]
        vt = values[p, h].astype(F32).T
        hi = w.astype(BF16)
        lo = (w - hi.astype(F32)).astype(BF16)
        rid = lax.broadcasted_iota(jnp.int32, (16, T), 0)
        extra = jnp.where(
            rid == 0,
            jnp.broadcast_to(hi.astype(F32), (16, T)),
            jnp.where(rid == 1, jnp.broadcast_to(lo.astype(F32), (16, T)), 0.0),
        )
        lhs = jnp.concatenate([(vt * w).astype(BF16), extra.astype(BF16)], axis=0)
        st = jnp.dot(lhs, keys[p, h], preferred_element_type=F32)
        kvs[p, h] = st[0:D]
        nkv[p, pl.ds(h, 1), :] = st[D : D + 1] + st[D + 1 : D + 2]

    def states(p, g):
        with jax.named_scope("states"):
            for u in range(HG):
                state(p, g * HG + u, kx, vx)

    inner(0)

    def own(i, _):
        for u in range(4):
            state(x, i * 4 + u, kv, vv)
        return 0

    lax.fori_loop(0, 2, own, 0)
    serve(0, "b")
    begin(0, 1)
    with jax.named_scope("xgates"):
        for k, (src, dst) in enumerate(small):
            arrived(dst.at[0:3], xs_r.at[k])
        for d in (1, 3, 2):
            p = lax.rem(x - d + NX, NX)
            block_gates(p, ix[p], fx[p])

    shift = []
    before = jnp.zeros((H, D), F32)
    top = None
    for i in range(NX):
        a = amax[i] - before
        shift.append(a)
        top = a if top is None else jnp.maximum(top, a)
        before = before + esum[i]
    scale = [jnp.exp(a - top) for a in shift]

    lanes = lax.broadcasted_iota(jnp.int32, (1, H), 1)

    def total(g):
        with jax.named_scope(f"xin{g}"):
            for k, ref in enumerate((kx, vx)):
                arrived(ref.at[0:3, 0:HG], xk_r.at[k, g])
        for d in (1, 3, 2):
            states(lax.rem(x - d + NX, NX), g)
        for h in range(g * HG, g * HG + HG):
            ntot[h : h + 1, :] = sum(scale[i][h : h + 1] * nkv[i, h : h + 1, :] for i in range(NX))
            tot[h] = sum(scale[i][h : h + 1] * kvs[i, h] for i in range(NX))

    def cz(d):
        p = lax.rem(z + d, NZ)
        return [
            remote(cz_send, cz_recv.at[z], sent.at[5], tz_r.at[0], zat(p)),
            remote(nz_send, nz_recv.at[z], sent.at[6], tz_r.at[1], zat(p)),
        ]

    for i in range(NX):
        turn[4 * i : 4 * i + 4, 0:H] = nx[i]
        for h in range(H):
            turn[16 + 16 * h + 4 * i : 20 + 16 * h + 4 * i, :] = cx[i, 4 * h : 4 * h + 4, :]
    first_lanes = lax.broadcasted_iota(jnp.int32, (H, D), 1) < 4 * NX
    nz_send[...] = jnp.where(first_lanes, turn[0:D, :].T[0:H], 0.0)
    for h in range(H):
        cz_send[h] = turn[16 + 16 * h : 32 + 16 * h, :].astype(BF16)

    def pz(h):
        return [
            remote(pm_send.at[h], pm_recv.at[h], sent.at[8], pz_r.at[0, h], zat(lax.rem(z + 1, NZ))),
            remote(p_send.at[h], p_recv.at[h], sent.at[9], pz_r.at[1, h], zat(lax.rem(z + 1, NZ))),
        ]

    def first(g):
        @pl.when(z == 0)
        def _():
            if g == 0:
                pl.semaphore_wait(hello_next, 1)
            for h in range(g * HG, g * HG + HG):
                p_send[h] = tot[h].astype(BF16)
                pm_send[h, 0:1, :] = ntot[h : h + 1, :]
                pm_send[h, 1:2, :] = before[h : h + 1] + top[h : h + 1]
                pm_send[h, 2:3, :] = before[h : h + 1]
                p_recv[h] = jnp.zeros((D, D), BF16)
                pm_recv[h] = jnp.where(small_rows == 1, NEG, 0.0)
            for h in range(g * HG, g * HG + HG):
                for copy in pz(h):
                    copy.start()

    small_rows = lax.broadcasted_iota(jnp.int32, (8, D), 0)

    def chain(g):
        @pl.when(z > 0)
        def _():
            if g == 0:

                @pl.when(z < NZ - 1)
                def _():
                    pl.semaphore_wait(hello_next, 1)

            for h in range(g * HG, g * HG + HG):
                with jax.named_scope(f"chain{g}"):
                    arrived(pm_recv.at[h], pz_r.at[0, h])
                    arrived(p_recv.at[h], pz_r.at[1, h])

                @pl.when(z < NZ - 1)
                def _():
                    m = pm_recv[h, 1:2, :]
                    hi = jnp.maximum(m, top[h : h + 1])
                    keep, add = jnp.exp(m - hi), jnp.exp(top[h : h + 1] - hi)
                    p_send[h] = (keep * p_recv[h].astype(F32) + add * tot[h]).astype(BF16)
                    pm_send[h, 0:1, :] = keep * pm_recv[h, 0:1, :] + add * ntot[h : h + 1, :]
                    pm_send[h, 1:2, :] = before[h : h + 1] + hi
                    pm_send[h, 2:3, :] = before[h : h + 1] + pm_recv[h, 2:3, :]
                    for copy in pz(h):
                        copy.start()

    def starts():
        with jax.named_scope("zstart"):
            arrived(cz_recv.at[0 : NZ - 1], tz_r.at[0])
            arrived(nz_recv.at[0 : NZ - 1], tz_r.at[1])
        with jax.named_scope("starts"):
            cz_recv[z] = cz_send[...]
            nz_recv[z] = nz_send[...]
            rows = nz_recv[0]
            for i in range(1, NZ):
                rows = rows + pltpu.roll(nz_recv[i], 4 * NX * i, 1)
            first_n[...] = rows
            for h in range(H):
                first_c[h] = jnp.concatenate([cz_recv[i, h].astype(F32) for i in range(NZ)], axis=0).T

    def xo(d, g):
        p = lax.rem(x + d, NX)
        heads = pl.ds(g * HG, HG)
        return [
            remote(bm_send.at[p, g], bm_recv.at[x, g], sent.at[10], xo_r.at[0, g], xdev(d)),
            remote(b_send.at[p, heads], b_recv.at[x, heads], sent.at[11], xo_r.at[1, g], xdev(d)),
        ]

    def spread(g):
        for u in range(HG):
            h = g * HG + u
            m = jnp.sum(jnp.where(lanes == h, level[pl.ds(x, 1), :], 0.0), axis=1, keepdims=True)
            m = m + pm_recv[h, 2:3, :]
            come = pm_recv[h, 1:2, :]
            hi = jnp.maximum(m, come)
            keep, add = jnp.exp(m - hi), jnp.exp(come - hi)
            cur = keep * first_c[h] + add * p_recv[h].astype(F32)
            nrow = keep * first_n[h : h + 1, :] + add * pm_recv[h, 0:1, :]
            m = hi
            for i in range(NX):
                b_send[i, h] = cur.astype(BF16)
                bm_send[i, g, 2 * u : 2 * u + 1, :] = nrow
                bm_send[i, g, 2 * u + 1 : 2 * u + 2, :] = m
                if i < NX - 1:
                    am = amax[i, h : h + 1, :]
                    hi = jnp.maximum(m, am)
                    keep, add = jnp.exp(m - hi), jnp.exp(am - hi)
                    cur = keep * cur + add * kvs[i, h]
                    nrow = keep * nrow + add * nkv[i, h : h + 1, :]
                    m = esum[i, h : h + 1, :] + hi
        for d in (2, 1, 3):
            for copy in xo(d, g):
                copy.start()
        heads = pl.ds(g * HG, HG)
        b_recv[x, heads] = b_send[x, heads]
        bm_recv[x, g] = bm_send[x, g]

    def finish_one(j, g):
        for u in range(HG):
            h = g * HG + u
            i = j * H + h
            q = qv[j, h]
            nrow = bm_recv[j, g, 2 * u : 2 * u + 1, :]
            m = bm_recv[j, g, 2 * u + 1 : 2 * u + 2, :]
            qc = nt(q, b_recv[j, h])
            qn = jnp.sum(q.astype(F32) * nrow, axis=1, keepdims=True)
            a = amx_s[i]
            hi = jnp.maximum(a, m)
            keep, add = jnp.exp(m - hi) * FACTOR, jnp.exp(a - hi)
            den = add * den_s[i] + keep * qn
            num = add * num_s[i] + keep * qc
            o = (num / jnp.maximum(jnp.abs(den), 1.0)).astype(BF16)
            normed = (o.astype(F32) * gain[h : h + 1, :]).astype(BF16)
            hid[pl.ds(pl.multiple_of(j * T, T), T), h * D : h * D + D] = normed

    def finish(g):
        with jax.named_scope("finish"):
            finish_one(x, g)
        with jax.named_scope(f"xout{g}"):
            arrived(bm_recv.at[0:3, 0], xo_r.at[0, g])
            arrived(b_recv.at[0:3, 0:HG], xo_r.at[1, g])
        with jax.named_scope("finish"):
            for d in (1, 3, 2):
                finish_one(lax.rem(x - d + NX, NX), g)

    def columns(core, r):
        block = lax.rem(y + r, NY) * 2 + core
        return pl.ds(pl.multiple_of(block * 256, 256), 256)

    def early_one(r):
        for core in (0, 1):
            acc[core, r] = jnp.dot(hid[:, 0:RA], wall[core, r, 0:RA], preferred_element_type=F32)

    def late_one(r):
        for core in (0, 1):
            part = jnp.dot(hid[:, RA:1024], wall[core, r, RA:1024], preferred_element_type=F32)
            out[:, columns(core, r)] = (acc[core, r] + part).astype(BF16)

    def twos(name, fn, low, high):
        def body(i, _):
            fn(lax.rem(NY - 2 + 2 * i, NY))
            fn(lax.rem(NY - 1 + 2 * i, NY))
            return 0

        with jax.named_scope(name):
            lax.fori_loop(low, high, body, 0)

    def last():
        with jax.named_scope("last"):
            for core in (0, 1):
                whole = jnp.dot(hid[...], wall[core, NY // 2], preferred_element_type=F32)
                out[:, columns(core, NY // 2)] = whole.astype(BF16)

    def mates(level):
        with jax.named_scope("mate"):
            count = (4, 2, 1)[level]
            arrived(wall.at[c, 0:count, 0:RA], wd_r.at[level])

    def zgate():
        with jax.named_scope("zgate"):

            @pl.when(z < NZ - 1)
            def _():
                pl.semaphore_wait(hello, NZ - 1 - z)

    def cz_all():
        for d in (4, 3, 5, 2, 6, 1, 7):
            for copy in cz(d):
                copy.start()

    def wspread_start():
        for d in (2, 1, 3):
            wspread(d).start()

    def wspread_done():
        with jax.named_scope("wspread"):
            arrived(wall.at[c, 1:NY, 0 : 3 * RB], ws_r.at[0])
        wrest().start()

    def sent_cell():
        for k, ref in enumerate((iv, fv, cv, nv)):
            arrived(ref.at[0:3], sent.at[k])
        arrived(b_send.at[0:3], sent.at[4])
        arrived(cz_recv.at[0 : NZ - 1], sent.at[5])
        arrived(nz_recv.at[0 : NZ - 1], sent.at[6])

        @pl.when(z < NZ - 1)
        def _():
            arrived(pm_send, sent.at[8])
            arrived(p_send, sent.at[9])

        arrived(wall.at[c, 1:NY, 0 : 3 * RB], sent.at[14])

    def sent_rest():
        arrived(bm_send.at[0:3], sent.at[10])
        arrived(b_send.at[0:3], sent.at[11])
        arrived(wall.at[c, :, 0:352], sent.at[15])

    def sent_ring():
        arrived(wall.at[c, 1:NY, 0:832], sent.at[12])
        arrived(wall.at[c, 1:NY, 0:768], sent.at[13])

    @pl.when(z >= NZ // 2)
    def _():
        zgate()
        cz_all()

    inner(1)
    serve(1, "b")
    begin(0, 2)
    total(0)

    @pl.when(z < NZ // 2)
    def _():
        first(0)
        inner(2)
        total(1)
        first(1)
        zgate()
        cz_all()
        serve(2, "b")
        serve(0, 0)
        serve(0, 1)
        inner(3)
        chain(0)
        total(2)
        first(2)
        serve(3, "half")
        wspread_start()
        chain(1)
        serve(0, 2)
        total(3)
        first(3)
        chain(2)
        serve(1, 0)
        starts()
        spread(0)
        chain(3)
        spread(1)
        serve(1, 1)
        spread(2)
        spread(3)
        serve(1, 2)
        finish(0)
        wspread_done()
        serve(2, 0)
        finish(1)
        sent_cell()
        arrived(wall.at[c, 0], wo_r.at[0])
        serve(2, 1)
        mates(0)
        finish(2)
        serve(2, 2)
        twos("early", early_one, 0, 2)
        finish(3)
        serve(3, 0)
        mates(1)
        with jax.named_scope("early"):
            early_one(2)
            early_one(3)
            early_one(5)
        serve(3, "cut")

    @pl.when(jnp.logical_and(z >= NZ // 2, z < NZ - 2))
    def _():
        inner(2)
        total(1)
        serve(2, "b")
        serve(0, 0)
        serve(0, 1)
        inner(3)
        total(2)
        serve(3, "half")
        wspread_start()
        serve(0, 2)
        total(3)
        starts()
        serve(1, 0)
        chain(0)
        spread(0)
        chain(1)
        serve(1, 1)
        spread(1)
        chain(2)
        serve(1, 2)
        spread(2)
        chain(3)
        spread(3)
        finish(0)
        serve(2, 0)
        wspread_done()
        finish(1)
        serve(2, 1)
        sent_cell()
        arrived(wall.at[c, 0], wo_r.at[0])
        mates(0)
        finish(2)
        serve(2, 2)
        twos("early", early_one, 0, 2)
        finish(3)
        serve(3, 0)
        mates(1)
        with jax.named_scope("early"):
            early_one(2)
            early_one(3)
            early_one(5)
        serve(3, "cut")

    @pl.when(z >= NZ - 2)
    def _():
        inner(2)
        total(1)
        serve(2, "b")
        serve(0, 0)
        serve(0, 1)
        inner(3)
        total(2)
        serve(3, "half")
        wspread_start()
        serve(0, 2)
        total(3)
        starts()
        serve(1, 0)
        serve(1, 1)
        chain(0)
        spread(0)
        serve(1, 2)
        chain(1)
        spread(1)
        serve(2, 0)
        chain(2)
        spread(2)
        serve(2, 1)
        finish(0)
        chain(3)
        spread(3)
        wspread_done()
        serve(2, 2)
        finish(1)
        sent_cell()
        arrived(wall.at[c, 0], wo_r.at[0])
        mates(0)
        finish(2)
        twos("early", early_one, 0, 2)
        serve(3, 0)
        finish(3)
        mates(1)
        with jax.named_scope("early"):
            early_one(2)
            early_one(3)
            early_one(5)
        serve(3, "cut")

    arrived(wall.at[c, 1:NY, RA:1024], ws_r.at[2])
    twos("late", late_one, 0, 3)
    with jax.named_scope("late"):
        late_one(5)
    sent_rest()
    mates(2)
    last()
    sent_ring()


def on_device(queries, keys, values, input_gate, forget_gate, start_memory, start_norm, start_level, head_gain, out_weight):
    arrays = (
        input_gate, forget_gate, queries, keys, values, start_memory.reshape(S, 32, D),
        jnp.transpose(start_norm, (0, 2, 1)), out_weight, start_level, head_gain,
    )
    dma, vmem = pltpu.SemaphoreType.DMA, pltpu.VMEM
    out = pl.pallas_call(
        kernel,
        out_shape=pltpu.VMEM((S * T, 4096), BF16),
        in_specs=[pl.BlockSpec(memory_space=pltpu.HBM)] * len(arrays),
        out_specs=pl.BlockSpec(memory_space=pltpu.VMEM),
        scratch_shapes=[
            vmem((S, H, T, D), BF16), vmem((S, H, T, D), BF16), vmem((S, H, T, D), BF16),
            vmem((S, H, T), BF16), vmem((S, H, T), BF16), vmem((S, 32, D), F32), vmem((S, 4, H), F32),
            vmem((NX, H, T, D), BF16), vmem((NX, H, T, D), BF16),
            vmem((NX, H, T), BF16), vmem((NX, H, T), BF16), vmem((NX, 32, D), F32), vmem((NX, 4, H), F32),
            vmem((S, H), F32), vmem((H, D), F32),
            vmem((2, NY, 1024, 256), BF16),
            vmem((S * H, T), F32),
            vmem((S * H, T, D), F32), vmem((S * H, T, D), F32), vmem((S * H, T, D), F32),
            vmem((NX, H, T), F32), vmem((NX, H, D), F32), vmem((NX, H, D), F32),
            vmem((NX, H, D, D), F32), vmem((NX, H, D), F32), vmem((16 + D, D), F32),
            vmem((H, 16, D), BF16), vmem((NZ, H, 16, D), BF16), vmem((H, D), F32), vmem((NZ, H, D), F32),
            vmem((H, D, D), F32), vmem((H, D), F32), vmem((H, D, D), F32), vmem((H, D), F32),
            vmem((H, D, D), BF16), vmem((H, D, D), BF16),
            vmem((H, 8, D), F32), vmem((H, 8, D), F32),
            vmem((NX, H, D, D), BF16), vmem((S, H, D, D), BF16),
            vmem((NX, G, 8, D), F32), vmem((S, G, 8, D), F32),
            vmem((S * T, H * D), BF16), vmem((2, NY, S * T, 256), F32),
            dma((7,)), dma((16,)), dma((4,)), dma((2, G)), dma((2,)), dma((2, H)), dma((2, G)),
            dma((15,)), dma((3,)), dma((3,)), dma((1,)), pltpu.SemaphoreType.REGULAR, pltpu.SemaphoreType.REGULAR,
        ],
        compiler_params=pltpu.CompilerParams(
            collective_id=0, has_side_effects=True, vmem_limit_bytes=50_000_000
        ),
        name="cell_layer",
    )(*(pltpu.with_memory_space_constraint(array, pltpu.HBM) for array in arrays))
    return out.reshape(S, T, 4096)


def solution(mesh):
    return jax.shard_map(
        on_device,
        mesh=mesh,
        in_specs=(
            P("dp", None, "sp", None),
            P("dp", None, "sp", None),
            P("dp", None, "sp", None),
            P("dp", None, "sp"),
            P("dp", None, "sp"),
            P("dp", None, "sp", None),
            P("dp", None, "sp"),
            P("dp", None),
            P(),
            P(None, "dp"),
        ),
        out_specs=P("dp", "sp", None),
        check_vma=False,
    )
```

```python
import jax
import jax.numpy as jnp
from jax import lax
from jax.experimental import pallas as pl
from jax.experimental.pallas import tpu as pltpu
from jax.sharding import PartitionSpec as P

MESH = pl.DeviceIdType.MESH
F32 = jnp.float32
BF16 = jnp.bfloat16
S, H, T, D = 4, 8, 64, 128
NX, NZ, NY = 4, 8, 8
FACTOR = D**-0.5
NEG = -1e30
NQ = NZ // 2
G = 4
HG = H // G
RA = 768
RB = (1024 - RA) // NX


def nt(a, b):
    return lax.dot_general(a, b, (((1,), (1,)), ((), ())), preferred_element_type=F32)


def kernel(
    i_hbm, f_hbm, q_hbm, k_hbm, v_hbm, c_hbm, n_hbm, w_hbm, level_hbm, gain_hbm, out,
    qv, kv, vv, iv, fv, cv, nv, kx, vx, ix, fx, cx, nx, level, gain, wall, a_loc, num_s, den_s, amx_s,
    wrow, esum, amax, kvs, nkv, turn, cz_send, cz_recv, h_send, h_recv, hm_send, hm_recv, t_send, t_recv, tm_send, tm_recv,
    p_send, p_recv, pm_send, pm_recv, b_send, b_recv, bm_send, bm_recv, hid, acc,
    lsem, sent, xs_r, xk_r, tz_r, pz_r, xo_r, wy_r, wd_r, ws_r, wo_r, hr_r, hello, hello_far,
):
    sp = lax.axis_index("sp")
    dp = lax.axis_index("dp")
    x, z = lax.rem(sp, NX), lax.div(sp, NX)
    y, c = lax.div(dp, 2), lax.rem(dp, 2)
    zq = lax.rem(z, NQ)
    below = z - zq
    def xdev(d):
        return {"sp": z * NX + lax.rem(x + d, NX), "dp": dp}

    def zat(p):
        return {"sp": p * NX + x, "dp": dp}

    def ydev(d):
        return {"sp": sp, "dp": lax.rem(y + d + NY, NY) * 2 + c}

    mate = {"sp": sp, "dp": y * 2 + (1 - c)}

    def remote(src, dst, ssem, rsem, dev):
        return pltpu.make_async_remote_copy(
            src_ref=src, dst_ref=dst, send_sem=ssem, recv_sem=rsem,
            device_id=dev, device_id_type=MESH,
        )

    barrier = pltpu.get_barrier_semaphore()
    peers = [xdev(d) for d in range(1, NX)] + [ydev(1), ydev(-1), mate]
    for dev in peers:
        pl.semaphore_signal(barrier, inc=1, device_id=dev, device_id_type=MESH)
    for d in range(1, NZ):

        @pl.when(z + d < NZ)
        def _():
            dev = zat(lax.rem(z + d, NZ))
            pl.semaphore_signal(barrier, inc=1, device_id=dev, device_id_type=MESH)

    loads = [
        (i_hbm, iv, 0), (f_hbm, fv, 1), (k_hbm, kv, 2), (v_hbm, vv, 2), (w_hbm, wall.at[c, 0], 2), (q_hbm, qv, 2),
        (c_hbm, cv, 3), (n_hbm, nv, 4), (level_hbm, level, 5), (gain_hbm, gain, 6),
    ]
    for src, dst, k in loads:
        pltpu.make_async_copy(src, dst, lsem.at[k]).start()

    rows64 = lax.broadcasted_iota(jnp.int32, (T, T), 0)
    cols64 = lax.broadcasted_iota(jnp.int32, (T, T), 1)
    upper = jnp.where(rows64 <= cols64, 1.0, 0.0).astype(F32)
    causal = rows64 >= cols64

    def gates(li, f):
        li, f = li.astype(F32), f.astype(F32)
        lf = jnp.minimum(f, 0.0) - jnp.log1p(jnp.exp(-jnp.abs(f)))
        b = jnp.dot(lf, upper, precision=lax.Precision.HIGHEST, preferred_element_type=F32)
        return li - b, b[:, T - 1 : T]

    def arrived(ref, sem):
        pltpu.make_async_copy(ref, ref, sem).wait()

    with jax.named_scope("loads"):
        arrived(iv, lsem.at[0])
        arrived(fv, lsem.at[1])
    for j in range(S):
        a, _ = gates(iv[j], fv[j])
        a_loc[8 * j : 8 * j + 8, :] = a

    def block_gates(p, li, f):
        a, e = gates(li, f)
        am = jnp.max(a, axis=1, keepdims=True)
        esum[p] = jnp.broadcast_to(e, (H, D))
        amax[p] = jnp.broadcast_to(am, (H, D))
        wrow[p] = jnp.exp(a - am)

    block_gates(x, iv[x], fv[x])
    arrived(wall.at[c, 0:4], lsem.at[2])
    for k, ref in ((3, cv), (4, nv), (5, level), (6, gain)):
        arrived(ref, lsem.at[k])
    cx[x] = cv[x]
    nx[x] = nv[x]

    with jax.named_scope("barrier"):
        pl.semaphore_wait(barrier, len(peers) + z)
    for d in range(1, NQ):

        @pl.when(zq >= d)
        def _():
            dev = zat(lax.rem(z - d + NZ, NZ))
            pl.semaphore_signal(hello, inc=1, device_id=dev, device_id_type=MESH)

    @pl.when(z >= NQ)
    def _():
        pl.semaphore_signal(hello_far, inc=1, device_id=zat(lax.rem(z + NQ, NZ)), device_id_type=MESH)

    def rows_of(side, kind):
        if kind == "b":
            return pl.ds(pl.multiple_of(RA + RB * x, RB), RB)
        if kind == "half":
            return pl.ds(pl.multiple_of(RA + RB * x + side * (RB // 2), RB // 2), RB // 2)
        if kind == "cut":
            return pl.ds(256 + 128 * side, 128)
        return pl.ds(256 * (2 - kind if side else kind), 256)

    ring = [(0, "b"), (0, 0), (1, "b"), (0, 1), (2, "b"), (0, 2), (3, "half")]
    ring += [(1, 0), (1, 1), (1, 2), (2, 0), (2, 1), (2, 2), (3, 0), (3, "cut")]
    onward = {(0, "b"): (1, "b"), (1, "b"): (2, "b"), (2, "b"): (3, "half"), (2, 1): (3, "cut")}
    for k in range(3):
        onward[0, k], onward[1, k] = (1, k), (2, k)
    onward[2, 0] = (3, 0)

    def wsend(side, item):
        level, kind = item
        k = ring.index(item)
        rows = rows_of(side, kind)
        src, dst = (level, level + 1) if side else ((NY - level) % NY, NY - 1 - level)
        return remote(
            wall.at[c, src, rows], wall.at[c, dst, rows],
            sent.at[12], wy_r.at[k], ydev(-1 if side else 1),
        )

    def wmate(side, item):
        level, kind = item
        ref = wall.at[c, level + 1 if side else NY - 1 - level, rows_of(side, kind)]
        return remote(ref, ref, sent.at[13], wd_r.at[max(0, level - 1)], mate)

    def serve(level, kind):
        item = (level, kind)
        count = {"b": RB, "half": RB // 2, "cut": 128}.get(kind, 256)
        with jax.named_scope(f"serve{level}{kind}"):
            arrived(wall.at[c, 0:2, 0:count], wy_r.at[ring.index(item)])
        for side in (0, 1):
            if item in onward:
                wsend(side, onward[item]).start()
            if kind not in ("b", "half"):
                wmate(side, item).start()

    def begin(level, kind):
        for side in (0, 1):
            wsend(side, (level, kind)).start()

    def wspread(d):
        rows = pl.ds(pl.multiple_of(RA + RB * x, RB), RB)
        ref = wall.at[c, 1:NY, rows]
        return remote(ref, ref, sent.at[14], ws_r.at[0], xdev(d))

    def wrest():
        ref = wall.at[c, 1:NY, RA:1024]
        return remote(ref, ref, sent.at[15], ws_r.at[2], mate)

    small = [(iv, ix), (fv, fx), (cv, cx), (nv, nx)]

    def xsmall(d):
        p = lax.rem(x + d, NX)
        return [
            remote(src.at[p], dst.at[x], sent.at[k], xs_r.at[k], xdev(d)) for k, (src, dst) in enumerate(small)
        ]

    def xkeys(d, g):
        p = lax.rem(x + d, NX)
        heads = pl.ds(g * HG, HG)
        return [
            remote(src.at[p, heads], dst.at[x, heads], sent.at[4], xk_r.at[k, g], xdev(d))
            for k, (src, dst) in enumerate([(kv, kx), (vv, vx)])
        ]

    begin(0, "b")
    begin(0, 0)
    for d in (2, 1, 3):
        for copy in xsmall(d):
            copy.start()
    for g in range(G):
        for d in (2, 1, 3):
            for copy in xkeys(d, g):
                copy.start()
    remote(wall.at[c, 0], wall.at[c, 0], sent.at[15], wo_r.at[0], mate).start()

    def intra(i):
        j, h = lax.div(i, H), lax.rem(i, H)
        arow = a_loc[pl.ds(i, 1), :]
        masked = jnp.where(causal, jnp.broadcast_to(arow, (T, T)), NEG)
        top = jnp.max(masked, axis=1, keepdims=True)
        weight = jnp.exp(masked - top)
        scores = nt(qv[j, h], kv[j, h]) * FACTOR * weight
        den_s[i] = jnp.broadcast_to(jnp.sum(scores, axis=1, keepdims=True), (T, D))
        amx_s[i] = jnp.broadcast_to(top, (T, D))
        num_s[i] = jnp.dot(scores.astype(BF16), vv[j, h], preferred_element_type=F32)

    def inner(part):
        def body(i, _):
            for u in range(4):
                intra(part * 8 + i * 4 + u)
            return 0

        with jax.named_scope("intra"):
            lax.fori_loop(0, 2, body, 0)

    def state(p, h, keys, values):
        w = wrow[p, pl.ds(h, 1), :]
        vt = values[p, h].astype(F32).T
        hi = w.astype(BF16)
        lo = (w - hi.astype(F32)).astype(BF16)
        rid = lax.broadcasted_iota(jnp.int32, (16, T), 0)
        extra = jnp.where(
            rid == 0,
            jnp.broadcast_to(hi.astype(F32), (16, T)),
            jnp.where(rid == 1, jnp.broadcast_to(lo.astype(F32), (16, T)), 0.0),
        )
        lhs = jnp.concatenate([(vt * w).astype(BF16), extra.astype(BF16)], axis=0)
        st = jnp.dot(lhs, keys[p, h], preferred_element_type=F32)
        kvs[p, h] = st[0:D]
        nkv[p, pl.ds(h, 1), :] = st[D : D + 1] + st[D + 1 : D + 2]

    def states(p, g):
        with jax.named_scope("states"):
            for u in range(HG):
                state(p, g * HG + u, kx, vx)

    inner(0)

    def own(i, _):
        for u in range(4):
            state(x, i * 4 + u, kv, vv)
        return 0

    lax.fori_loop(0, 2, own, 0)
    serve(0, "b")
    begin(0, 1)
    with jax.named_scope("xgates"):
        for k, (src, dst) in enumerate(small):
            arrived(dst.at[0:3], xs_r.at[k])
        for d in (1, 3, 2):
            p = lax.rem(x - d + NX, NX)
            block_gates(p, ix[p], fx[p])

    shift = []
    before = jnp.zeros((H, D), F32)
    top = None
    for i in range(NX):
        a = amax[i] - before
        shift.append(a)
        top = a if top is None else jnp.maximum(top, a)
        before = before + esum[i]
    scale = [jnp.exp(a - top) for a in shift]

    def tz(h):
        w = h // NQ
        to = zat(below + h % NQ)
        return [
            remote(tm_send.at[h], tm_recv.at[w, zq], sent.at[5], tz_r.at[0, w], to),
            remote(t_send.at[h], t_recv.at[w, zq], sent.at[6], tz_r.at[1, w], to),
        ]

    def total(g):
        with jax.named_scope(f"xin{g}"):
            for k, ref in enumerate((kx, vx)):
                arrived(ref.at[0:3, 0:HG], xk_r.at[k, g])
        for d in (1, 3, 2):
            states(lax.rem(x - d + NX, NX), g)
        for h in range(g * HG, g * HG + HG):
            ntot = sum(scale[i][h : h + 1] * nkv[i, h : h + 1, :] for i in range(NX))
            t_send[h] = sum(scale[i][h : h + 1] * kvs[i, h] for i in range(NX)).astype(BF16)
            tm_send[h, 0:1, :] = ntot
            tm_send[h, 1:2, :] = before[h : h + 1]
            tm_send[h, 2:3, :] = top[h : h + 1]

    def total_send(g):
        for h in range(g * HG, g * HG + HG):
            copies = tz(h)

            @pl.when(jnp.logical_and(zq != h % NQ, z < NZ - 1))
            def _():
                for copy in copies:
                    copy.start()

    def cz(o):
        return remote(cz_send.at[o], cz_recv.at[z], sent.at[7], tz_r.at[2, 0], zat(o))

    for i in range(NX):
        turn[4 * i : 4 * i + 4, 0:H] = nx[i]
        for h in range(H):
            at = 16 * (h // NQ) + 4 * i
            cz_send[h % NQ, at : at + 4, :] = cx[i, 4 * h : 4 * h + 4, :]
    first_lanes = lax.broadcasted_iota(jnp.int32, (H, D), 1) < 4 * NX
    nfirst = jnp.where(first_lanes, turn[...].T[0:H], 0.0)
    for h in range(H):
        cz_send[h % NQ, 32 + h // NQ : 33 + h // NQ, :] = nfirst[h : h + 1]

    def scan_step(w, i, cur, nrow, m):
        am = tm_recv[w, i, 2:3, :]
        hi = jnp.maximum(m, am)
        keep, add = jnp.exp(m - hi), jnp.exp(am - hi)
        cur = keep * cur + add * t_recv[w, i].astype(F32)
        nrow = keep * nrow + add * tm_recv[w, i, 0:1, :]
        return cur, nrow, tm_recv[w, i, 1:2, :] + hi

    def scan_states(g, head, cur, nrow, m):
        w = g // 2
        for i in range(NQ):
            p_send[w, i] = cur.astype(BF16)
            pm_send[w, i, 0:1, :] = nrow
            pm_send[w, i, 1:2, :] = m
            if i < NQ - 1:
                cur, nrow, m = scan_step(w, i, cur, nrow, m)
        for i in range(NQ):

            @pl.when(zq != i)
            def _():
                to = zat(below + i)
                remote(pm_send.at[w, i], pm_recv.at[head], sent.at[8], pz_r.at[0, g], to).start()
                remote(p_send.at[w, i], p_recv.at[head], sent.at[9], pz_r.at[1, g], to).start()

            @pl.when(zq == i)
            def _():
                p_recv[head] = p_send[w, i]
                pm_recv[head] = pm_send[w, i]

        return cur, nrow, m

    def totals_wait(w, count):
        arrived(tm_recv.at[w, 0:count], tz_r.at[0, w])
        arrived(t_recv.at[w, 0:count], tz_r.at[1, w])

    runs = lax.div(zq, 2)

    def scan(g):
        w = g // 2
        head = zq + NQ * w

        @pl.when(jnp.logical_and(runs == g % 2, z < NQ))
        def _():
            with jax.named_scope(f"zin{g}"):
                if w == 0:
                    arrived(cz_recv.at[0 : NZ - 1], tz_r.at[2, 0])
                    cz_recv[z] = cz_send[zq]
                    pl.semaphore_wait(hello_far, 1)
                totals_wait(w, NQ - 1)
            with jax.named_scope("scan"):
                t_recv[w, zq] = t_send[head]
                tm_recv[w, zq] = tm_send[head]
                lanes = lax.broadcasted_iota(jnp.int32, (1, H), 1)
                m = jnp.sum(jnp.where(lanes == head, level[pl.ds(x, 1), :], 0.0), axis=1, keepdims=True)
                m = jnp.broadcast_to(m, (1, D))
                nrow = cz_recv[0, 32 + w : 33 + w, :]
                for i in range(1, NZ):
                    nrow = nrow + pltpu.roll(cz_recv[i, 32 + w : 33 + w, :], 4 * NX * i, 1)
                cur = jnp.concatenate([cz_recv[i, 16 * w : 16 * w + 16, :] for i in range(NZ)], axis=0).T
                cur, nrow, m = scan_step(w, NQ - 1, *scan_states(g, head, cur, nrow, m))
                h_send[w] = cur.astype(BF16)
                hm_send[w, 0:1, :] = nrow
                hm_send[w, 1:2, :] = m
                to = zat(lax.rem(z + NQ, NZ))
                remote(hm_send.at[w], hm_recv.at[w], sent.at[16], hr_r.at[0, w], to).start()
                remote(h_send.at[w], h_recv.at[w], sent.at[17], hr_r.at[1, w], to).start()

        @pl.when(jnp.logical_and(runs == g % 2, z >= NQ))
        def _():
            with jax.named_scope(f"zin{g}"):

                @pl.when(z < NZ - 1)
                def _():
                    totals_wait(w, NQ - 2)

                @pl.when(z == NZ - 1)
                def _():
                    totals_wait(w, NQ - 1)

                arrived(hm_recv.at[w], hr_r.at[0, w])
                arrived(h_recv.at[w], hr_r.at[1, w])
            with jax.named_scope("scan"):
                t_recv[w, zq] = t_send[head]
                tm_recv[w, zq] = tm_send[head]
                scan_states(g, head, h_recv[w].astype(F32), hm_recv[w, 0:1, :], hm_recv[w, 1:2, :])

    def xo(d, g):
        p = lax.rem(x + d, NX)
        heads = pl.ds(g * HG, HG)
        return [
            remote(bm_send.at[p, g], bm_recv.at[x, g], sent.at[10], xo_r.at[0, g], xdev(d)),
            remote(b_send.at[p, heads], b_recv.at[x, heads], sent.at[11], xo_r.at[1, g], xdev(d)),
        ]

    def spread(g):
        with jax.named_scope(f"zout{g}"):

            @pl.when(runs == g % 2)
            def _():
                for k, ref in enumerate((pm_recv, p_recv)):
                    arrived(ref.at[0 : HG - 1], pz_r.at[k, g])

            @pl.when(runs != g % 2)
            def _():
                for k, ref in enumerate((pm_recv, p_recv)):
                    arrived(ref.at[0:HG], pz_r.at[k, g])

        for u in range(HG):
            h = g * HG + u
            cur = p_recv[h].astype(F32)
            nrow = pm_recv[h, 0:1, :]
            m = pm_recv[h, 1:2, :]
            for i in range(NX):
                b_send[i, h] = cur.astype(BF16)
                bm_send[i, g, 2 * u : 2 * u + 1, :] = nrow
                bm_send[i, g, 2 * u + 1 : 2 * u + 2, :] = m
                if i < NX - 1:
                    am = amax[i, h : h + 1, :]
                    hi = jnp.maximum(m, am)
                    keep, add = jnp.exp(m - hi), jnp.exp(am - hi)
                    cur = keep * cur + add * kvs[i, h]
                    nrow = keep * nrow + add * nkv[i, h : h + 1, :]
                    m = esum[i, h : h + 1, :] + hi
        for d in (2, 1, 3):
            for copy in xo(d, g):
                copy.start()
        heads = pl.ds(g * HG, HG)
        b_recv[x, heads] = b_send[x, heads]
        bm_recv[x, g] = bm_send[x, g]

    def finish_one(j, g):
        for u in range(HG):
            h = g * HG + u
            i = j * H + h
            q = qv[j, h]
            nrow = bm_recv[j, g, 2 * u : 2 * u + 1, :]
            m = bm_recv[j, g, 2 * u + 1 : 2 * u + 2, :]
            qc = nt(q, b_recv[j, h])
            qn = jnp.sum(q.astype(F32) * nrow, axis=1, keepdims=True)
            a = amx_s[i]
            hi = jnp.maximum(a, m)
            keep, add = jnp.exp(m - hi) * FACTOR, jnp.exp(a - hi)
            den = add * den_s[i] + keep * qn
            num = add * num_s[i] + keep * qc
            o = (num / jnp.maximum(jnp.abs(den), 1.0)).astype(BF16)
            normed = (o.astype(F32) * gain[h : h + 1, :]).astype(BF16)
            hid[pl.ds(pl.multiple_of(j * T, T), T), h * D : h * D + D] = normed

    def finish(g):
        with jax.named_scope("finish"):
            finish_one(x, g)
        with jax.named_scope(f"xout{g}"):
            arrived(bm_recv.at[0:3, 0], xo_r.at[0, g])
            arrived(b_recv.at[0:3, 0:HG], xo_r.at[1, g])
        with jax.named_scope("finish"):
            for d in (1, 3, 2):
                finish_one(lax.rem(x - d + NX, NX), g)

    def columns(core, r):
        block = lax.rem(y + r, NY) * 2 + core
        return pl.ds(pl.multiple_of(block * 256, 256), 256)

    def early_one(r):
        for core in (0, 1):
            acc[core, r] = jnp.dot(hid[:, 0:RA], wall[core, r, 0:RA], preferred_element_type=F32)

    def late_one(r):
        for core in (0, 1):
            part = jnp.dot(hid[:, RA:1024], wall[core, r, RA:1024], preferred_element_type=F32)
            out[:, columns(core, r)] = (acc[core, r] + part).astype(BF16)

    def twos(name, fn, low, high):
        def body(i, _):
            fn(lax.rem(NY - 2 + 2 * i, NY))
            fn(lax.rem(NY - 1 + 2 * i, NY))
            return 0

        with jax.named_scope(name):
            lax.fori_loop(low, high, body, 0)

    def last():
        with jax.named_scope("last"):
            for core in (0, 1):
                whole = jnp.dot(hid[...], wall[core, NY // 2], preferred_element_type=F32)
                out[:, columns(core, NY // 2)] = whole.astype(BF16)

    def mates(level):
        with jax.named_scope("mate"):
            count = (4, 2, 1)[level]
            arrived(wall.at[c, 0:count, 0:RA], wd_r.at[level])

    def zgate():
        with jax.named_scope("zgate"):

            @pl.when(zq < NQ - 1)
            def _():
                pl.semaphore_wait(hello, NQ - 1 - zq)

    def cz_all():
        for o in range(NQ):

            @pl.when(z != o)
            def _():
                cz(o).start()


    def wspread_start():
        for d in (2, 1, 3):
            wspread(d).start()

    def wspread_done():
        with jax.named_scope("wspread"):
            arrived(wall.at[c, 1:NY, 0 : 3 * RB], ws_r.at[0])
        wrest().start()

    def sent_cell():
        for k, ref in enumerate((iv, fv, cv, nv)):
            arrived(ref.at[0:3], sent.at[k])
        arrived(b_send.at[0:3], sent.at[4])
        arrived(pm_send.at[:, 0 : NQ - 1], sent.at[8])
        arrived(p_send.at[:, 0 : NQ - 1], sent.at[9])

        @pl.when(z < NZ - 1)
        def _():
            arrived(tm_send.at[0 : H - 2], sent.at[5])
            arrived(t_send.at[0 : H - 2], sent.at[6])

        @pl.when(z < NQ)
        def _():
            arrived(cz_send.at[0 : NQ - 1], sent.at[7])
            arrived(hm_send, sent.at[16])
            arrived(h_send, sent.at[17])

        @pl.when(z >= NQ)
        def _():
            arrived(cz_send, sent.at[7])

        arrived(wall.at[c, 1:NY, 0 : 3 * RB], sent.at[14])

    def sent_rest():
        arrived(bm_send.at[0:3], sent.at[10])
        arrived(b_send.at[0:3], sent.at[11])
        arrived(wall.at[c, :, 0:352], sent.at[15])

    def sent_ring():
        arrived(wall.at[c, 1:NY, 0:832], sent.at[12])
        arrived(wall.at[c, 1:NY, 0:768], sent.at[13])

    @pl.when(z >= NZ // 2)
    def _():
        zgate()
        cz_all()

    inner(1)
    serve(1, "b")
    begin(0, 2)
    total(0)

    @pl.when(z < NZ // 2)
    def _():
        zgate()
        total_send(0)
        cz_all()
        inner(2)
        total(1)
        total_send(1)
        serve(2, "b")
        serve(0, 0)
        serve(0, 1)
        inner(3)
        total(2)
        total_send(2)
        serve(3, "half")
        wspread_start()
        serve(0, 2)
        total(3)
        total_send(3)
        scan(1)
        scan(0)
        serve(1, 0)
        scan(2)
        serve(1, 1)
        scan(3)
        spread(0)
        spread(1)
        serve(1, 2)
        spread(2)
        serve(2, 0)
        finish(0)
        spread(3)
        wspread_done()
        serve(2, 1)
        finish(1)
        sent_cell()
        arrived(wall.at[c, 0], wo_r.at[0])
        mates(0)
        serve(2, 2)
        finish(2)
        twos("early", early_one, 0, 2)
        serve(3, 0)
        mates(1)
        with jax.named_scope("early"):
            early_one(2)
            early_one(3)
            early_one(5)
        serve(3, "cut")
        finish(3)

    @pl.when(z >= NZ // 2)
    def _():
        total_send(0)
        inner(2)
        total(1)
        total_send(1)
        serve(2, "b")
        serve(0, 0)
        serve(0, 1)
        inner(3)
        total(2)
        total_send(2)
        serve(3, "half")
        wspread_start()
        serve(0, 2)
        total(3)
        total_send(3)
        serve(1, 0)
        scan(0)
        scan(1)
        serve(1, 1)
        spread(0)
        scan(2)
        scan(3)
        spread(1)
        serve(1, 2)
        spread(2)
        finish(0)
        serve(2, 0)
        spread(3)
        finish(1)
        wspread_done()
        serve(2, 1)
        arrived(wall.at[c, 0], wo_r.at[0])
        mates(0)
        finish(2)
        serve(2, 2)
        twos("early", early_one, 0, 2)
        sent_cell()
        serve(3, 0)
        mates(1)
        with jax.named_scope("early"):
            early_one(2)
            early_one(3)
            early_one(5)
        finish(3)
        serve(3, "cut")

    arrived(wall.at[c, 1:NY, RA:1024], ws_r.at[2])
    twos("late", late_one, 0, 3)
    with jax.named_scope("late"):
        late_one(5)
    sent_rest()
    mates(2)
    last()
    sent_ring()


def on_device(queries, keys, values, input_gate, forget_gate, start_memory, start_norm, start_level, head_gain, out_weight):
    arrays = (
        input_gate, forget_gate, queries, keys, values, start_memory.reshape(S, 32, D),
        jnp.transpose(start_norm, (0, 2, 1)), out_weight, start_level, head_gain,
    )
    dma, vmem = pltpu.SemaphoreType.DMA, pltpu.VMEM
    out = pl.pallas_call(
        kernel,
        out_shape=pltpu.VMEM((S * T, 4096), BF16),
        in_specs=[pl.BlockSpec(memory_space=pltpu.HBM)] * len(arrays),
        out_specs=pl.BlockSpec(memory_space=pltpu.VMEM),
        scratch_shapes=[
            vmem((S, H, T, D), BF16), vmem((S, H, T, D), BF16), vmem((S, H, T, D), BF16),
            vmem((S, H, T), BF16), vmem((S, H, T), BF16), vmem((S, 32, D), F32), vmem((S, 4, H), F32),
            vmem((NX, H, T, D), BF16), vmem((NX, H, T, D), BF16),
            vmem((NX, H, T), BF16), vmem((NX, H, T), BF16), vmem((NX, 32, D), F32), vmem((NX, 4, H), F32),
            vmem((S, H), F32), vmem((H, D), F32),
            vmem((2, NY, 1024, 256), BF16),
            vmem((S * H, T), F32),
            vmem((S * H, T, D), F32), vmem((S * H, T, D), F32), vmem((S * H, T, D), F32),
            vmem((NX, H, T), F32), vmem((NX, H, D), F32), vmem((NX, H, D), F32),
            vmem((NX, H, D, D), F32), vmem((NX, H, D), F32), vmem((D, D), F32),
            vmem((NQ, 40, D), F32), vmem((NZ, 40, D), F32),
            vmem((2, D, D), BF16), vmem((2, D, D), BF16), vmem((2, 8, D), F32), vmem((2, 8, D), F32),
            vmem((H, D, D), BF16), vmem((2, NQ, D, D), BF16),
            vmem((H, 8, D), F32), vmem((2, NQ, 8, D), F32),
            vmem((2, NQ, D, D), BF16), vmem((H, D, D), BF16),
            vmem((2, NQ, 8, D), F32), vmem((H, 8, D), F32),
            vmem((NX, H, D, D), BF16), vmem((S, H, D, D), BF16),
            vmem((NX, G, 8, D), F32), vmem((S, G, 8, D), F32),
            vmem((S * T, H * D), BF16), vmem((2, NY, S * T, 256), F32),
            dma((7,)), dma((18,)), dma((4,)), dma((2, G)), dma((3, 2)), dma((2, G)), dma((2, G)),
            dma((15,)), dma((3,)), dma((3,)), dma((1,)), dma((2, 2)), pltpu.SemaphoreType.REGULAR, pltpu.SemaphoreType.REGULAR,
        ],
        compiler_params=pltpu.CompilerParams(
            collective_id=0, has_side_effects=True, vmem_limit_bytes=50_000_000
        ),
        name="cell_layer",
    )(*(pltpu.with_memory_space_constraint(array, pltpu.HBM) for array in arrays))
    return out.reshape(S, T, 4096)


def solution(mesh):
    return jax.shard_map(
        on_device,
        mesh=mesh,
        in_specs=(
            P("dp", None, "sp", None),
            P("dp", None, "sp", None),
            P("dp", None, "sp", None),
            P("dp", None, "sp"),
            P("dp", None, "sp"),
            P("dp", None, "sp", None),
            P("dp", None, "sp"),
            P("dp", None),
            P(),
            P(None, "dp"),
        ),
        out_specs=P("dp", "sp", None),
        check_vma=False,
    )
```

```python
import jax
import jax.numpy as jnp
from jax import lax
from jax.experimental import pallas as pl
from jax.experimental.pallas import tpu as pltpu
from jax.sharding import PartitionSpec as P

MESH = pl.DeviceIdType.MESH
F32 = jnp.float32
BF16 = jnp.bfloat16
S, H, T, D = 4, 8, 64, 128
NX, NZ, NY = 4, 8, 8
FACTOR = D**-0.5
NEG = -1e30
NQ = NZ // 2
G = 4
HG = H // G
RA = 768
RB = (1024 - RA) // NX


def nt(a, b):
    return lax.dot_general(a, b, (((1,), (1,)), ((), ())), preferred_element_type=F32)


def kernel(
    i_hbm, f_hbm, q_hbm, k_hbm, v_hbm, c_hbm, n_hbm, w_hbm, level_hbm, gain_hbm, out,
    qv, kv, vv, iv, fv, cv, nv, kx, vx, ix, fx, cx, nx, level, gain, wall, a_loc, num_s, den_s, amx_s,
    wrow, esum, amax, kvs, nkv, turn, cz_send, cz_recv, h_send, h_recv, hm_send, hm_recv, t_send, t_recv, tm_send, tm_recv,
    p_send, p_recv, pm_send, pm_recv, b_send, b_recv, bm_send, bm_recv, hid, acc,
    lsem, sent, xs_r, xk_r, tz_r, pz_r, xo_r, wy_r, wd_r, ws_r, wo_r, hr_r, hello, hello_far,
):
    sp = lax.axis_index("sp")
    dp = lax.axis_index("dp")
    x, z = lax.rem(sp, NX), lax.div(sp, NX)
    y, c = lax.div(dp, 2), lax.rem(dp, 2)
    zq = lax.rem(z, NQ)
    below = z - zq
    def xdev(d):
        return {"sp": z * NX + lax.rem(x + d, NX), "dp": dp}

    def zat(p):
        return {"sp": p * NX + x, "dp": dp}

    def ydev(d):
        return {"sp": sp, "dp": lax.rem(y + d + NY, NY) * 2 + c}

    mate = {"sp": sp, "dp": y * 2 + (1 - c)}

    def remote(src, dst, ssem, rsem, dev):
        return pltpu.make_async_remote_copy(
            src_ref=src, dst_ref=dst, send_sem=ssem, recv_sem=rsem,
            device_id=dev, device_id_type=MESH,
        )

    barrier = pltpu.get_barrier_semaphore()
    peers = [xdev(d) for d in range(1, NX)] + [ydev(1), ydev(-1), mate]
    for dev in peers:
        pl.semaphore_signal(barrier, inc=1, device_id=dev, device_id_type=MESH)
    for d in range(1, NZ):

        @pl.when(z + d < NZ)
        def _():
            dev = zat(lax.rem(z + d, NZ))
            pl.semaphore_signal(barrier, inc=1, device_id=dev, device_id_type=MESH)

    loads = [
        (i_hbm, iv, 0), (f_hbm, fv, 1), (k_hbm, kv, 2), (v_hbm, vv, 2), (w_hbm, wall.at[c, 0], 2), (q_hbm, qv, 2),
        (c_hbm, cv, 3), (n_hbm, nv, 4), (level_hbm, level, 5), (gain_hbm, gain, 6),
    ]
    for src, dst, k in loads:
        pltpu.make_async_copy(src, dst, lsem.at[k]).start()

    rows64 = lax.broadcasted_iota(jnp.int32, (T, T), 0)
    cols64 = lax.broadcasted_iota(jnp.int32, (T, T), 1)
    upper = jnp.where(rows64 <= cols64, 1.0, 0.0).astype(F32)
    causal = rows64 >= cols64

    def gates(li, f):
        li, f = li.astype(F32), f.astype(F32)
        lf = jnp.minimum(f, 0.0) - jnp.log1p(jnp.exp(-jnp.abs(f)))
        b = jnp.dot(lf, upper, precision=lax.Precision.HIGHEST, preferred_element_type=F32)
        return li - b, b[:, T - 1 : T]

    def arrived(ref, sem):
        pltpu.make_async_copy(ref, ref, sem).wait()

    with jax.named_scope("loads"):
        arrived(iv, lsem.at[0])
        arrived(fv, lsem.at[1])
    for j in range(S):
        a, _ = gates(iv[j], fv[j])
        a_loc[8 * j : 8 * j + 8, :] = a

    def block_gates(p, li, f):
        a, e = gates(li, f)
        am = jnp.max(a, axis=1, keepdims=True)
        esum[p] = jnp.broadcast_to(e, (H, D))
        amax[p] = jnp.broadcast_to(am, (H, D))
        wrow[p] = jnp.exp(a - am)

    block_gates(x, iv[x], fv[x])
    arrived(wall.at[c, 0:4], lsem.at[2])
    for k, ref in ((3, cv), (4, nv), (5, level), (6, gain)):
        arrived(ref, lsem.at[k])
    cx[x] = cv[x]
    nx[x] = nv[x]

    with jax.named_scope("barrier"):
        pl.semaphore_wait(barrier, len(peers) + z)
    for d in range(1, NQ):

        @pl.when(zq >= d)
        def _():
            dev = zat(lax.rem(z - d + NZ, NZ))
            pl.semaphore_signal(hello, inc=1, device_id=dev, device_id_type=MESH)

    @pl.when(z >= NQ)
    def _():
        pl.semaphore_signal(hello_far, inc=1, device_id=zat(lax.rem(z + NQ, NZ)), device_id_type=MESH)

    def rows_of(side, kind):
        if kind == "b":
            return pl.ds(pl.multiple_of(RA + RB * x, RB), RB)
        if kind == "half":
            return pl.ds(pl.multiple_of(RA + RB * x + side * (RB // 2), RB // 2), RB // 2)
        if kind == "cut":
            return pl.ds(256 + 128 * side, 128)
        return pl.ds(256 * (2 - kind if side else kind), 256)

    ring = [(0, "b"), (0, 0), (1, "b"), (0, 1), (2, "b"), (0, 2), (3, "half")]
    ring += [(1, 0), (1, 1), (1, 2), (2, 0), (2, 1), (2, 2), (3, 0), (3, "cut")]
    onward = {(0, "b"): (1, "b"), (1, "b"): (2, "b"), (2, "b"): (3, "half"), (2, 1): (3, "cut")}
    for k in range(3):
        onward[0, k], onward[1, k] = (1, k), (2, k)
    onward[2, 0] = (3, 0)

    def wsend(side, item):
        level, kind = item
        k = ring.index(item)
        rows = rows_of(side, kind)
        src, dst = (level, level + 1) if side else ((NY - level) % NY, NY - 1 - level)
        return remote(
            wall.at[c, src, rows], wall.at[c, dst, rows],
            sent.at[12], wy_r.at[k], ydev(-1 if side else 1),
        )

    def wmate(side, item):
        level, kind = item
        ref = wall.at[c, level + 1 if side else NY - 1 - level, rows_of(side, kind)]
        return remote(ref, ref, sent.at[13], wd_r.at[max(0, level - 1)], mate)

    def serve(level, kind):
        item = (level, kind)
        count = {"b": RB, "half": RB // 2, "cut": 128}.get(kind, 256)
        with jax.named_scope(f"serve{level}{kind}"):
            arrived(wall.at[c, 0:2, 0:count], wy_r.at[ring.index(item)])
        for side in (0, 1):
            if item in onward:
                wsend(side, onward[item]).start()
            if kind not in ("b", "half"):
                wmate(side, item).start()

    def begin(level, kind):
        for side in (0, 1):
            wsend(side, (level, kind)).start()

    def wspread(side, far):
        own = lax.rem(x + far * (1 if side else NX - 1), NX)
        start = pl.multiple_of(RA + RB * own + far * side * (RB // 2), RB // 2)
        ref = wall.at[c, 1:NY, pl.ds(start, RB // 2 if far else RB)]
        return remote(ref, ref, sent.at[14], ws_r.at[far], xdev(NX - 1 if side else 1))

    def wrest():
        ref = wall.at[c, 1:NY, RA:1024]
        return remote(ref, ref, sent.at[15], ws_r.at[2], mate)

    small = [(iv, ix), (fv, fx), (cv, cx), (nv, nx)]

    def xsmall(d):
        p = lax.rem(x + d, NX)
        return [
            remote(src.at[p], dst.at[x], sent.at[k], xs_r.at[k], xdev(d)) for k, (src, dst) in enumerate(small)
        ]

    def xkeys(d, g):
        p = lax.rem(x + d, NX)
        heads = pl.ds(g * HG, HG)
        return [
            remote(src.at[p, heads], dst.at[x, heads], sent.at[4], xk_r.at[k, g], xdev(d))
            for k, (src, dst) in enumerate([(kv, kx), (vv, vx)])
        ]

    begin(0, "b")
    begin(0, 0)
    for d in (2, 1, 3):
        for copy in xsmall(d):
            copy.start()
    for g in range(G):
        for d in (2, 1, 3):
            for copy in xkeys(d, g):
                copy.start()
    remote(wall.at[c, 0], wall.at[c, 0], sent.at[15], wo_r.at[0], mate).start()

    def intra(i):
        j, h = lax.div(i, H), lax.rem(i, H)
        arow = a_loc[pl.ds(i, 1), :]
        masked = jnp.where(causal, jnp.broadcast_to(arow, (T, T)), NEG)
        top = jnp.max(masked, axis=1, keepdims=True)
        weight = jnp.exp(masked - top)
        scores = nt(qv[j, h], kv[j, h]) * FACTOR * weight
        den_s[i] = jnp.broadcast_to(jnp.sum(scores, axis=1, keepdims=True), (T, D))
        amx_s[i] = jnp.broadcast_to(top, (T, D))
        num_s[i] = jnp.dot(scores.astype(BF16), vv[j, h], preferred_element_type=F32)

    def inner(part):
        def body(i, _):
            for u in range(4):
                intra(part * 8 + i * 4 + u)
            return 0

        with jax.named_scope("intra"):
            lax.fori_loop(0, 2, body, 0)

    def state(p, h, keys, values):
        w = wrow[p, pl.ds(h, 1), :]
        vt = values[p, h].astype(F32).T
        hi = w.astype(BF16)
        lo = (w - hi.astype(F32)).astype(BF16)
        rid = lax.broadcasted_iota(jnp.int32, (16, T), 0)
        extra = jnp.where(
            rid == 0,
            jnp.broadcast_to(hi.astype(F32), (16, T)),
            jnp.where(rid == 1, jnp.broadcast_to(lo.astype(F32), (16, T)), 0.0),
        )
        lhs = jnp.concatenate([(vt * w).astype(BF16), extra.astype(BF16)], axis=0)
        st = jnp.dot(lhs, keys[p, h], preferred_element_type=F32)
        kvs[p, h] = st[0:D]
        nkv[p, pl.ds(h, 1), :] = st[D : D + 1] + st[D + 1 : D + 2]

    def states(p, g):
        with jax.named_scope("states"):
            for u in range(HG):
                state(p, g * HG + u, kx, vx)

    inner(0)

    def own(i, _):
        for u in range(4):
            state(x, i * 4 + u, kv, vv)
        return 0

    lax.fori_loop(0, 2, own, 0)
    serve(0, "b")
    begin(0, 1)
    with jax.named_scope("xgates"):
        for k, (src, dst) in enumerate(small):
            arrived(dst.at[0:3], xs_r.at[k])
        for d in (1, 3, 2):
            p = lax.rem(x - d + NX, NX)
            block_gates(p, ix[p], fx[p])

    shift = []
    before = jnp.zeros((H, D), F32)
    top = None
    for i in range(NX):
        a = amax[i] - before
        shift.append(a)
        top = a if top is None else jnp.maximum(top, a)
        before = before + esum[i]
    scale = [jnp.exp(a - top) for a in shift]

    def tz(h):
        w = h // NQ
        to = zat(below + h % NQ)
        return [
            remote(tm_send.at[h], tm_recv.at[w, zq], sent.at[5], tz_r.at[0, w], to),
            remote(t_send.at[h], t_recv.at[w, zq], sent.at[6], tz_r.at[1, w], to),
        ]

    def total(g):
        with jax.named_scope(f"xin{g}"):
            for k, ref in enumerate((kx, vx)):
                arrived(ref.at[0:3, 0:HG], xk_r.at[k, g])
        for d in (1, 3, 2):
            states(lax.rem(x - d + NX, NX), g)
        for h in range(g * HG, g * HG + HG):
            ntot = sum(scale[i][h : h + 1] * nkv[i, h : h + 1, :] for i in range(NX))
            t_send[h] = sum(scale[i][h : h + 1] * kvs[i, h] for i in range(NX)).astype(BF16)
            tm_send[h, 0:1, :] = ntot
            tm_send[h, 1:2, :] = before[h : h + 1]
            tm_send[h, 2:3, :] = top[h : h + 1]

    def total_send(g):
        for h in range(g * HG, g * HG + HG):
            copies = tz(h)

            @pl.when(jnp.logical_and(zq != h % NQ, z < NZ - 1))
            def _():
                for copy in copies:
                    copy.start()

    def cz(o):
        return remote(cz_send.at[o], cz_recv.at[z], sent.at[7], tz_r.at[2, 0], zat(o))

    for i in range(NX):
        turn[4 * i : 4 * i + 4, 0:H] = nx[i]
        for h in range(H):
            at = 16 * (h // NQ) + 4 * i
            cz_send[h % NQ, at : at + 4, :] = cx[i, 4 * h : 4 * h + 4, :]
    first_lanes = lax.broadcasted_iota(jnp.int32, (H, D), 1) < 4 * NX
    nfirst = jnp.where(first_lanes, turn[...].T[0:H], 0.0)
    for h in range(H):
        cz_send[h % NQ, 32 + h // NQ : 33 + h // NQ, :] = nfirst[h : h + 1]

    def scan_step(w, i, cur, nrow, m):
        am = tm_recv[w, i, 2:3, :]
        hi = jnp.maximum(m, am)
        keep, add = jnp.exp(m - hi), jnp.exp(am - hi)
        cur = keep * cur + add * t_recv[w, i].astype(F32)
        nrow = keep * nrow + add * tm_recv[w, i, 0:1, :]
        return cur, nrow, tm_recv[w, i, 1:2, :] + hi

    def scan_states(g, head, cur, nrow, m):
        w = g // 2
        for i in range(NQ):
            p_send[w, i] = cur.astype(BF16)
            pm_send[w, i, 0:1, :] = nrow
            pm_send[w, i, 1:2, :] = m
            if i < NQ - 1:
                cur, nrow, m = scan_step(w, i, cur, nrow, m)
        return cur, nrow, m

    def scan_send(g, head):
        w = g // 2
        for i in range(NQ):

            @pl.when(zq != i)
            def _():
                to = zat(below + i)
                remote(pm_send.at[w, i], pm_recv.at[head], sent.at[8], pz_r.at[0, g], to).start()
                remote(p_send.at[w, i], p_recv.at[head], sent.at[9], pz_r.at[1, g], to).start()

            @pl.when(zq == i)
            def _():
                p_recv[head] = p_send[w, i]
                pm_recv[head] = pm_send[w, i]

    def totals_wait(w, count):
        arrived(tm_recv.at[w, 0:count], tz_r.at[0, w])
        arrived(t_recv.at[w, 0:count], tz_r.at[1, w])

    runs = lax.div(zq, 2)

    def scan(g):
        w = g // 2
        head = zq + NQ * w

        @pl.when(jnp.logical_and(runs == g % 2, z < NQ))
        def _():
            with jax.named_scope(f"zin{g}"):
                if w == 0:
                    arrived(cz_recv.at[0 : NZ - 1], tz_r.at[2, 0])
                    cz_recv[z] = cz_send[zq]
                    pl.semaphore_wait(hello_far, 1)
                totals_wait(w, NQ - 1)
            with jax.named_scope("scan"):
                t_recv[w, zq] = t_send[head]
                tm_recv[w, zq] = tm_send[head]
                lanes = lax.broadcasted_iota(jnp.int32, (1, H), 1)
                m = jnp.sum(jnp.where(lanes == head, level[pl.ds(x, 1), :], 0.0), axis=1, keepdims=True)
                m = jnp.broadcast_to(m, (1, D))
                nrow = cz_recv[0, 32 + w : 33 + w, :]
                for i in range(1, NZ):
                    nrow = nrow + pltpu.roll(cz_recv[i, 32 + w : 33 + w, :], 4 * NX * i, 1)
                cur = jnp.concatenate([cz_recv[i, 16 * w : 16 * w + 16, :] for i in range(NZ)], axis=0).T
                cur, nrow, m = scan_step(w, NQ - 1, *scan_states(g, head, cur, nrow, m))
                h_send[w] = cur.astype(BF16)
                hm_send[w, 0:1, :] = nrow
                hm_send[w, 1:2, :] = m
                to = zat(lax.rem(z + NQ, NZ))
                remote(hm_send.at[w], hm_recv.at[w], sent.at[16], hr_r.at[0, w], to).start()
                remote(h_send.at[w], h_recv.at[w], sent.at[17], hr_r.at[1, w], to).start()
                scan_send(g, head)

        @pl.when(jnp.logical_and(runs == g % 2, z >= NQ))
        def _():
            with jax.named_scope(f"zin{g}"):

                @pl.when(z < NZ - 1)
                def _():
                    totals_wait(w, NQ - 2)

                @pl.when(z == NZ - 1)
                def _():
                    totals_wait(w, NQ - 1)

                arrived(hm_recv.at[w], hr_r.at[0, w])
                arrived(h_recv.at[w], hr_r.at[1, w])
            with jax.named_scope("scan"):
                t_recv[w, zq] = t_send[head]
                tm_recv[w, zq] = tm_send[head]
                scan_states(g, head, h_recv[w].astype(F32), hm_recv[w, 0:1, :], hm_recv[w, 1:2, :])
                scan_send(g, head)

    def xo(d, g):
        p = lax.rem(x + d, NX)
        heads = pl.ds(g * HG, HG)
        return [
            remote(bm_send.at[p, g], bm_recv.at[x, g], sent.at[10], xo_r.at[0, g], xdev(d)),
            remote(b_send.at[p, heads], b_recv.at[x, heads], sent.at[11], xo_r.at[1, g], xdev(d)),
        ]

    def spread(g):
        with jax.named_scope(f"zout{g}"):

            @pl.when(runs == g % 2)
            def _():
                for k, ref in enumerate((pm_recv, p_recv)):
                    arrived(ref.at[0 : HG - 1], pz_r.at[k, g])

            @pl.when(runs != g % 2)
            def _():
                for k, ref in enumerate((pm_recv, p_recv)):
                    arrived(ref.at[0:HG], pz_r.at[k, g])

        for u in range(HG):
            h = g * HG + u
            cur = p_recv[h].astype(F32)
            nrow = pm_recv[h, 0:1, :]
            m = pm_recv[h, 1:2, :]
            for i in range(NX):
                b_send[i, h] = cur.astype(BF16)
                bm_send[i, g, 2 * u : 2 * u + 1, :] = nrow
                bm_send[i, g, 2 * u + 1 : 2 * u + 2, :] = m
                if i < NX - 1:
                    am = amax[i, h : h + 1, :]
                    hi = jnp.maximum(m, am)
                    keep, add = jnp.exp(m - hi), jnp.exp(am - hi)
                    cur = keep * cur + add * kvs[i, h]
                    nrow = keep * nrow + add * nkv[i, h : h + 1, :]
                    m = esum[i, h : h + 1, :] + hi
        for d in (2, 1, 3):
            for copy in xo(d, g):
                copy.start()
        heads = pl.ds(g * HG, HG)
        b_recv[x, heads] = b_send[x, heads]
        bm_recv[x, g] = bm_send[x, g]

    def finish_one(j, g):
        for u in range(HG):
            h = g * HG + u
            i = j * H + h
            q = qv[j, h]
            nrow = bm_recv[j, g, 2 * u : 2 * u + 1, :]
            m = bm_recv[j, g, 2 * u + 1 : 2 * u + 2, :]
            qc = nt(q, b_recv[j, h])
            qn = jnp.sum(q.astype(F32) * nrow, axis=1, keepdims=True)
            a = amx_s[i]
            hi = jnp.maximum(a, m)
            keep, add = jnp.exp(m - hi) * FACTOR, jnp.exp(a - hi)
            den = add * den_s[i] + keep * qn
            num = add * num_s[i] + keep * qc
            o = (num / jnp.maximum(jnp.abs(den), 1.0)).astype(BF16)
            normed = (o.astype(F32) * gain[h : h + 1, :]).astype(BF16)
            hid[pl.ds(pl.multiple_of(j * T, T), T), h * D : h * D + D] = normed

    def finish(g):
        with jax.named_scope("finish"):
            finish_one(x, g)
        with jax.named_scope(f"xout{g}"):
            arrived(bm_recv.at[0:3, 0], xo_r.at[0, g])
            arrived(b_recv.at[0:3, 0:HG], xo_r.at[1, g])
        with jax.named_scope("finish"):
            for d in (1, 3, 2):
                finish_one(lax.rem(x - d + NX, NX), g)

    def columns(core, r):
        block = lax.rem(y + r, NY) * 2 + core
        return pl.ds(pl.multiple_of(block * 256, 256), 256)

    def early_one(r):
        for core in (0, 1):
            acc[core, r] = jnp.dot(hid[:, 0:RA], wall[core, r, 0:RA], preferred_element_type=F32)

    def late_one(r):
        for core in (0, 1):
            part = jnp.dot(hid[:, RA:1024], wall[core, r, RA:1024], preferred_element_type=F32)
            out[:, columns(core, r)] = (acc[core, r] + part).astype(BF16)

    def twos(name, fn, low, high):
        def body(i, _):
            fn(lax.rem(NY - 2 + 2 * i, NY))
            fn(lax.rem(NY - 1 + 2 * i, NY))
            return 0

        with jax.named_scope(name):
            lax.fori_loop(low, high, body, 0)

    def last():
        with jax.named_scope("last"):
            for core in (0, 1):
                whole = jnp.dot(hid[...], wall[core, NY // 2], preferred_element_type=F32)
                out[:, columns(core, NY // 2)] = whole.astype(BF16)

    def mates(level):
        with jax.named_scope("mate"):
            count = (4, 2, 1)[level]
            arrived(wall.at[c, 0:count, 0:RA], wd_r.at[level])

    def zgate():
        with jax.named_scope("zgate"):

            @pl.when(zq < NQ - 1)
            def _():
                pl.semaphore_wait(hello, NQ - 1 - zq)

    def cz_all():
        for o in range(NQ):

            @pl.when(z != o)
            def _():
                cz(o).start()


    def wspread_start():
        wspread(0, 0).start()
        wspread(1, 0).start()

    def wspread_near():
        with jax.named_scope("wnear"):
            arrived(wall.at[c, 1:NY, 0 : 2 * RB], ws_r.at[0])
        wspread(0, 1).start()
        wspread(1, 1).start()

    def wspread_done():
        with jax.named_scope("wspread"):
            arrived(wall.at[c, 1:NY, 0:RB], ws_r.at[1])
        wrest().start()

    def sent_cell():
        for k, ref in enumerate((iv, fv, cv, nv)):
            arrived(ref.at[0:3], sent.at[k])
        arrived(b_send.at[0:3], sent.at[4])
        arrived(pm_send.at[:, 0 : NQ - 1], sent.at[8])
        arrived(p_send.at[:, 0 : NQ - 1], sent.at[9])

        @pl.when(z < NZ - 1)
        def _():
            arrived(tm_send.at[0 : H - 2], sent.at[5])
            arrived(t_send.at[0 : H - 2], sent.at[6])

        @pl.when(z < NQ)
        def _():
            arrived(cz_send.at[0 : NQ - 1], sent.at[7])
            arrived(hm_send, sent.at[16])
            arrived(h_send, sent.at[17])

        @pl.when(z >= NQ)
        def _():
            arrived(cz_send, sent.at[7])

        arrived(wall.at[c, 1:NY, 0 : 3 * RB], sent.at[14])

    def sent_rest():
        arrived(bm_send.at[0:3], sent.at[10])
        arrived(b_send.at[0:3], sent.at[11])
        arrived(wall.at[c, :, 0:352], sent.at[15])

    def sent_ring():
        arrived(wall.at[c, 1:NY, 0:832], sent.at[12])
        arrived(wall.at[c, 1:NY, 0:768], sent.at[13])

    @pl.when(z >= NZ // 2)
    def _():
        zgate()
        cz_all()

    inner(1)
    serve(1, "b")
    begin(0, 2)
    total(0)

    @pl.when(z < NZ // 2)
    def _():
        zgate()
        total_send(0)
        cz_all()
        inner(2)
        total(1)
        total_send(1)
        serve(2, "b")
        serve(0, 0)
        serve(0, 1)
        inner(3)
        total(2)
        total_send(2)
        serve(3, "half")
        wspread_start()
        serve(0, 2)
        total(3)
        total_send(3)
        scan(1)
        scan(0)
        serve(1, 0)
        scan(2)
        serve(1, 1)
        wspread_near()
        scan(3)
        spread(0)
        spread(1)
        serve(1, 2)
        spread(2)
        serve(2, 0)
        spread(3)
        serve(2, 1)
        finish(0)
        wspread_done()
        sent_cell()
        serve(2, 2)
        finish(1)
        arrived(wall.at[c, 0], wo_r.at[0])
        mates(0)
        finish(2)
        twos("early", early_one, 0, 2)
        serve(3, 0)
        mates(1)
        with jax.named_scope("early"):
            early_one(2)
            early_one(3)
            early_one(5)
        serve(3, "cut")
        finish(3)

    @pl.when(z >= NZ // 2)
    def _():
        total_send(0)
        inner(2)
        total(1)
        total_send(1)
        serve(2, "b")
        serve(0, 0)
        serve(0, 1)
        inner(3)
        total(2)
        total_send(2)
        serve(3, "half")
        wspread_start()
        serve(0, 2)
        total(3)
        total_send(3)
        serve(1, 0)
        scan(0)
        scan(1)
        serve(1, 1)
        wspread_near()
        spread(0)
        scan(2)
        scan(3)
        spread(1)
        serve(1, 2)
        spread(2)
        serve(2, 0)
        spread(3)
        serve(2, 1)
        finish(0)
        wspread_done()
        sent_cell()
        serve(2, 2)
        finish(1)
        arrived(wall.at[c, 0], wo_r.at[0])
        mates(0)
        finish(2)
        twos("early", early_one, 0, 2)
        serve(3, 0)
        mates(1)
        with jax.named_scope("early"):
            early_one(2)
            early_one(3)
            early_one(5)
        serve(3, "cut")
        finish(3)

    arrived(wall.at[c, 1:NY, RA:1024], ws_r.at[2])
    twos("late", late_one, 0, 3)
    with jax.named_scope("late"):
        late_one(5)
    sent_rest()
    mates(2)
    last()
    sent_ring()


def on_device(queries, keys, values, input_gate, forget_gate, start_memory, start_norm, start_level, head_gain, out_weight):
    arrays = (
        input_gate, forget_gate, queries, keys, values, start_memory.reshape(S, 32, D),
        jnp.transpose(start_norm, (0, 2, 1)), out_weight, start_level, head_gain,
    )
    dma, vmem = pltpu.SemaphoreType.DMA, pltpu.VMEM
    out = pl.pallas_call(
        kernel,
        out_shape=pltpu.VMEM((S * T, 4096), BF16),
        in_specs=[pl.BlockSpec(memory_space=pltpu.HBM)] * len(arrays),
        out_specs=pl.BlockSpec(memory_space=pltpu.VMEM),
        scratch_shapes=[
            vmem((S, H, T, D), BF16), vmem((S, H, T, D), BF16), vmem((S, H, T, D), BF16),
            vmem((S, H, T), BF16), vmem((S, H, T), BF16), vmem((S, 32, D), F32), vmem((S, 4, H), F32),
            vmem((NX, H, T, D), BF16), vmem((NX, H, T, D), BF16),
            vmem((NX, H, T), BF16), vmem((NX, H, T), BF16), vmem((NX, 32, D), F32), vmem((NX, 4, H), F32),
            vmem((S, H), F32), vmem((H, D), F32),
            vmem((2, NY, 1024, 256), BF16),
            vmem((S * H, T), F32),
            vmem((S * H, T, D), F32), vmem((S * H, T, D), F32), vmem((S * H, T, D), F32),
            vmem((NX, H, T), F32), vmem((NX, H, D), F32), vmem((NX, H, D), F32),
            vmem((NX, H, D, D), F32), vmem((NX, H, D), F32), vmem((D, D), F32),
            vmem((NQ, 40, D), F32), vmem((NZ, 40, D), F32),
            vmem((2, D, D), BF16), vmem((2, D, D), BF16), vmem((2, 8, D), F32), vmem((2, 8, D), F32),
            vmem((H, D, D), BF16), vmem((2, NQ, D, D), BF16),
            vmem((H, 8, D), F32), vmem((2, NQ, 8, D), F32),
            vmem((2, NQ, D, D), BF16), vmem((H, D, D), BF16),
            vmem((2, NQ, 8, D), F32), vmem((H, 8, D), F32),
            vmem((NX, H, D, D), BF16), vmem((S, H, D, D), BF16),
            vmem((NX, G, 8, D), F32), vmem((S, G, 8, D), F32),
            vmem((S * T, H * D), BF16), vmem((2, NY, S * T, 256), F32),
            dma((7,)), dma((18,)), dma((4,)), dma((2, G)), dma((3, 2)), dma((2, G)), dma((2, G)),
            dma((15,)), dma((3,)), dma((3,)), dma((1,)), dma((2, 2)), pltpu.SemaphoreType.REGULAR, pltpu.SemaphoreType.REGULAR,
        ],
        compiler_params=pltpu.CompilerParams(
            collective_id=0, has_side_effects=True, vmem_limit_bytes=50_000_000
        ),
        name="cell_layer",
    )(*(pltpu.with_memory_space_constraint(array, pltpu.HBM) for array in arrays))
    return out.reshape(S, T, 4096)


def solution(mesh):
    return jax.shard_map(
        on_device,
        mesh=mesh,
        in_specs=(
            P("dp", None, "sp", None),
            P("dp", None, "sp", None),
            P("dp", None, "sp", None),
            P("dp", None, "sp"),
            P("dp", None, "sp"),
            P("dp", None, "sp", None),
            P("dp", None, "sp"),
            P("dp", None),
            P(),
            P(None, "dp"),
        ),
        out_specs=P("dp", "sp", None),
        check_vma=False,
    )
```

```python
import jax
import jax.numpy as jnp
from jax import lax
from jax.experimental import pallas as pl
from jax.experimental.pallas import tpu as pltpu
from jax.sharding import PartitionSpec as P

MESH = pl.DeviceIdType.MESH
F32 = jnp.float32
BF16 = jnp.bfloat16
S, H, T, D = 4, 8, 64, 128
NX, NZ, NY = 4, 8, 8
FACTOR = D**-0.5
NEG = -1e30
NQ = NZ // 2
G = 4
HG = H // G
RA = 768
RB = (1024 - RA) // NX


def nt(a, b):
    return lax.dot_general(a, b, (((1,), (1,)), ((), ())), preferred_element_type=F32)


def kernel(
    i_hbm, f_hbm, q_hbm, k_hbm, v_hbm, c_hbm, n_hbm, w_hbm, level_hbm, gain_hbm, out,
    qv, kv, vv, iv, fv, cv, nv, kx, vx, ix, fx, cx, nx, level, gain, wall, a_loc, num_s, den_s, amx_s,
    wrow, esum, amax, kvs, nkv, turn, cz_send, cz_recv, h_send, h_recv, hm_send, hm_recv, t_send, t_recv, tm_send, tm_recv,
    p_send, p_recv, pm_send, pm_recv, b_send, b_recv, bm_send, bm_recv, hid, acc,
    lsem, sent, xs_r, xk_r, tz_r, pz_r, xo_r, wy_r, wd_r, ws_r, wo_r, hr_r, hello, hello_far,
):
    sp = lax.axis_index("sp")
    dp = lax.axis_index("dp")
    x, z = lax.rem(sp, NX), lax.div(sp, NX)
    y, c = lax.div(dp, 2), lax.rem(dp, 2)
    zq = lax.rem(z, NQ)
    below = z - zq
    def xdev(d):
        return {"sp": z * NX + lax.rem(x + d, NX), "dp": dp}

    def zat(p):
        return {"sp": p * NX + x, "dp": dp}

    def ydev(d):
        return {"sp": sp, "dp": lax.rem(y + d + NY, NY) * 2 + c}

    mate = {"sp": sp, "dp": y * 2 + (1 - c)}

    def remote(src, dst, ssem, rsem, dev):
        return pltpu.make_async_remote_copy(
            src_ref=src, dst_ref=dst, send_sem=ssem, recv_sem=rsem,
            device_id=dev, device_id_type=MESH,
        )

    barrier = pltpu.get_barrier_semaphore()
    peers = [xdev(d) for d in range(1, NX)] + [ydev(1), ydev(-1), mate]
    for dev in peers:
        pl.semaphore_signal(barrier, inc=1, device_id=dev, device_id_type=MESH)
    for d in range(1, NZ):

        @pl.when(z + d < NZ)
        def _():
            dev = zat(lax.rem(z + d, NZ))
            pl.semaphore_signal(barrier, inc=1, device_id=dev, device_id_type=MESH)

    loads = [
        (i_hbm, iv, 0), (f_hbm, fv, 1), (k_hbm, kv, 2), (v_hbm, vv, 2), (w_hbm, wall.at[c, 0], 2), (q_hbm, qv, 2),
        (c_hbm, cv, 3), (n_hbm, nv, 4), (level_hbm, level, 5), (gain_hbm, gain, 6),
    ]
    for src, dst, k in loads:
        pltpu.make_async_copy(src, dst, lsem.at[k]).start()

    rows64 = lax.broadcasted_iota(jnp.int32, (T, T), 0)
    cols64 = lax.broadcasted_iota(jnp.int32, (T, T), 1)
    upper = jnp.where(rows64 <= cols64, 1.0, 0.0).astype(F32)
    causal = rows64 >= cols64

    def gates(li, f):
        li, f = li.astype(F32), f.astype(F32)
        lf = jnp.minimum(f, 0.0) - jnp.log1p(jnp.exp(-jnp.abs(f)))
        b = jnp.dot(lf, upper, precision=lax.Precision.HIGHEST, preferred_element_type=F32)
        return li - b, b[:, T - 1 : T]

    def arrived(ref, sem):
        pltpu.make_async_copy(ref, ref, sem).wait()

    with jax.named_scope("loads"):
        arrived(iv, lsem.at[0])
        arrived(fv, lsem.at[1])
    for j in range(S):
        a, _ = gates(iv[j], fv[j])
        a_loc[8 * j : 8 * j + 8, :] = a

    def block_gates(p, li, f):
        a, e = gates(li, f)
        am = jnp.max(a, axis=1, keepdims=True)
        esum[p] = jnp.broadcast_to(e, (H, D))
        amax[p] = jnp.broadcast_to(am, (H, D))
        wrow[p] = jnp.exp(a - am)

    block_gates(x, iv[x], fv[x])
    arrived(wall.at[c, 0:4], lsem.at[2])
    for k, ref in ((3, cv), (4, nv), (5, level), (6, gain)):
        arrived(ref, lsem.at[k])
    cx[x] = cv[x]
    nx[x] = nv[x]

    with jax.named_scope("barrier"):
        pl.semaphore_wait(barrier, len(peers) + z)
    for d in range(1, NQ):

        @pl.when(zq >= d)
        def _():
            dev = zat(lax.rem(z - d + NZ, NZ))
            pl.semaphore_signal(hello, inc=1, device_id=dev, device_id_type=MESH)

    @pl.when(z >= NQ)
    def _():
        pl.semaphore_signal(hello_far, inc=1, device_id=zat(lax.rem(z + NQ, NZ)), device_id_type=MESH)

    def rows_of(side, kind):
        if kind == "b":
            return pl.ds(pl.multiple_of(RA + RB * x, RB), RB)
        if kind == "half":
            return pl.ds(pl.multiple_of(RA + RB * x + side * (RB // 2), RB // 2), RB // 2)
        if kind == "cut":
            return pl.ds(256 + 128 * side, 128)
        return pl.ds(256 * (2 - kind if side else kind), 256)

    ring = [(0, "b"), (0, 0), (1, "b"), (0, 1), (2, "b"), (0, 2), (3, "half")]
    ring += [(1, 0), (1, 1), (1, 2), (2, 0), (2, 1), (2, 2), (3, 0), (3, "cut")]
    onward = {(0, "b"): (1, "b"), (1, "b"): (2, "b"), (2, "b"): (3, "half"), (2, 1): (3, "cut")}
    for k in range(3):
        onward[0, k], onward[1, k] = (1, k), (2, k)
    onward[2, 0] = (3, 0)

    def wsend(side, item):
        level, kind = item
        k = ring.index(item)
        rows = rows_of(side, kind)
        src, dst = (level, level + 1) if side else ((NY - level) % NY, NY - 1 - level)
        return remote(
            wall.at[c, src, rows], wall.at[c, dst, rows],
            sent.at[12], wy_r.at[k], ydev(-1 if side else 1),
        )

    def wmate(side, item):
        level, kind = item
        ref = wall.at[c, level + 1 if side else NY - 1 - level, rows_of(side, kind)]
        return remote(ref, ref, sent.at[13], wd_r.at[max(0, level - 1)], mate)

    def serve(level, kind):
        item = (level, kind)
        count = {"b": RB, "half": RB // 2, "cut": 128}.get(kind, 256)
        with jax.named_scope(f"serve{level}{kind}"):
            arrived(wall.at[c, 0:2, 0:count], wy_r.at[ring.index(item)])
        for side in (0, 1):
            if item in onward:
                wsend(side, onward[item]).start()
            if kind not in ("b", "half"):
                wmate(side, item).start()

    def begin(level, kind):
        for side in (0, 1):
            wsend(side, (level, kind)).start()

    def wspread(side, far):
        own = lax.rem(x + far * (1 if side else NX - 1), NX)
        start = pl.multiple_of(RA + RB * own + far * side * (RB // 2), RB // 2)
        ref = wall.at[c, 1:NY, pl.ds(start, RB // 2 if far else RB)]
        return remote(ref, ref, sent.at[14], ws_r.at[far], xdev(NX - 1 if side else 1))

    def wrest():
        ref = wall.at[c, 1:NY, RA:1024]
        return remote(ref, ref, sent.at[15], ws_r.at[2], mate)

    small = [(iv, ix), (fv, fx), (cv, cx), (nv, nx)]

    def xsmall(d):
        p = lax.rem(x + d, NX)
        return [
            remote(src.at[p], dst.at[x], sent.at[k], xs_r.at[k], xdev(d)) for k, (src, dst) in enumerate(small)
        ]

    def xkeys(d, g):
        p = lax.rem(x + d, NX)
        heads = pl.ds(g * HG, HG)
        return [
            remote(src.at[p, heads], dst.at[x, heads], sent.at[4], xk_r.at[k, g], xdev(d))
            for k, (src, dst) in enumerate([(kv, kx), (vv, vx)])
        ]

    begin(0, "b")
    begin(0, 0)
    for d in (2, 1, 3):
        for copy in xsmall(d):
            copy.start()
    for g in range(G):
        for d in (2, 1, 3):
            for copy in xkeys(d, g):
                copy.start()
    remote(wall.at[c, 0], wall.at[c, 0], sent.at[15], wo_r.at[0], mate).start()

    def intra(i):
        j, h = lax.div(i, H), lax.rem(i, H)
        arow = a_loc[pl.ds(i, 1), :]
        masked = jnp.where(causal, jnp.broadcast_to(arow, (T, T)), NEG)
        top = jnp.max(masked, axis=1, keepdims=True)
        weight = jnp.exp(masked - top)
        scores = nt(qv[j, h], kv[j, h]) * FACTOR * weight
        den_s[i] = jnp.broadcast_to(jnp.sum(scores, axis=1, keepdims=True), (T, D))
        amx_s[i] = jnp.broadcast_to(top, (T, D))
        num_s[i] = jnp.dot(scores.astype(BF16), vv[j, h], preferred_element_type=F32)

    def inner(part):
        def body(i, _):
            for u in range(4):
                intra(part * 8 + i * 4 + u)
            return 0

        with jax.named_scope("intra"):
            lax.fori_loop(0, 2, body, 0)

    def state(p, h, keys, values):
        w = wrow[p, pl.ds(h, 1), :]
        vt = values[p, h].astype(F32).T
        hi = w.astype(BF16)
        lo = (w - hi.astype(F32)).astype(BF16)
        rid = lax.broadcasted_iota(jnp.int32, (16, T), 0)
        extra = jnp.where(
            rid == 0,
            jnp.broadcast_to(hi.astype(F32), (16, T)),
            jnp.where(rid == 1, jnp.broadcast_to(lo.astype(F32), (16, T)), 0.0),
        )
        lhs = jnp.concatenate([(vt * w).astype(BF16), extra.astype(BF16)], axis=0)
        st = jnp.dot(lhs, keys[p, h], preferred_element_type=F32)
        kvs[p, h] = st[0:D]
        nkv[p, pl.ds(h, 1), :] = st[D : D + 1] + st[D + 1 : D + 2]

    def states(p, g):
        with jax.named_scope("states"):
            for u in range(HG):
                state(p, g * HG + u, kx, vx)

    inner(0)

    def own(i, _):
        for u in range(4):
            state(x, i * 4 + u, kv, vv)
        return 0

    lax.fori_loop(0, 2, own, 0)
    serve(0, "b")
    begin(0, 1)
    with jax.named_scope("xgates"):
        for k, (src, dst) in enumerate(small):
            arrived(dst.at[0:3], xs_r.at[k])
        for d in (1, 3, 2):
            p = lax.rem(x - d + NX, NX)
            block_gates(p, ix[p], fx[p])

    shift = []
    before = jnp.zeros((H, D), F32)
    top = None
    for i in range(NX):
        a = amax[i] - before
        shift.append(a)
        top = a if top is None else jnp.maximum(top, a)
        before = before + esum[i]
    scale = [jnp.exp(a - top) for a in shift]

    def tz(h):
        w = h // NQ
        to = zat(below + h % NQ)
        return [
            remote(tm_send.at[h], tm_recv.at[w, zq], sent.at[5], tz_r.at[0, w], to),
            remote(t_send.at[h], t_recv.at[w, zq], sent.at[6], tz_r.at[1, w], to),
        ]

    def total(g):
        with jax.named_scope(f"xin{g}"):
            for k, ref in enumerate((kx, vx)):
                arrived(ref.at[0:3, 0:HG], xk_r.at[k, g])
        for d in (1, 3, 2):
            states(lax.rem(x - d + NX, NX), g)
        for h in range(g * HG, g * HG + HG):
            ntot = sum(scale[i][h : h + 1] * nkv[i, h : h + 1, :] for i in range(NX))
            t_send[h] = sum(scale[i][h : h + 1] * kvs[i, h] for i in range(NX)).astype(BF16)
            tm_send[h, 0:1, :] = ntot
            tm_send[h, 1:2, :] = before[h : h + 1]
            tm_send[h, 2:3, :] = top[h : h + 1]

    def total_send(g):
        for h in range(g * HG, g * HG + HG):
            copies = tz(h)

            @pl.when(jnp.logical_and(zq != h % NQ, z < NZ - 1))
            def _():
                for copy in copies:
                    copy.start()

    def cz(o):
        return remote(cz_send.at[o], cz_recv.at[z], sent.at[7], tz_r.at[2, 0], zat(o))

    for i in range(NX):
        turn[4 * i : 4 * i + 4, 0:H] = nx[i]
        for h in range(H):
            at = 16 * (h // NQ) + 4 * i
            cz_send[h % NQ, at : at + 4, :] = cx[i, 4 * h : 4 * h + 4, :]
    first_lanes = lax.broadcasted_iota(jnp.int32, (H, D), 1) < 4 * NX
    nfirst = jnp.where(first_lanes, turn[...].T[0:H], 0.0)
    for h in range(H):
        cz_send[h % NQ, 32 + h // NQ : 33 + h // NQ, :] = nfirst[h : h + 1]

    def scan_step(w, i, cur, nrow, m):
        am = tm_recv[w, i, 2:3, :]
        hi = jnp.maximum(m, am)
        keep, add = jnp.exp(m - hi), jnp.exp(am - hi)
        cur = keep * cur + add * t_recv[w, i].astype(F32)
        nrow = keep * nrow + add * tm_recv[w, i, 0:1, :]
        return cur, nrow, tm_recv[w, i, 1:2, :] + hi

    def scan_states(g, head, cur, nrow, m):
        w = g // 2
        for i in range(NQ):
            p_send[w, i] = cur.astype(BF16)
            pm_send[w, i, 0:1, :] = nrow
            pm_send[w, i, 1:2, :] = m
            if i < NQ - 1:
                cur, nrow, m = scan_step(w, i, cur, nrow, m)
        return cur, nrow, m

    def scan_send(g, head):
        w = g // 2
        for i in reversed(range(NQ)):

            @pl.when(zq != i)
            def _():
                to = zat(below + i)
                remote(pm_send.at[w, i], pm_recv.at[head], sent.at[8], pz_r.at[0, g], to).start()
                remote(p_send.at[w, i], p_recv.at[head], sent.at[9], pz_r.at[1, g], to).start()

            @pl.when(zq == i)
            def _():
                p_recv[head] = p_send[w, i]
                pm_recv[head] = pm_send[w, i]

    def totals_wait(w, count):
        arrived(tm_recv.at[w, 0:count], tz_r.at[0, w])
        arrived(t_recv.at[w, 0:count], tz_r.at[1, w])

    runs = lax.div(zq, 2)

    def scan(g):
        w = g // 2
        head = zq + NQ * w

        @pl.when(jnp.logical_and(runs == g % 2, z < NQ))
        def _():
            with jax.named_scope(f"zin{g}"):
                if w == 0:
                    arrived(cz_recv.at[0 : NZ - 1], tz_r.at[2, 0])
                    cz_recv[z] = cz_send[zq]
                    pl.semaphore_wait(hello_far, 1)
                totals_wait(w, NQ - 1)
            with jax.named_scope("scan"):
                t_recv[w, zq] = t_send[head]
                tm_recv[w, zq] = tm_send[head]
                lanes = lax.broadcasted_iota(jnp.int32, (1, H), 1)
                m = jnp.sum(jnp.where(lanes == head, level[pl.ds(x, 1), :], 0.0), axis=1, keepdims=True)
                m = jnp.broadcast_to(m, (1, D))
                nrow = cz_recv[0, 32 + w : 33 + w, :]
                for i in range(1, NZ):
                    nrow = nrow + pltpu.roll(cz_recv[i, 32 + w : 33 + w, :], 4 * NX * i, 1)
                cur = jnp.concatenate([cz_recv[i, 16 * w : 16 * w + 16, :] for i in range(NZ)], axis=0).T
                cur, nrow, m = scan_step(w, NQ - 1, *scan_states(g, head, cur, nrow, m))
                h_send[w] = cur.astype(BF16)
                hm_send[w, 0:1, :] = nrow
                hm_send[w, 1:2, :] = m
                to = zat(lax.rem(z + NQ, NZ))
                remote(hm_send.at[w], hm_recv.at[w], sent.at[16], hr_r.at[0, w], to).start()
                remote(h_send.at[w], h_recv.at[w], sent.at[17], hr_r.at[1, w], to).start()
                scan_send(g, head)

        @pl.when(jnp.logical_and(runs == g % 2, z >= NQ))
        def _():
            with jax.named_scope(f"zin{g}"):

                @pl.when(z < NZ - 1)
                def _():
                    totals_wait(w, NQ - 2)

                @pl.when(z == NZ - 1)
                def _():
                    totals_wait(w, NQ - 1)

                arrived(hm_recv.at[w], hr_r.at[0, w])
                arrived(h_recv.at[w], hr_r.at[1, w])
            with jax.named_scope("scan"):
                t_recv[w, zq] = t_send[head]
                tm_recv[w, zq] = tm_send[head]
                scan_states(g, head, h_recv[w].astype(F32), hm_recv[w, 0:1, :], hm_recv[w, 1:2, :])
                scan_send(g, head)

    def xo(d, g):
        p = lax.rem(x + d, NX)
        heads = pl.ds(g * HG, HG)
        return [
            remote(bm_send.at[p, g], bm_recv.at[x, g], sent.at[10], xo_r.at[0, g], xdev(d)),
            remote(b_send.at[p, heads], b_recv.at[x, heads], sent.at[11], xo_r.at[1, g], xdev(d)),
        ]

    def spread(g):
        with jax.named_scope(f"zout{g}"):

            @pl.when(runs == g % 2)
            def _():
                for k, ref in enumerate((pm_recv, p_recv)):
                    arrived(ref.at[0 : HG - 1], pz_r.at[k, g])

            @pl.when(runs != g % 2)
            def _():
                for k, ref in enumerate((pm_recv, p_recv)):
                    arrived(ref.at[0:HG], pz_r.at[k, g])

        for u in range(HG):
            h = g * HG + u
            cur = p_recv[h].astype(F32)
            nrow = pm_recv[h, 0:1, :]
            m = pm_recv[h, 1:2, :]
            for i in range(NX):
                b_send[i, h] = cur.astype(BF16)
                bm_send[i, g, 2 * u : 2 * u + 1, :] = nrow
                bm_send[i, g, 2 * u + 1 : 2 * u + 2, :] = m
                if i < NX - 1:
                    am = amax[i, h : h + 1, :]
                    hi = jnp.maximum(m, am)
                    keep, add = jnp.exp(m - hi), jnp.exp(am - hi)
                    cur = keep * cur + add * kvs[i, h]
                    nrow = keep * nrow + add * nkv[i, h : h + 1, :]
                    m = esum[i, h : h + 1, :] + hi
        for d in (2, 1, 3):
            for copy in xo(d, g):
                copy.start()
        heads = pl.ds(g * HG, HG)
        b_recv[x, heads] = b_send[x, heads]
        bm_recv[x, g] = bm_send[x, g]

    def finish_one(j, g):
        for u in range(HG):
            h = g * HG + u
            i = j * H + h
            q = qv[j, h]
            nrow = bm_recv[j, g, 2 * u : 2 * u + 1, :]
            m = bm_recv[j, g, 2 * u + 1 : 2 * u + 2, :]
            qc = nt(q, b_recv[j, h])
            qn = jnp.sum(q.astype(F32) * nrow, axis=1, keepdims=True)
            a = amx_s[i]
            hi = jnp.maximum(a, m)
            keep, add = jnp.exp(m - hi) * FACTOR, jnp.exp(a - hi)
            den = add * den_s[i] + keep * qn
            num = add * num_s[i] + keep * qc
            o = (num / jnp.maximum(jnp.abs(den), 1.0)).astype(BF16)
            normed = (o.astype(F32) * gain[h : h + 1, :]).astype(BF16)
            hid[pl.ds(pl.multiple_of(j * T, T), T), h * D : h * D + D] = normed

    def finish(g):
        with jax.named_scope("finish"):
            finish_one(x, g)
        with jax.named_scope(f"xout{g}"):
            arrived(bm_recv.at[0:3, 0], xo_r.at[0, g])
            arrived(b_recv.at[0:3, 0:HG], xo_r.at[1, g])
        with jax.named_scope("finish"):
            for d in (1, 3, 2):
                finish_one(lax.rem(x - d + NX, NX), g)

    def columns(core, r):
        block = lax.rem(y + r, NY) * 2 + core
        return pl.ds(pl.multiple_of(block * 256, 256), 256)

    def early_one(r):
        for core in (0, 1):
            acc[core, r] = jnp.dot(hid[:, 0:RA], wall[core, r, 0:RA], preferred_element_type=F32)

    def late_one(r):
        for core in (0, 1):
            part = jnp.dot(hid[:, RA:1024], wall[core, r, RA:1024], preferred_element_type=F32)
            out[:, columns(core, r)] = (acc[core, r] + part).astype(BF16)

    def twos(name, fn, low, high):
        def body(i, _):
            fn(lax.rem(NY - 2 + 2 * i, NY))
            fn(lax.rem(NY - 1 + 2 * i, NY))
            return 0

        with jax.named_scope(name):
            lax.fori_loop(low, high, body, 0)

    def last():
        with jax.named_scope("last"):
            for core in (0, 1):
                whole = jnp.dot(hid[...], wall[core, NY // 2], preferred_element_type=F32)
                out[:, columns(core, NY // 2)] = whole.astype(BF16)

    def mates(level):
        with jax.named_scope("mate"):
            count = (4, 2, 1)[level]
            arrived(wall.at[c, 0:count, 0:RA], wd_r.at[level])

    def zgate():
        with jax.named_scope("zgate"):

            @pl.when(zq < NQ - 1)
            def _():
                pl.semaphore_wait(hello, NQ - 1 - zq)

    def cz_all():
        for o in range(NQ):

            @pl.when(z != o)
            def _():
                cz(o).start()


    def wspread_start():
        wspread(0, 0).start()
        wspread(1, 0).start()

    def wspread_near():
        with jax.named_scope("wnear"):
            arrived(wall.at[c, 1:NY, 0 : 2 * RB], ws_r.at[0])
        wspread(0, 1).start()
        wspread(1, 1).start()

    def wspread_done():
        with jax.named_scope("wspread"):
            arrived(wall.at[c, 1:NY, 0:RB], ws_r.at[1])
        wrest().start()

    def sent_cell():
        for k, ref in enumerate((iv, fv, cv, nv)):
            arrived(ref.at[0:3], sent.at[k])
        arrived(b_send.at[0:3], sent.at[4])
        arrived(pm_send.at[:, 0 : NQ - 1], sent.at[8])
        arrived(p_send.at[:, 0 : NQ - 1], sent.at[9])

        @pl.when(z < NZ - 1)
        def _():
            arrived(tm_send.at[0 : H - 2], sent.at[5])
            arrived(t_send.at[0 : H - 2], sent.at[6])

        @pl.when(z < NQ)
        def _():
            arrived(cz_send.at[0 : NQ - 1], sent.at[7])
            arrived(hm_send, sent.at[16])
            arrived(h_send, sent.at[17])

        @pl.when(z >= NQ)
        def _():
            arrived(cz_send, sent.at[7])

        arrived(wall.at[c, 1:NY, 0 : 3 * RB], sent.at[14])

    def sent_rest():
        arrived(bm_send.at[0:3], sent.at[10])
        arrived(b_send.at[0:3], sent.at[11])
        arrived(wall.at[c, :, 0:352], sent.at[15])

    def sent_ring():
        arrived(wall.at[c, 1:NY, 0:832], sent.at[12])
        arrived(wall.at[c, 1:NY, 0:768], sent.at[13])

    @pl.when(z >= NZ // 2)
    def _():
        zgate()
        cz_all()

    inner(1)
    serve(1, "b")
    begin(0, 2)
    total(0)

    @pl.when(z < NZ // 2)
    def _():
        zgate()
        total_send(0)
        cz_all()
        inner(2)
        total(1)
        total_send(1)
        serve(2, "b")
        serve(0, 0)
        serve(0, 1)
        inner(3)
        total(2)
        total_send(2)
        serve(3, "half")
        wspread_start()
        serve(0, 2)
        total(3)
        total_send(3)
        scan(1)
        scan(0)
        serve(1, 0)
        scan(2)
        serve(1, 1)
        wspread_near()
        scan(3)
        spread(0)
        spread(1)
        serve(1, 2)
        spread(2)
        serve(2, 0)
        spread(3)
        serve(2, 1)
        finish(0)
        wspread_done()
        sent_cell()
        serve(2, 2)
        finish(1)
        arrived(wall.at[c, 0], wo_r.at[0])
        mates(0)
        finish(2)
        twos("early", early_one, 0, 2)
        serve(3, 0)
        mates(1)
        with jax.named_scope("early"):
            early_one(2)
            early_one(3)
            early_one(5)
        serve(3, "cut")
        finish(3)

    @pl.when(z >= NZ // 2)
    def _():
        total_send(0)
        inner(2)
        total(1)
        total_send(1)
        serve(2, "b")
        serve(0, 0)
        serve(0, 1)
        inner(3)
        total(2)
        total_send(2)
        serve(3, "half")
        wspread_start()
        serve(0, 2)
        total(3)
        total_send(3)
        serve(1, 0)
        scan(0)
        scan(1)
        serve(1, 1)
        wspread_near()
        spread(0)
        scan(2)
        scan(3)
        spread(1)
        serve(1, 2)
        spread(2)
        serve(2, 0)
        spread(3)
        serve(2, 1)
        finish(0)
        wspread_done()
        sent_cell()
        serve(2, 2)
        finish(1)
        arrived(wall.at[c, 0], wo_r.at[0])
        mates(0)
        finish(2)
        twos("early", early_one, 0, 2)
        serve(3, 0)
        mates(1)
        with jax.named_scope("early"):
            early_one(2)
            early_one(3)
            early_one(5)
        serve(3, "cut")
        finish(3)

    arrived(wall.at[c, 1:NY, RA:1024], ws_r.at[2])
    twos("late", late_one, 0, 3)
    with jax.named_scope("late"):
        late_one(5)
    sent_rest()
    mates(2)
    last()
    sent_ring()


def on_device(queries, keys, values, input_gate, forget_gate, start_memory, start_norm, start_level, head_gain, out_weight):
    arrays = (
        input_gate, forget_gate, queries, keys, values, start_memory.reshape(S, 32, D),
        jnp.transpose(start_norm, (0, 2, 1)), out_weight, start_level, head_gain,
    )
    dma, vmem = pltpu.SemaphoreType.DMA, pltpu.VMEM
    out = pl.pallas_call(
        kernel,
        out_shape=pltpu.VMEM((S * T, 4096), BF16),
        in_specs=[pl.BlockSpec(memory_space=pltpu.HBM)] * len(arrays),
        out_specs=pl.BlockSpec(memory_space=pltpu.VMEM),
        scratch_shapes=[
            vmem((S, H, T, D), BF16), vmem((S, H, T, D), BF16), vmem((S, H, T, D), BF16),
            vmem((S, H, T), BF16), vmem((S, H, T), BF16), vmem((S, 32, D), F32), vmem((S, 4, H), F32),
            vmem((NX, H, T, D), BF16), vmem((NX, H, T, D), BF16),
            vmem((NX, H, T), BF16), vmem((NX, H, T), BF16), vmem((NX, 32, D), F32), vmem((NX, 4, H), F32),
            vmem((S, H), F32), vmem((H, D), F32),
            vmem((2, NY, 1024, 256), BF16),
            vmem((S * H, T), F32),
            vmem((S * H, T, D), F32), vmem((S * H, T, D), F32), vmem((S * H, T, D), F32),
            vmem((NX, H, T), F32), vmem((NX, H, D), F32), vmem((NX, H, D), F32),
            vmem((NX, H, D, D), F32), vmem((NX, H, D), F32), vmem((D, D), F32),
            vmem((NQ, 40, D), F32), vmem((NZ, 40, D), F32),
            vmem((2, D, D), BF16), vmem((2, D, D), BF16), vmem((2, 8, D), F32), vmem((2, 8, D), F32),
            vmem((H, D, D), BF16), vmem((2, NQ, D, D), BF16),
            vmem((H, 8, D), F32), vmem((2, NQ, 8, D), F32),
            vmem((2, NQ, D, D), BF16), vmem((H, D, D), BF16),
            vmem((2, NQ, 8, D), F32), vmem((H, 8, D), F32),
            vmem((NX, H, D, D), BF16), vmem((S, H, D, D), BF16),
            vmem((NX, G, 8, D), F32), vmem((S, G, 8, D), F32),
            vmem((S * T, H * D), BF16), vmem((2, NY, S * T, 256), F32),
            dma((7,)), dma((18,)), dma((4,)), dma((2, G)), dma((3, 2)), dma((2, G)), dma((2, G)),
            dma((15,)), dma((3,)), dma((3,)), dma((1,)), dma((2, 2)), pltpu.SemaphoreType.REGULAR, pltpu.SemaphoreType.REGULAR,
        ],
        compiler_params=pltpu.CompilerParams(
            collective_id=0, has_side_effects=True, vmem_limit_bytes=50_000_000
        ),
        name="cell_layer",
    )(*(pltpu.with_memory_space_constraint(array, pltpu.HBM) for array in arrays))
    return out.reshape(S, T, 4096)


def solution(mesh):
    return jax.shard_map(
        on_device,
        mesh=mesh,
        in_specs=(
            P("dp", None, "sp", None),
            P("dp", None, "sp", None),
            P("dp", None, "sp", None),
            P("dp", None, "sp"),
            P("dp", None, "sp"),
            P("dp", None, "sp", None),
            P("dp", None, "sp"),
            P("dp", None),
            P(),
            P(None, "dp"),
        ),
        out_specs=P("dp", "sp", None),
        check_vma=False,
    )
```
